32 devices in a mesh: sp: 8 (over z, x), tp: 4 (over y, core).
Axes of the slice: x: 2, y: 2, z: 4, core: 2. Of those that a mesh axis runs over, the one named last changes fastest.
Arguments:
- moe_input: bfloat16 [1024, 2048], P('sp'), may hold values from -6 to 6
- out_grad: bfloat16 [1024, 2048], P('sp'), may hold values from -6 to 6
- routes: int32 [1024, 2], P('sp'), may hold values from 0 to 3, all different within a row; in each aligned block of 128 rows (0 to 127, 128 to 255, ...) at most 96 rows name the same one
- route_weights: float32 [1024, 2], P('sp'), may hold values from 0.2 to 1
- gate_cols: bfloat16 [2048, 14336], P(None, ('sp', 'tp')), may hold values from -0.125 to 0.125
- up_cols: bfloat16 [2048, 14336], P(None, ('sp', 'tp')), may hold values from -0.125 to 0.125
- down_rows: bfloat16 [14336, 2048], P(('sp', 'tp')), may hold values from -0.09375 to 0.09375
- out_proj: bfloat16 [2048, 512], P(None, 'tp'), may hold values from -0.25 to 0.25
- conv_out: bfloat16 [1024, 512], P('sp', 'tp'), may hold values from -6 to 6
- gate_b: bfloat16 [1024, 512], P('sp', 'tp'), may hold values from -6 to 6
- gate_c: bfloat16 [1024, 512], P('sp', 'tp'), may hold values from -6 to 6
- hidden_h: bfloat16 [1024, 512], P('sp', 'tp'), may hold values from -6 to 6
- conv_taps: float32 [3, 512], P(None, 'tp'), may hold values from -3.5 to 3.5
Outputs:
- grad_gate: bfloat16 [2048, 14336], P(None, ('sp', 'tp'))
- grad_up: bfloat16 [2048, 14336], P(None, ('sp', 'tp'))
- grad_down: bfloat16 [14336, 2048], P(('sp', 'tp'))
- grad_proj: float32 [2048, 512], P('sp', 'tp')
- grad_hidden: bfloat16 [1024, 512], P('sp', 'tp')
- grad_gate_b: bfloat16 [1024, 512], P('sp', 'tp')
- grad_gate_c: bfloat16 [1024, 512], P('sp', 'tp')
The draws below stay inside these ranges and needn't reach their ends.
Inputs may be any that keep to these rules, and one draw needn't show every extreme that they name: `routes`: each row names 2 different experts. Among the rows of one device no expert is named more than 96 times, a bound that some block reaches.
All inputs are finite; a program needn't handle non-finite values.
Results may differ from the reference program's by a relative error of at most 0.01.
Values may be sent and summed in bfloat16 or wider, within the bound.
A program may use at most 128 MiB of HBM per device.

```python
import math
from functools import partial
import jax
import jax.numpy as jnp
import numpy as np
from jax import lax

D = 2048
FF = 3584
CW = 512
KERNEL = 3
TOP = 2
TOK_DEV = 128
TOKENS = 1024
EXPERTS = 4
CAP = 96
N_SP = 8
N_TP = 4


def strengthened(drawn, own_key, source, target, blocks, factor):
    def block_of(position):
        return (jnp.arange(drawn.shape[position]) // (drawn.shape[position] // blocks)).reshape((-1,) + (1,) * (drawn.ndim - 1 - position))

    first = jax.random.permutation(own_key, blocks)[block_of(target)]
    second = (block_of(target) + blocks // 2) % blocks
    return jnp.where((block_of(source) == first) | (block_of(source) == second), factor * drawn, drawn)


def shard_levels(own_key, shape, split, least, high):
    def one(position, parts):
        steps = jax.random.uniform(jax.random.fold_in(jax.random.fold_in(own_key, 6), position), (parts,), jnp.float32, least / len(split), high / len(split))
        return jnp.repeat(jnp.exp(steps), shape[position] // parts).reshape((-1,) + (1,) * (len(shape) - position - 1))

    factor_of = one(*split[0])
    for cut in split[1:]:
        factor_of = factor_of * one(*cut)
    return factor_of


def assign_block(stream_key, own, number, rows, number_of, top, bound, slope):
    sequence = jax.random.permutation(stream_key, number_of)
    packed, common = load_shares(number_of, rows * top, bound, slope, True), load_shares(number_of, rows * top, bound, slope, False)
    places = jnp.arange(number_of)

    def named(sizes, offset_by):
        used = int((sizes > 0).sum())
        fixed = max(1, used // 4)
        shifted = fixed + (places - fixed + offset_by * (used - fixed)) % max(1, number_of - fixed)
        return jnp.zeros((number_of,), jnp.int32).at[sequence[jnp.where(places < fixed, places, shifted)]].set(jnp.asarray(sizes, jnp.int32))

    sizes = jnp.where(number % 4 == 0, named(packed, number // 4), named(common, number - number // 4 - 1))
    mixed = jax.random.permutation(jax.random.fold_in(own, 3), number_of)
    giver, taker = mixed[0:number_of // 2 * 2:2], mixed[1:number_of // 2 * 2:2]
    room = jnp.minimum(sizes[giver] - 1, bound - sizes[taker]) // 2
    room = jnp.where((giver == sequence[0]) | (taker == sequence[0]) | (sizes[taker] == 0), 0, jnp.maximum(room, 0))
    shifted = jax.random.randint(jax.random.fold_in(own, 4), (number_of // 2,), 0, 1 << 20) % (room + 1)
    sizes = sizes.at[giver].add(-shifted).at[taker].add(shifted)
    members = jnp.searchsorted(jnp.cumsum(sizes), jnp.arange(rows * top), side="right").astype(jnp.int32)
    grid = members.reshape(top, rows).T
    grid = grid[jax.random.permutation(jax.random.fold_in(own, 1), rows)]
    offset_by = jax.random.randint(jax.random.fold_in(own, 2), (rows, 1), 0, top)
    return jnp.take_along_axis(grid, (jnp.arange(top)[None, :] + offset_by) % top, axis=1)


def load_shares(number_of, total, reach, skew, full):
    loads = [(1 << 20) // math.isqrt(grade ** skew) + 1 for grade in range(1, number_of + 1)]
    largest = reach if full else min(reach, max(-(-total // number_of), total * loads[0] // sum(loads)))
    least = 1 if total - largest >= number_of - 1 else 0
    given, rest = [largest] + [least] * (number_of - 1), total - largest - least * (number_of - 1)
    while rest > 0:
        free = [i for i in range(1, number_of) if given[i] < largest] or [i for i in range(1, number_of) if given[i] < reach]
        mass, remaining = sum([loads[i] for i in free]), rest
        for i in free:
            addition = min(reach - given[i], max(1, remaining * loads[i] // mass), rest)
            given[i] = given[i] + addition
            rest = rest - addition
    return np.array(given)


def normal_values(key, dims, width, bound, split=(), kind=jnp.bfloat16):
    values = jax.random.normal(key, dims, jnp.float32) * width
    if len(split) > 0:
        values = shard_levels(key, dims, split, -0.22, 0.18) * values
    return jnp.clip(values, min=-bound, max=bound).astype(kind)


def noise_with(rng, dims, width, most, cuts, heavy, kind=jnp.bfloat16):
    values = width * jax.random.normal(rng, dims, jnp.float32)
    if cuts:
        values = values * shard_levels(rng, dims, cuts, -0.22, 0.18)
    return jnp.clip(strengthened(values, jax.random.fold_in(rng, 3), *heavy), -most, most).astype(kind)


def setup_inputs(seed: int = 0) -> dict:
    streams_of = jax.random.split(jax.random.key(seed), 14)
    moe_input = normal_values(streams_of[0], (TOKENS, D), 1.0, 6.0, ((0, 8),))
    out_grad = noise_with(streams_of[1], (TOKENS, D), 1.0, 6.0, ((0, 8),), (0, 1, 8, 2.0))
    routes_keys = jax.random.split(jax.random.fold_in(streams_of[2], 1), TOKENS // TOK_DEV)
    routes_turns = jax.random.permutation(jax.random.fold_in(streams_of[2], 3), TOKENS // TOK_DEV)
    routes = jax.vmap(lambda own, number: assign_block(jax.random.fold_in(streams_of[2], 2), own, number, TOK_DEV, EXPERTS, TOP, CAP, 2))(routes_keys, routes_turns).reshape((TOKENS, TOP))
    route_weights = jnp.clip(0.2 + 0.8 * jax.random.uniform(streams_of[3], (TOKENS, TOP), jnp.float32) ** shard_levels(streams_of[3], (TOKENS, TOP), ((0, 8),), -0.2, 0.2), 0.2, 1.0)
    gate_cols = normal_values(streams_of[4], (D, EXPERTS * FF), D ** -0.5, 0.125, ((1, 32),))
    up_cols = normal_values(streams_of[5], (D, EXPERTS * FF), D ** -0.5, 0.125, ((1, 32),))
    down_rows = normal_values(streams_of[6], (EXPERTS * FF, D), FF ** -0.5, 0.09375, ((0, 32),))
    out_proj = normal_values(streams_of[7], (D, CW), CW ** -0.5, 0.25, ((1, 4),))
    conv_out = normal_values(streams_of[8], (TOKENS, CW), 1.0, 6.0, ((0, 8), (1, 4)))
    gate_b = normal_values(streams_of[9], (TOKENS, CW), 1.0, 6.0, ((0, 8), (1, 4)))
    gate_c = normal_values(streams_of[10], (TOKENS, CW), 1.0, 6.0, ((0, 8), (1, 4)))
    hidden_h = normal_values(streams_of[11], (TOKENS, CW), 1.0, 6.0, ((0, 8), (1, 4)))
    conv_taps = normal_values(streams_of[12], (KERNEL, CW), KERNEL ** -0.5, 3.5, ((1, 4),), jnp.float32)
    return dict(moe_input=moe_input, out_grad=out_grad, routes=routes, route_weights=route_weights, gate_cols=gate_cols, up_cols=up_cols, down_rows=down_rows, out_proj=out_proj, conv_out=conv_out, gate_b=gate_b, gate_c=gate_c, hidden_h=hidden_h, conv_taps=conv_taps)


def slot_positions(route_block, experts, capacity):
    flat_ids = route_block.reshape(-1)
    one_hot = (flat_ids[:, None] == jnp.arange(experts, dtype=jnp.int32)[None, :]).astype(jnp.int32)
    earlier = jnp.cumsum(one_hot, axis=0) - one_hot
    ranked = jnp.sum(earlier * one_hot, axis=1)
    return (flat_ids * capacity + ranked).astype(jnp.int32)


def contract_rows(left_side, right_side):
    return lax.dot_general(left_side, right_side, (((0,), (0,)), ((), ())), preferred_element_type=jnp.float32)


def contract_cols(left_side, right_side):
    return lax.dot_general(left_side, right_side, (((1,), (1,)), ((), ())), preferred_element_type=jnp.float32)


def fill_table(slot_place, route_vals):
    return jnp.full((EXPERTS * CAP,), TOKENS * TOP, jnp.int32).at[slot_place].set(route_vals)


def reference(moe_input, out_grad, routes, route_weights, gate_cols, up_cols, down_rows, out_proj, conv_out, gate_b, gate_c, hidden_h, conv_taps):
    positions = jax.vmap(partial(slot_positions, experts=EXPERTS, capacity=CAP))(routes.reshape(N_SP, TOK_DEV, TOP))
    pair_ids = (jnp.arange(N_SP, dtype=jnp.int32)[:, None] * (TOK_DEV * TOP)
                + jnp.arange(TOK_DEV * TOP, dtype=jnp.int32)[None, :])
    tables = jax.vmap(fill_table)(positions, pair_ids)
    tables = jnp.transpose(tables.reshape(N_SP, EXPERTS, CAP), (1, 0, 2))
    scaled = (route_weights[:, :, None] * out_grad[:, None, :].astype(jnp.float32)).astype(jnp.bfloat16)
    scaled = scaled.reshape(TOKENS * TOP, D)
    zero_row = jnp.zeros((1, D), jnp.bfloat16)
    padded_x = jnp.concatenate([moe_input, zero_row], axis=0)
    padded_g = jnp.concatenate([scaled, zero_row], axis=0)
    unit_block = FF // (2 * N_TP)

    def expert_step(gathered, inputs):
        slot_table, expert_index = inputs
        route_rows = slot_table.reshape(-1)
        token_rows = route_rows // TOP
        rows_x = padded_x[token_rows]
        rows_g = padded_g[route_rows]
        w_gate = lax.dynamic_slice_in_dim(gate_cols, expert_index * FF, FF, 1)
        w_up = lax.dynamic_slice_in_dim(up_cols, expert_index * FF, FF, 1)
        w_down = lax.dynamic_slice_in_dim(down_rows, expert_index * FF, FF, 0)
        gate_pre = jnp.dot(rows_x, w_gate, preferred_element_type=jnp.float32)
        up_pre = jnp.dot(rows_x, w_up, preferred_element_type=jnp.float32)
        sigmoid_g = jax.nn.sigmoid(gate_pre)
        silu_g = gate_pre * sigmoid_g
        activation = (silu_g * up_pre).astype(jnp.bfloat16)
        grad_down_e = contract_rows(activation, rows_g).astype(jnp.bfloat16)
        d_act = contract_cols(rows_g, w_down)
        d_up = (d_act * silu_g).astype(jnp.bfloat16)
        d_gate = (d_act * up_pre * sigmoid_g * (1.0 + gate_pre * (1.0 - sigmoid_g))).astype(jnp.bfloat16)
        grad_gate_e = contract_rows(rows_x, d_gate).astype(jnp.bfloat16)
        grad_up_e = contract_rows(rows_x, d_up).astype(jnp.bfloat16)
        back_rows = jnp.zeros((route_rows.shape[0], D), jnp.float32)
        for half_index in range(2):
            running = jnp.zeros((route_rows.shape[0], D), jnp.float32)
            for quarter_index in range(N_TP):
                first_unit = (half_index * N_TP + quarter_index) * unit_block
                piece_sum = (contract_cols(d_gate[:, first_unit:first_unit + unit_block], w_gate[:, first_unit:first_unit + unit_block])
                             + contract_cols(d_up[:, first_unit:first_unit + unit_block], w_up[:, first_unit:first_unit + unit_block]))
                piece_sum = lax.optimization_barrier(piece_sum.astype(jnp.bfloat16))
                running = running + piece_sum.astype(jnp.float32)
            half_sum = lax.optimization_barrier(running.astype(jnp.bfloat16))
            back_rows = back_rows + half_sum.astype(jnp.float32)
        gathered = gathered.at[token_rows].add(back_rows)
        return gathered, (grad_gate_e, grad_up_e, grad_down_e)

    start_back = jnp.zeros((TOKENS + 1, D), jnp.float32)
    moe_back, stacked = lax.scan(expert_step, start_back, (tables, jnp.arange(EXPERTS, dtype=jnp.int32)))
    grad_gate = jnp.transpose(stacked[0], (1, 0, 2)).reshape(D, EXPERTS * FF)
    grad_up = jnp.transpose(stacked[1], (1, 0, 2)).reshape(D, EXPERTS * FF)
    grad_down = stacked[2].reshape(EXPERTS * FF, D)
    stream_grad = (out_grad.astype(jnp.float32) + moe_back[:TOKENS]).astype(jnp.bfloat16)
    branch = (gate_b.astype(jnp.float32) * conv_out.astype(jnp.float32)).astype(jnp.bfloat16)
    d_branch = jnp.dot(stream_grad, out_proj, preferred_element_type=jnp.float32)
    grad_proj = contract_rows(stream_grad, branch)
    grad_gate_b = (d_branch * conv_out.astype(jnp.float32)).astype(jnp.bfloat16)
    d_conv = d_branch * gate_b.astype(jnp.float32)
    extended = jnp.concatenate([d_conv, jnp.zeros((KERNEL - 1, CW), jnp.float32)], axis=0)
    d_input = jnp.zeros((TOKENS, CW), jnp.float32)
    for tap_index in range(KERNEL):
        offset = KERNEL - 1 - tap_index
        d_input = d_input + conv_taps[tap_index][None, :] * extended[offset:offset + TOKENS]
    grad_hidden = (d_input * gate_c.astype(jnp.float32)).astype(jnp.bfloat16)
    grad_gate_c = (d_input * hidden_h.astype(jnp.float32)).astype(jnp.bfloat16)
    return (grad_gate, grad_up, grad_down, grad_proj, grad_hidden, grad_gate_b, grad_gate_c)
```

```python
import functools

import jax
import jax.numpy as jnp
from jax import lax
from jax.experimental import pallas as pl
from jax.experimental.pallas import tpu as pltpu
from jax.sharding import PartitionSpec as P


def from_behind(block, axis, distance):
    devices = range(lax.axis_size(axis))
    route = [(i - distance, i) for i in devices if i - distance in devices]
    return lax.ppermute(block, axis, route)


MESH = pl.DeviceIdType.MESH
VMEM = pl.BlockSpec(memory_space=pltpu.VMEM)


def columns(index, width):
    return pl.ds(pl.multiple_of(index * width, width), width)


def wait_arrival(ref, sem):
    pltpu.make_async_copy(ref, ref, sem).wait()


def greet(peers):
    barrier = pltpu.get_barrier_semaphore()
    for peer in peers:
        pl.semaphore_signal(barrier, inc=1, device_id=peer, device_id_type=MESH)
    pl.semaphore_wait(barrier, len(peers))


def place(n_tp):
    sp, tp = lax.axis_index("sp"), lax.axis_index("tp")
    expert, parity = sp // 2, lax.rem(sp, 2)
    row, core = tp // 2, lax.rem(tp, 2)
    return sp, tp, expert, parity, row, core


def dispatch_kernel(
    n_sp, n_tp, chunks,
    x_ref, g_ref, branch_ref, head_ref,
    out_x, out_g, out_b, out_head,
    z_send, z_recv, own_send, relay_send, near_recv, diag_recv, pair_send, pair_recv, b_send, b_recv, h_send, h_recv,
):
    experts = n_sp // 2
    sp, tp, expert, parity, row, core = place(n_tp)
    width = x_ref.shape[-1]
    size = experts // chunks
    x_side = (2 * expert + 1 - parity, tp)
    y_side = (sp, 2 * (1 - row) + core)
    pair = (sp, 2 * row + 1 - core)
    greet([(lax.rem(sp + d, n_sp), tp) for d in range(1, n_sp)] + [y_side, pair])
    started = []
    sources, outs = (x_ref, g_ref), (out_x, out_g)

    def spot(t, par, first, quarter, count):
        return outs[t].at[par, pl.ds(first, count), :, columns(quarter, width)]

    def send(src, device, send_sem, recv_sem):
        copy = pltpu.make_async_remote_copy(
            src_ref=src, dst_ref=src, send_sem=send_sem, recv_sem=recv_sem,
            device_id=device, device_id_type=MESH,
        )
        copy.start()
        started.append(copy)

    for t in range(2):
        for d in range(experts):
            target = lax.rem(expert + d, experts)
            src = sources[t].at[pl.ds(target, 1)]
            dst = spot(t, parity, expert, tp, 1)
            if d == 0:
                pltpu.make_async_copy(src, dst, z_recv.at[t, 0]).start()
                continue
            copy = pltpu.make_async_remote_copy(
                src_ref=src, dst_ref=dst, send_sem=z_send.at[t, d], recv_sem=z_recv.at[t, d],
                device_id=(2 * target + parity, tp), device_id_type=MESH,
            )
            copy.start()
            started.append(copy)
    for d in range(n_sp):
        dst = out_b.at[sp]
        if d == 0:
            pltpu.make_async_copy(branch_ref, dst, b_recv.at[0]).start()
            continue
        copy = pltpu.make_async_remote_copy(
            src_ref=branch_ref, dst_ref=dst, send_sem=b_send.at[d], recv_sem=b_recv.at[d],
            device_id=(lax.rem(sp + d, n_sp), tp), device_id_type=MESH,
        )
        copy.start()
        started.append(copy)

    copy = pltpu.make_async_remote_copy(
        src_ref=head_ref, dst_ref=out_head, send_sem=h_send.at[0], recv_sem=h_recv.at[0],
        device_id=(lax.rem(sp + n_sp - 1, n_sp), tp), device_id_type=MESH,
    )
    copy.start()
    started.append(copy)

    own_chunk = expert // size
    other_quarter = 2 * (1 - row) + core

    def first_of(k):
        return lax.rem(own_chunk + chunks - k, chunks) * size

    def own_stage(k, t):
        first = first_of(k)
        for i in range(size):
            source = first + i
            d = lax.rem(expert + experts - source, experts)
            wait_arrival(spot(t, parity, source, tp, 1), z_recv.at[t, d])
        block = spot(t, parity, first, tp, size)
        send(block, x_side, own_send.at[t, k, 0], near_recv.at[t, k, 0])
        send(block, y_side, own_send.at[t, k, 1], near_recv.at[t, k, 1])
        send(block, pair, pair_send.at[t, k, 0], pair_recv.at[t, k, 0])

    def near_stage(k, t):
        first = first_of(k)
        from_x = spot(t, 1 - parity, first, tp, size)
        from_y = spot(t, parity, first, other_quarter, size)
        wait_arrival(from_x, near_recv.at[t, k, 0])
        if (k + t) % 2 == 0:
            send(from_x, y_side, relay_send.at[t, k], diag_recv.at[t, k])
        send(from_x, pair, pair_send.at[t, k, 1], pair_recv.at[t, k, 1])
        wait_arrival(from_y, near_recv.at[t, k, 1])
        if (k + t) % 2 == 1:
            send(from_y, x_side, relay_send.at[t, k], diag_recv.at[t, k])
        send(from_y, pair, pair_send.at[t, k, 2], pair_recv.at[t, k, 2])

    def far_stage(k, t):
        block = spot(t, 1 - parity, first_of(k), other_quarter, size)
        wait_arrival(block, diag_recv.at[t, k])
        send(block, pair, pair_send.at[t, k, 3], pair_recv.at[t, k, 3])

    order = [0] + [k for n in range(1, chunks // 2 + 1) for k in dict.fromkeys((n, chunks - n))]
    steps = [(k, t) for k in order for t in range(2)]
    for n in range(len(steps) + 3):
        if n < len(steps):
            own_stage(*steps[n])
        if 1 <= n < len(steps) + 1:
            near_stage(*steps[n - 1])
        if 3 <= n < len(steps) + 3:
            far_stage(*steps[n - 3])
    for k, t in steps:
        first = first_of(k)
        quarters = (2 * row + 1 - core, 2 * (1 - row) + 1 - core)
        spots = ((parity, quarters[0]), (1 - parity, quarters[0]),
                 (parity, quarters[1]), (1 - parity, quarters[1]))
        for j, (par, quarter) in enumerate(spots):
            wait_arrival(spot(t, par, first, quarter, size), pair_recv.at[t, k, j])
    for d in range(n_sp):
        wait_arrival(out_b.at[lax.rem(sp + n_sp - d, n_sp)], b_recv.at[d])
    wait_arrival(out_head, h_recv.at[0])
    for copy in started:
        copy.wait_send()


def dispatch(x, g, branch, head, n_sp, n_tp):
    experts, capacity, width = x.shape
    chunks = min(experts, 4)
    dma = pltpu.SemaphoreType.DMA
    rows = jax.ShapeDtypeStruct((2, experts, capacity, width * n_tp), jnp.bfloat16)
    return pl.pallas_call(
        functools.partial(dispatch_kernel, n_sp, n_tp, chunks),
        out_shape=(
            rows, rows, jax.ShapeDtypeStruct((n_sp,) + branch.shape, branch.dtype),
            jax.ShapeDtypeStruct(head.shape, head.dtype),
        ),
        in_specs=[VMEM] * 4,
        out_specs=(VMEM,) * 4,
        scratch_shapes=[
            dma((2, experts)), dma((2, experts)), dma((2, chunks, 2)), dma((2, chunks)),
            dma((2, chunks, 2)), dma((2, chunks)), dma((2, chunks, 4)), dma((2, chunks, 4)),
            dma((n_sp,)), dma((n_sp,)), dma((1,)), dma((1,)),
        ],
        compiler_params=pltpu.CompilerParams(
            collective_id=0, has_side_effects=True, vmem_limit_bytes=48 * 1024 * 1024
        ),
    )(x, g, branch, head)


def return_kernel(
    n_sp, n_tp, chunks,
    part_ref, out_ref,
    from_pair, summed, from_chips, final,
    pair_send, pair_recv, chip_send, chip_recv, z_send, z_recv,
):
    experts = n_sp // 2
    sp, tp, expert, parity, row, core = place(n_tp)
    width = out_ref.shape[-1]
    pair = (sp, 2 * row + 1 - core)
    offsets = ((1, 1), (1, 0), (0, 1), (0, 0))

    def other(dp, dr):
        return lax.rem(parity + dp, 2), lax.rem(row + dr, 2)

    chips = [(2 * expert + other(dp, dr)[0], 2 * other(dp, dr)[1] + core) for dp, dr in offsets[:3]]
    along = [(2 * lax.rem(expert + d, experts) + parity, tp) for d in range(1, experts)]
    greet([pair] + chips + along)
    started, guarded = [], []

    def send(src, dst, send_sem, recv_sem, device):
        copy = pltpu.make_async_remote_copy(
            src_ref=src, dst_ref=dst, send_sem=send_sem, recv_sem=recv_sem,
            device_id=device, device_id_type=MESH,
        )
        copy.start()
        started.append(copy)

    size = experts // chunks
    own_chunk = expert // size
    order = [chunks // 2] if chunks > 1 else []
    order += [k for k in range(1, chunks) if k not in order] + [0]

    def first_of(k):
        return lax.rem(own_chunk + k, chunks) * size

    for k in order:
        part = pl.ds(first_of(k), size)
        for n, (dp, dr) in enumerate(offsets):
            par, line = other(dp, dr)
            src = part_ref.at[par, part, :, columns(2 * line + 1 - core, width)]
            send(src, from_pair.at[n, part], pair_send.at[n, k], pair_recv.at[n, k], pair)
    for k in order:
        first = first_of(k)
        part = pl.ds(first, size)
        for n, (dp, dr) in enumerate(offsets):
            par, line = other(dp, dr)
            wait_arrival(from_pair.at[n, part], pair_recv.at[n, k])
            for i in range(size):
                mine = part_ref[par, first + i, :, columns(2 * line + core, width)]
                total = mine.astype(jnp.float32) + from_pair[n, first + i].astype(jnp.float32)
                summed[n, first + i] = total.astype(jnp.bfloat16)
            if n < 3:
                send(summed.at[n, part], from_chips.at[n, part], chip_send.at[n, k],
                     chip_recv.at[n, k], chips[n])
    for k in order:
        first = first_of(k)
        part = pl.ds(first, size)
        for n in range(3):
            wait_arrival(from_chips.at[n, part], chip_recv.at[n, k])
        for i in range(size):
            target = first + i
            total = summed[3, target].astype(jnp.float32)
            for n in range(3):
                total = total + from_chips[n, target].astype(jnp.float32)
            final[target] = total.astype(jnp.bfloat16)
            away = target != expert
            copy = pltpu.make_async_remote_copy(
                src_ref=final.at[target], dst_ref=out_ref.at[expert],
                send_sem=z_send.at[target], recv_sem=z_recv.at[expert],
                device_id=(2 * target + parity, tp), device_id_type=MESH,
            )
            if size == 1 and k:
                copy.start()
                started.append(copy)
                continue
            if size == 1:
                out_ref[expert] = final[target]
                continue

            @pl.when(away)
            def _(copy=copy):
                copy.start()

            @pl.when(jnp.logical_not(away))
            def _():
                out_ref[expert] = final[expert]

            guarded.append((away, copy))
    for d in range(1, experts):
        source = lax.rem(expert + experts - d, experts)
        wait_arrival(out_ref.at[source], z_recv.at[source])
    for copy in started:
        copy.wait_send()
    for away, copy in guarded:
        pl.when(away)(copy.wait_send)


def give_back(part, n_sp, n_tp):
    _, experts, capacity, model_width = part.shape
    width = model_width // n_tp
    dma = pltpu.SemaphoreType.DMA
    block = (experts, capacity, width)
    chunks = min(experts, 4)
    return pl.pallas_call(
        functools.partial(return_kernel, n_sp, n_tp, chunks),
        out_shape=jax.ShapeDtypeStruct(block, jnp.bfloat16),
        in_specs=[VMEM],
        out_specs=VMEM,
        scratch_shapes=[
            pltpu.VMEM((4,) + block, jnp.bfloat16), pltpu.VMEM((4,) + block, jnp.bfloat16),
            pltpu.VMEM((3,) + block, jnp.bfloat16), pltpu.VMEM(block, jnp.bfloat16),
            dma((4, chunks)), dma((4, chunks)), dma((3, chunks)), dma((3, chunks)),
            dma((experts,)), dma((experts,)),
        ],
        compiler_params=pltpu.CompilerParams(
            collective_id=1, has_side_effects=True, vmem_limit_bytes=48 * 1024 * 1024
        ),
    )(part)


def dot(left, right, left_dim, right_dim):
    return lax.dot_general(
        left, right, (((left_dim,), (right_dim,)), ((), ())), preferred_element_type=jnp.float32
    )


def flipped(index, bits):
    bit = 1
    while bit <= bits:
        if bits & bit:
            index = index + bit - 2 * bit * lax.rem(index // bit, 2)
        bit *= 2
    return index


def expert_kernel(
    n_sp, n_tp,
    sent_x, sent_g, own_x, own_g, branch_ref, head_ref, wg, wu, wd,
    out_back, out_b, out_head, out_gate, out_up, out_down,
    rows_x, rows_g, act, dup, dgt, part_out, part_mine, from_pair, summed,
    near_x, near_y, passed, far_x, far_y, final,
    z_send, z_recv, own_send, own_recv, line_send, line_recv, relay_send, relay_recv,
    pair_send, pair_recv, own_pair_send, own_pair_recv, b_send, b_recv, h_send, h_recv,
    rp_send, rp_recv, near_send, near_recv, far_send, far_recv, back_send, back_recv,
):
    experts = n_sp // 2
    sp, tp, expert, parity, row, core = place(n_tp)
    capacity, width = sent_x.shape[1:]
    model_width = own_x.shape[1]
    wide = model_width // 2
    half = width // 2
    x_side = (2 * expert + 1 - parity, tp)
    y_side = (sp, 2 * (1 - row) + core)
    pair = (sp, 2 * row + 1 - core)
    other_quarter = 2 * (1 - row) + core
    sources, owned, rows = (sent_x, sent_g), (own_x, own_g), (rows_x, rows_g)
    started = []

    def send(src, dst, send_sem, recv_sem, device):
        copy = pltpu.make_async_remote_copy(
            src_ref=src, dst_ref=dst, send_sem=send_sem, recv_sem=recv_sem,
            device_id=device, device_id_type=MESH,
        )
        copy.start()
        started.append(copy)

    def spot(t, j, par, quarter):
        return rows[t].at[flipped(expert, j), par, :, columns(quarter, width)]

    def side(t, par, which):
        return rows[t].at[expert, par, :, columns(which, wide)]

    greet([(lax.rem(sp + d, n_sp), tp) for d in range(1, n_sp)] + [y_side, pair])
    order = [1] + list(range(experts - 1, 1, -1))
    steps = [(j, t) for j in order for t in range(2)]
    for j, t in steps:
        target = flipped(expert, j)
        send(sources[t].at[target], rows[t].at[expert, parity, :, columns(tp, width)],
             z_send.at[t, j], z_recv.at[t, j], (2 * target + parity, tp))
    for t in range(2):
        send(owned[t].at[:, columns(core, wide)], side(t, parity, core), own_send.at[t], own_recv.at[t], x_side)
    for t in range(2):
        rows[t][expert, parity] = owned[t][...]

    def own_stage(n):
        j, t = steps[n]
        block = spot(t, j, parity, tp)
        wait_arrival(block, z_recv.at[t, j])
        send(block, block, line_send.at[t, j, 0], line_recv.at[t, j, 0], x_side)
        send(block, block, line_send.at[t, j, 1], line_recv.at[t, j, 1], y_side)
        send(block, block, pair_send.at[t, j, 0], pair_recv.at[t, j, 0], pair)

    def across_stage(t):
        block = side(t, 1 - parity, core)
        wait_arrival(block, own_recv.at[t])
        send(block, block, own_pair_send.at[t], own_pair_recv.at[t], pair)

    def near_x_stage(n):
        j, t = steps[n]
        block = spot(t, j, 1 - parity, tp)
        wait_arrival(block, line_recv.at[t, j, 0])
        if n % 3:
            send(block, block, relay_send.at[t, j], relay_recv.at[t, j], y_side)
        send(block, block, pair_send.at[t, j, 1], pair_recv.at[t, j, 1], pair)

    def near_y_stage(n):
        j, t = steps[n]
        block = spot(t, j, parity, other_quarter)
        wait_arrival(block, line_recv.at[t, j, 1])
        if n % 3 == 0:
            send(block, block, relay_send.at[t, j], relay_recv.at[t, j], x_side)
        send(block, block, pair_send.at[t, j, 2], pair_recv.at[t, j, 2], pair)

    def far_stage(n):
        j, t = steps[n]
        block = spot(t, j, 1 - parity, other_quarter)
        wait_arrival(block, relay_recv.at[t, j])
        send(block, block, pair_send.at[t, j, 3], pair_recv.at[t, j, 3], pair)

    def forward(j):
        source = flipped(expert, j)
        for t in range(2):
            if j == 0:
                wait_arrival(side(t, 1 - parity, 1 - core), own_pair_recv.at[t])
                continue
            quarters = (2 * row + 1 - core, 2 * (1 - row) + 1 - core)
            spots = ((parity, quarters[0]), (1 - parity, quarters[0]),
                     (parity, quarters[1]), (1 - parity, quarters[1]))
            for n, (par, quarter) in enumerate(spots):
                wait_arrival(spot(t, j, par, quarter), pair_recv.at[t, j, n])
        x = rows_x[source].reshape(2 * capacity, model_width)
        g = rows_g[source].reshape(2 * capacity, model_width)
        gate = dot(x, wg[...], 1, 1)
        up = dot(x, wu[...], 1, 1)
        d_act = dot(g, wd[...], 1, 1)
        s = jax.nn.sigmoid(gate)
        silu = gate * s
        act[source] = (silu * up).astype(jnp.bfloat16)
        dup[source] = (d_act * silu).astype(jnp.bfloat16)
        dgt[source] = (d_act * up * s * (1.0 + gate * (1.0 - s))).astype(jnp.bfloat16)

    def backward(j):
        source = flipped(expert, j)
        for kept in range(2):
            side_core = core if kept else 1 - core
            store = part_mine if kept else part_out
            for line in range(2):
                cols = columns(2 * line + side_core, width)
                value = (
                    dot(dgt[source], wg[:, cols], 1, 0) + dot(dup[source], wu[:, cols], 1, 0)
                ).astype(jnp.bfloat16)
                for par in range(2):
                    piece = value[par * capacity : (par + 1) * capacity]
                    store[j, 0, par, line] = piece[:, :half]
                    store[j, 1, par, line] = piece[:, half:]
            if not kept:
                send(part_out.at[j], from_pair.at[j], rp_send.at[j], rp_recv.at[j], pair)

    def reduce_pair(j):
        wait_arrival(from_pair.at[j], rp_recv.at[j])
        total = part_mine[j].astype(jnp.float32) + from_pair[j].astype(jnp.float32)
        summed[j] = total.astype(jnp.bfloat16)
        send(summed.at[j, 0, 1 - parity], near_x.at[j], near_send.at[j, 0], near_recv.at[j, 0], x_side)
        send(summed.at[j, 1, :, 1 - row], near_y.at[j], near_send.at[j, 1], near_recv.at[j, 1], y_side)

    def reduce_near(j):
        wait_arrival(near_x.at[j], near_recv.at[j, 0])
        total = summed[j, 0, parity, 1 - row].astype(jnp.float32) + near_x[j, 1 - row].astype(jnp.float32)
        passed[j, 0] = total.astype(jnp.bfloat16)
        send(passed.at[j, 0], far_y.at[j], far_send.at[j, 0], far_recv.at[j, 0], y_side)
        wait_arrival(near_y.at[j], near_recv.at[j, 1])
        total = summed[j, 1, 1 - parity, row].astype(jnp.float32) + near_y[j, 1 - parity].astype(jnp.float32)
        passed[j, 1] = total.astype(jnp.bfloat16)
        send(passed.at[j, 1], far_x.at[j], far_send.at[j, 1], far_recv.at[j, 1], x_side)

    def reduce_far(j):
        wait_arrival(far_y.at[j], far_recv.at[j, 0])
        wait_arrival(far_x.at[j], far_recv.at[j, 1])
        left = summed[j, 0, parity, row].astype(jnp.float32) + near_x[j, row].astype(jnp.float32)
        left = (left + far_y[j].astype(jnp.float32)).astype(jnp.bfloat16)
        right = summed[j, 1, parity, row].astype(jnp.float32) + near_y[j, parity].astype(jnp.float32)
        right = (right + far_x[j].astype(jnp.float32)).astype(jnp.bfloat16)
        if j == 0:
            out_back[expert, :, :half] = left
            out_back[expert, :, half:] = right
            return
        final[j, :, :half] = left
        final[j, :, half:] = right
        target = flipped(expert, j)
        send(final.at[j], out_back.at[expert], back_send.at[j], back_recv.at[j], (2 * target + parity, tp))

    def weight_grad(out, left, right, pieces):
        tile = model_width // pieces
        lhs = left[...].reshape(-1, left.shape[-1])
        for n in range(pieces):
            rhs = right[..., n * tile : (n + 1) * tile].reshape(-1, tile)
            out[:, n * tile : (n + 1) * tile] = dot(lhs, rhs, 0, 0).astype(jnp.bfloat16)

    def share_branch():
        out_b[sp] = branch_ref[...]
        for d in range(1, n_sp):
            send(branch_ref, out_b.at[sp], b_send.at[d], b_recv.at[d], (lax.rem(sp + d, n_sp), tp))
        send(head_ref, out_head, h_send.at[0], h_recv.at[0], (lax.rem(sp + n_sp - 1, n_sp), tp))

    def some(stage, *numbers):
        for n in numbers:
            if n < len(steps):
                stage(n)

    chunk = [0] + order
    some(own_stage, 0, 1)
    across_stage(0)
    some(near_y_stage, 0, 1)
    across_stage(1)
    some(own_stage, 2, 3)
    forward(0)
    some(near_x_stage, 0, 1)
    backward(0)
    for i in range(1, experts):
        n = 2 * i
        some(near_y_stage, n, n + 1)
        some(far_stage, n - 2, n - 1)
        some(own_stage, n + 2, n + 3)
        reduce_pair(chunk[i - 1])
        if i == 2:
            share_branch()
        forward(chunk[i])
        some(near_x_stage, n, n + 1)
        reduce_near(chunk[i - 1])
        backward(chunk[i])
        reduce_far(chunk[i - 1])
    if experts == 2:
        share_branch()
    last = chunk[-1]
    reduce_pair(last)
    weight_grad(out_down, act, rows_g, 4)
    reduce_near(last)
    weight_grad(out_gate, dgt, rows_x, 4)
    reduce_far(last)
    weight_grad(out_up, dup, rows_x, 4)
    for j in order:
        wait_arrival(out_back.at[flipped(expert, j)], back_recv.at[j])
    for d in range(1, n_sp):
        wait_arrival(out_b.at[lax.rem(sp + n_sp - d, n_sp)], b_recv.at[d])
    wait_arrival(out_head, h_recv.at[0])
    for copy in started:
        copy.wait_send()


def run_experts(sent_x, sent_g, own_x, own_g, branch, head, wg, wu, wd, n_sp, n_tp):
    experts, capacity, width = sent_x.shape
    model_width = own_x.shape[1]
    units = wg.shape[0]
    half = width // 2
    dma = pltpu.SemaphoreType.DMA
    bf16 = jnp.bfloat16

    def out(*shape):
        return jax.ShapeDtypeStruct(shape, bf16)

    def vmem(*shape):
        return pltpu.VMEM(shape, bf16)

    rows = vmem(experts, 2, capacity, model_width)
    hidden = vmem(experts, 2 * capacity, units)
    blocks = vmem(experts, 2, 2, 2, capacity, half)
    near = vmem(experts, 2, capacity, half)
    far = vmem(experts, capacity, half)
    return pl.pallas_call(
        functools.partial(expert_kernel, n_sp, n_tp),
        out_shape=(
            out(experts, capacity, width), out(n_sp, *branch.shape), out(*head.shape),
            out(units, model_width), out(units, model_width), out(units, model_width),
        ),
        in_specs=[VMEM] * 9,
        out_specs=(VMEM,) * 6,
        scratch_shapes=[
            rows, rows, hidden, hidden, hidden, blocks, blocks, blocks, blocks,
            near, near, near, far, far, vmem(experts, capacity, width),
            dma((2, experts)), dma((2, experts)), dma((2,)), dma((2,)),
            dma((2, experts, 2)), dma((2, experts, 2)), dma((2, experts)), dma((2, experts)),
            dma((2, experts, 4)), dma((2, experts, 4)), dma((2,)), dma((2,)),
            dma((n_sp,)), dma((n_sp,)), dma((1,)), dma((1,)),
            dma((experts,)), dma((experts,)), dma((experts, 2)), dma((experts, 2)),
            dma((experts, 2)), dma((experts, 2)), dma((experts,)), dma((experts,)),
        ],
        compiler_params=pltpu.CompilerParams(
            collective_id=3, has_side_effects=True, vmem_limit_bytes=56 * 1024 * 1024
        ),
    )(sent_x, sent_g, own_x, own_g, branch, head, wg, wu, wd)


def stream_kernel(
    n_sp, n_tp, part_ref, stream_ref, block_ref,
    tp_send, tp_recv, h_send, h_recv, b_send, b_recv, s_send, s_recv,
):
    sp, tp = lax.axis_index("sp"), lax.axis_index("tp")
    tokens, width = part_ref.shape
    block = block_ref.shape[2]
    halo = stream_ref.shape[0] - tokens
    per_part, per_peer = width // block, n_sp // n_tp
    greet([
        (lax.rem(sp + i, n_sp), lax.rem(tp + j, n_tp))
        for i in range(n_sp) for j in range(n_tp) if i or j
    ])
    started = []

    def send(src, dst, send_sem, recv_sem, device):
        copy = pltpu.make_async_remote_copy(
            src_ref=src, dst_ref=dst, send_sem=send_sem, recv_sem=recv_sem,
            device_id=device, device_id_type=MESH,
        )
        copy.start()
        started.append((None, copy))

    keeper = sp // per_peer
    for b in range(per_part):
        target = tp * per_part + b
        src = part_ref.at[:, b * block : (b + 1) * block]
        dst = block_ref.at[sp]
        away = jnp.logical_or(target != sp, keeper != tp)
        copy = pltpu.make_async_remote_copy(
            src_ref=src, dst_ref=dst, send_sem=b_send.at[b], recv_sem=b_recv.at[lax.rem(sp, per_peer)],
            device_id=(target, keeper), device_id_type=MESH,
        )

        @pl.when(away)
        def _(copy=copy):
            copy.start()

        @pl.when(jnp.logical_not(away))
        def _(src=src, dst=dst):
            pltpu.make_async_copy(src, dst, b_recv.at[lax.rem(sp, per_peer)]).start()

        started.append((away, copy))
    mine = stream_ref.at[pl.ds(0, tokens), columns(tp, width)]
    edge = stream_ref.at[pl.ds(tokens, halo), columns(tp, width)]
    before = lax.rem(sp + n_sp - 1, n_sp)
    pltpu.make_async_copy(part_ref, mine, tp_recv.at[0]).start()
    for j in range(n_tp):
        peer = lax.rem(tp + j, n_tp)
        if j:
            send(part_ref, mine, tp_send.at[j], tp_recv.at[j], (sp, peer))
        send(part_ref.at[pl.ds(0, halo)], edge, h_send.at[j], h_recv.at[j], (before, peer))
    for n in range(per_peer):
        held = block_ref.at[tp * per_peer + n]
        wait_arrival(held, b_recv.at[n])
        for j in range(1, n_tp):
            send(held, held, s_send.at[n, j], s_recv.at[n, j], (sp, lax.rem(tp + j, n_tp)))
    for j in range(n_tp):
        source = lax.rem(tp + n_tp - j, n_tp)
        wait_arrival(stream_ref.at[pl.ds(0, tokens), columns(source, width)], tp_recv.at[j])
        wait_arrival(stream_ref.at[pl.ds(tokens, halo), columns(source, width)], h_recv.at[j])
        for n in range(per_peer):
            if j:
                wait_arrival(block_ref.at[source * per_peer + n], s_recv.at[n, j])
    for away, copy in started:
        if away is None:
            copy.wait_send()
        else:
            pl.when(away)(copy.wait_send)


def share_stream(part, halo, n_sp, n_tp):
    tokens, width = part.shape
    dma = pltpu.SemaphoreType.DMA
    block = width * n_tp // n_sp
    per_peer = n_sp // n_tp
    return pl.pallas_call(
        functools.partial(stream_kernel, n_sp, n_tp),
        out_shape=(
            jax.ShapeDtypeStruct((tokens + halo, width * n_tp), jnp.bfloat16),
            jax.ShapeDtypeStruct((n_sp, tokens, block), jnp.bfloat16),
        ),
        in_specs=[VMEM],
        out_specs=(VMEM, VMEM),
        scratch_shapes=[
            dma((n_tp,)), dma((n_tp,)), dma((n_tp,)), dma((n_tp,)),
            dma((width // block,)), dma((per_peer,)), dma((per_peer, n_tp)), dma((per_peer, n_tp)),
        ],
        compiler_params=pltpu.CompilerParams(collective_id=2, has_side_effects=True),
    )(part)


def slot_choice(routes, experts, capacity):
    flat_ids = routes.reshape(-1)
    one_hot = (flat_ids[:, None] == jnp.arange(experts, dtype=jnp.int32)[None, :])
    count = flat_ids.shape[0]
    before = jnp.arange(count)[:, None] > jnp.arange(count)[None, :]
    earlier = jnp.dot(
        before.astype(jnp.bfloat16), one_hot.astype(jnp.bfloat16), preferred_element_type=jnp.float32
    )
    ranked = jnp.sum(jnp.where(one_hot, earlier, 0.0), axis=1).astype(jnp.int32)
    return (flat_ids * capacity + ranked).reshape(routes.shape)


def contract_rows(left_side, right_side):
    return lax.dot_general(
        left_side, right_side, (((0,), (0,)), ((), ())), preferred_element_type=jnp.float32
    )


def contract_cols(left_side, right_side):
    return lax.dot_general(
        left_side, right_side, (((1,), (1,)), ((), ())), preferred_element_type=jnp.float32
    )


def per_device(
    moe_input,
    out_grad,
    routes,
    route_weights,
    gate_cols,
    up_cols,
    down_rows,
    out_proj,
    conv_out,
    gate_b,
    gate_c,
    hidden_h,
    conv_taps,
):
    seq_devices = lax.axis_size("sp")
    experts = seq_devices // 2
    tokens_here, model_width = moe_input.shape
    top_count = routes.shape[1]
    half_cap = 3 * tokens_here // seq_devices
    capacity = 2 * half_cap
    slot_count = experts * capacity
    n_tp = lax.axis_size("tp")
    positions = slot_choice(routes, experts, capacity)
    slots = jnp.arange(slot_count, dtype=jnp.int32)
    hits = slots[:, None, None] == positions[None]
    chosen = jnp.any(hits, axis=2).astype(jnp.bfloat16)
    slot_weight = jnp.sum(jnp.where(hits, route_weights[None], 0.0), axis=(1, 2))
    quarter = model_width // n_tp
    column_start = lax.axis_index("tp") * quarter
    source_x = lax.dynamic_slice_in_dim(moe_input, column_start, quarter, 1)
    source_g = lax.dynamic_slice_in_dim(out_grad, column_start, quarter, 1)
    sent_x = jnp.dot(chosen, source_x, preferred_element_type=jnp.float32).astype(jnp.bfloat16)
    sent_g = jnp.dot(chosen, source_g, preferred_element_type=jnp.float32)
    sent_g = (slot_weight[:, None] * sent_g).astype(jnp.bfloat16)
    branch = (gate_b.astype(jnp.float32) * conv_out.astype(jnp.float32)).astype(jnp.bfloat16)
    halo = 16
    aligned = model_width % (seq_devices * 128) == 0
    if aligned:
        own = lax.dynamic_slice_in_dim(
            chosen, (lax.axis_index("sp") // 2) * capacity, capacity, 0
        )
        own_weight = lax.dynamic_slice_in_dim(
            slot_weight, (lax.axis_index("sp") // 2) * capacity, capacity, 0
        )
        own_x = jnp.dot(own, moe_input, preferred_element_type=jnp.float32).astype(jnp.bfloat16)
        own_g = jnp.dot(own, out_grad, preferred_element_type=jnp.float32)
        own_g = (own_weight[:, None] * own_g).astype(jnp.bfloat16)
        returned, all_branch, next_gate_b, grad_gate, grad_up, grad_down = run_experts(
            sent_x.reshape(experts, capacity, quarter),
            sent_g.reshape(experts, capacity, quarter),
            own_x,
            own_g,
            branch,
            gate_b[:halo],
            gate_cols.T,
            up_cols.T,
            down_rows,
            seq_devices,
            n_tp,
        )
        returned = returned.reshape(slot_count, quarter)
        grad_gate, grad_up = grad_gate.T, grad_up.T
    else:
        rows_x, rows_g, all_branch, next_gate_b = dispatch(
            sent_x.reshape(experts, capacity, quarter),
            sent_g.reshape(experts, capacity, quarter),
            branch,
            gate_b[:halo],
            seq_devices,
            n_tp,
        )
        rows_x = rows_x.reshape(-1, model_width)
        rows_g = rows_g.reshape(-1, model_width)
        gate_pre = jnp.dot(rows_x, gate_cols, preferred_element_type=jnp.float32)
        up_pre = jnp.dot(rows_x, up_cols, preferred_element_type=jnp.float32)
        sigmoid_g = jax.nn.sigmoid(gate_pre)
        silu_g = gate_pre * sigmoid_g
        activation = (silu_g * up_pre).astype(jnp.bfloat16)
        grad_down = contract_rows(activation, rows_g).astype(jnp.bfloat16)
        d_act = contract_cols(rows_g, down_rows)
        d_up = (d_act * silu_g).astype(jnp.bfloat16)
        d_gate = (d_act * up_pre * sigmoid_g * (1.0 + gate_pre * (1.0 - sigmoid_g))).astype(
            jnp.bfloat16
        )
        grad_gate = contract_rows(rows_x, d_gate).astype(jnp.bfloat16)
        grad_up = contract_rows(rows_x, d_up).astype(jnp.bfloat16)
        partial_value = (contract_cols(d_gate, gate_cols) + contract_cols(d_up, up_cols)).astype(
            jnp.bfloat16
        )
        returned = give_back(
            partial_value.reshape(2, experts, capacity, model_width), seq_devices, n_tp
        ).reshape(slot_count, quarter)
    stream_part = (source_g.astype(jnp.float32) + contract_rows(chosen, returned)).astype(
        jnp.bfloat16
    )
    if aligned:
        stream, stream_block = share_stream(stream_part, halo, seq_devices, n_tp)
        grad_proj = contract_rows(
            stream_block.reshape(-1, stream_block.shape[2]),
            all_branch.reshape(-1, all_branch.shape[2]),
        )
    else:
        stream = lax.all_gather(stream_part, "tp", axis=1, tiled=True)
        grad_proj = lax.psum_scatter(
            contract_rows(stream, branch), "sp", scatter_dimension=0, tiled=True
        )
    d_branch = jnp.dot(stream, out_proj, preferred_element_type=jnp.float32)
    d_after = d_branch[tokens_here:]
    d_branch = d_branch[:tokens_here]
    grad_gate_b = (d_branch * conv_out.astype(jnp.float32)).astype(jnp.bfloat16)
    d_conv = d_branch * gate_b.astype(jnp.float32)
    kernel_taps = conv_taps.shape[0]
    kernel_reach = kernel_taps - 1
    if aligned:
        last = lax.axis_index("sp") == seq_devices - 1
        next_rows_in = jnp.where(last, 0.0, d_after * next_gate_b.astype(jnp.float32))[:kernel_reach]
    else:
        next_rows_in = from_behind(d_conv[:kernel_reach], "sp", -1)
    extended = jnp.concatenate([d_conv, next_rows_in], axis=0)
    d_input = jnp.zeros_like(d_conv)
    for tap_index in range(kernel_taps):
        offset = kernel_reach - tap_index
        d_input = d_input + conv_taps[tap_index][None, :] * extended[offset : offset + tokens_here]
    grad_hidden = (d_input * gate_c.astype(jnp.float32)).astype(jnp.bfloat16)
    grad_gate_c = (d_input * hidden_h.astype(jnp.float32)).astype(jnp.bfloat16)
    return (grad_gate, grad_up, grad_down, grad_proj, grad_hidden, grad_gate_b, grad_gate_c)


def solution(mesh):
    placed = (
        P("sp", None),
        P("sp", None),
        P("sp", None),
        P("sp", None),
        P(None, ("sp", "tp")),
        P(None, ("sp", "tp")),
        P(("sp", "tp"), None),
        P(None, "tp"),
        P("sp", "tp"),
        P("sp", "tp"),
        P("sp", "tp"),
        P("sp", "tp"),
        P(None, "tp"),
    )
    return jax.shard_map(
        per_device,
        mesh=mesh,
        in_specs=placed,
        out_specs=(
            P(None, ("sp", "tp")),
            P(None, ("sp", "tp")),
            P(("sp", "tp"), None),
            P("sp", "tp"),
            P("sp", "tp"),
            P("sp", "tp"),
            P("sp", "tp"),
        ),
        check_vma=False,
    )
```

```python
import functools

import jax
import jax.numpy as jnp
from jax import lax
from jax.experimental import pallas as pl
from jax.experimental.pallas import tpu as pltpu
from jax.sharding import PartitionSpec as P


def from_behind(block, axis, distance):
    devices = range(lax.axis_size(axis))
    route = [(i - distance, i) for i in devices if i - distance in devices]
    return lax.ppermute(block, axis, route)


MESH = pl.DeviceIdType.MESH
VMEM = pl.BlockSpec(memory_space=pltpu.VMEM)
ANY = pl.BlockSpec(memory_space=pl.ANY)


def columns(index, width):
    return pl.ds(pl.multiple_of(index * width, width), width)


def wait_arrival(ref, sem):
    pltpu.make_async_copy(ref, ref, sem).wait()


def greet(peers):
    barrier = pltpu.get_barrier_semaphore()
    for peer in peers:
        pl.semaphore_signal(barrier, inc=1, device_id=peer, device_id_type=MESH)
    pl.semaphore_wait(barrier, len(peers))


def place(n_tp):
    sp, tp = lax.axis_index("sp"), lax.axis_index("tp")
    expert, parity = sp // 2, lax.rem(sp, 2)
    row, core = tp // 2, lax.rem(tp, 2)
    return sp, tp, expert, parity, row, core


def dispatch_kernel(
    n_sp, n_tp, chunks,
    x_ref, g_ref, branch_ref, head_ref,
    out_x, out_g, out_b, out_head,
    z_send, z_recv, own_send, relay_send, near_recv, diag_recv, pair_send, pair_recv, b_send, b_recv, h_send, h_recv,
):
    experts = n_sp // 2
    sp, tp, expert, parity, row, core = place(n_tp)
    width = x_ref.shape[-1]
    size = experts // chunks
    x_side = (2 * expert + 1 - parity, tp)
    y_side = (sp, 2 * (1 - row) + core)
    pair = (sp, 2 * row + 1 - core)
    greet([(lax.rem(sp + d, n_sp), tp) for d in range(1, n_sp)] + [y_side, pair])
    started = []
    sources, outs = (x_ref, g_ref), (out_x, out_g)

    def spot(t, par, first, quarter, count):
        return outs[t].at[par, pl.ds(first, count), :, columns(quarter, width)]

    def send(src, device, send_sem, recv_sem):
        copy = pltpu.make_async_remote_copy(
            src_ref=src, dst_ref=src, send_sem=send_sem, recv_sem=recv_sem,
            device_id=device, device_id_type=MESH,
        )
        copy.start()
        started.append(copy)

    for t in range(2):
        for d in range(experts):
            target = lax.rem(expert + d, experts)
            src = sources[t].at[pl.ds(target, 1)]
            dst = spot(t, parity, expert, tp, 1)
            if d == 0:
                pltpu.make_async_copy(src, dst, z_recv.at[t, 0]).start()
                continue
            copy = pltpu.make_async_remote_copy(
                src_ref=src, dst_ref=dst, send_sem=z_send.at[t, d], recv_sem=z_recv.at[t, d],
                device_id=(2 * target + parity, tp), device_id_type=MESH,
            )
            copy.start()
            started.append(copy)
    for d in range(n_sp):
        dst = out_b.at[sp]
        if d == 0:
            pltpu.make_async_copy(branch_ref, dst, b_recv.at[0]).start()
            continue
        copy = pltpu.make_async_remote_copy(
            src_ref=branch_ref, dst_ref=dst, send_sem=b_send.at[d], recv_sem=b_recv.at[d],
            device_id=(lax.rem(sp + d, n_sp), tp), device_id_type=MESH,
        )
        copy.start()
        started.append(copy)

    copy = pltpu.make_async_remote_copy(
        src_ref=head_ref, dst_ref=out_head, send_sem=h_send.at[0], recv_sem=h_recv.at[0],
        device_id=(lax.rem(sp + n_sp - 1, n_sp), tp), device_id_type=MESH,
    )
    copy.start()
    started.append(copy)

    own_chunk = expert // size
    other_quarter = 2 * (1 - row) + core

    def first_of(k):
        return lax.rem(own_chunk + chunks - k, chunks) * size

    def own_stage(k, t):
        first = first_of(k)
        for i in range(size):
            source = first + i
            d = lax.rem(expert + experts - source, experts)
            wait_arrival(spot(t, parity, source, tp, 1), z_recv.at[t, d])
        block = spot(t, parity, first, tp, size)
        send(block, x_side, own_send.at[t, k, 0], near_recv.at[t, k, 0])
        send(block, y_side, own_send.at[t, k, 1], near_recv.at[t, k, 1])
        send(block, pair, pair_send.at[t, k, 0], pair_recv.at[t, k, 0])

    def near_stage(k, t):
        first = first_of(k)
        from_x = spot(t, 1 - parity, first, tp, size)
        from_y = spot(t, parity, first, other_quarter, size)
        wait_arrival(from_x, near_recv.at[t, k, 0])
        if (k + t) % 2 == 0:
            send(from_x, y_side, relay_send.at[t, k], diag_recv.at[t, k])
        send(from_x, pair, pair_send.at[t, k, 1], pair_recv.at[t, k, 1])
        wait_arrival(from_y, near_recv.at[t, k, 1])
        if (k + t) % 2 == 1:
            send(from_y, x_side, relay_send.at[t, k], diag_recv.at[t, k])
        send(from_y, pair, pair_send.at[t, k, 2], pair_recv.at[t, k, 2])

    def far_stage(k, t):
        block = spot(t, 1 - parity, first_of(k), other_quarter, size)
        wait_arrival(block, diag_recv.at[t, k])
        send(block, pair, pair_send.at[t, k, 3], pair_recv.at[t, k, 3])

    order = [0] + [k for n in range(1, chunks // 2 + 1) for k in dict.fromkeys((n, chunks - n))]
    steps = [(k, t) for k in order for t in range(2)]
    for n in range(len(steps) + 3):
        if n < len(steps):
            own_stage(*steps[n])
        if 1 <= n < len(steps) + 1:
            near_stage(*steps[n - 1])
        if 3 <= n < len(steps) + 3:
            far_stage(*steps[n - 3])
    for k, t in steps:
        first = first_of(k)
        quarters = (2 * row + 1 - core, 2 * (1 - row) + 1 - core)
        spots = ((parity, quarters[0]), (1 - parity, quarters[0]),
                 (parity, quarters[1]), (1 - parity, quarters[1]))
        for j, (par, quarter) in enumerate(spots):
            wait_arrival(spot(t, par, first, quarter, size), pair_recv.at[t, k, j])
    for d in range(n_sp):
        wait_arrival(out_b.at[lax.rem(sp + n_sp - d, n_sp)], b_recv.at[d])
    wait_arrival(out_head, h_recv.at[0])
    for copy in started:
        copy.wait_send()


def dispatch(x, g, branch, head, n_sp, n_tp):
    experts, capacity, width = x.shape
    chunks = min(experts, 4)
    dma = pltpu.SemaphoreType.DMA
    rows = jax.ShapeDtypeStruct((2, experts, capacity, width * n_tp), jnp.bfloat16)
    return pl.pallas_call(
        functools.partial(dispatch_kernel, n_sp, n_tp, chunks),
        out_shape=(
            rows, rows, jax.ShapeDtypeStruct((n_sp,) + branch.shape, branch.dtype),
            jax.ShapeDtypeStruct(head.shape, head.dtype),
        ),
        in_specs=[VMEM] * 4,
        out_specs=(VMEM,) * 4,
        scratch_shapes=[
            dma((2, experts)), dma((2, experts)), dma((2, chunks, 2)), dma((2, chunks)),
            dma((2, chunks, 2)), dma((2, chunks)), dma((2, chunks, 4)), dma((2, chunks, 4)),
            dma((n_sp,)), dma((n_sp,)), dma((1,)), dma((1,)),
        ],
        compiler_params=pltpu.CompilerParams(
            collective_id=0, has_side_effects=True, vmem_limit_bytes=48 * 1024 * 1024
        ),
    )(x, g, branch, head)


def return_kernel(
    n_sp, n_tp, chunks,
    part_ref, out_ref,
    from_pair, summed, from_chips, final,
    pair_send, pair_recv, chip_send, chip_recv, z_send, z_recv,
):
    experts = n_sp // 2
    sp, tp, expert, parity, row, core = place(n_tp)
    width = out_ref.shape[-1]
    pair = (sp, 2 * row + 1 - core)
    offsets = ((1, 1), (1, 0), (0, 1), (0, 0))

    def other(dp, dr):
        return lax.rem(parity + dp, 2), lax.rem(row + dr, 2)

    chips = [(2 * expert + other(dp, dr)[0], 2 * other(dp, dr)[1] + core) for dp, dr in offsets[:3]]
    along = [(2 * lax.rem(expert + d, experts) + parity, tp) for d in range(1, experts)]
    greet([pair] + chips + along)
    started, guarded = [], []

    def send(src, dst, send_sem, recv_sem, device):
        copy = pltpu.make_async_remote_copy(
            src_ref=src, dst_ref=dst, send_sem=send_sem, recv_sem=recv_sem,
            device_id=device, device_id_type=MESH,
        )
        copy.start()
        started.append(copy)

    size = experts // chunks
    own_chunk = expert // size
    order = [chunks // 2] if chunks > 1 else []
    order += [k for k in range(1, chunks) if k not in order] + [0]

    def first_of(k):
        return lax.rem(own_chunk + k, chunks) * size

    for k in order:
        part = pl.ds(first_of(k), size)
        for n, (dp, dr) in enumerate(offsets):
            par, line = other(dp, dr)
            src = part_ref.at[par, part, :, columns(2 * line + 1 - core, width)]
            send(src, from_pair.at[n, part], pair_send.at[n, k], pair_recv.at[n, k], pair)
    for k in order:
        first = first_of(k)
        part = pl.ds(first, size)
        for n, (dp, dr) in enumerate(offsets):
            par, line = other(dp, dr)
            wait_arrival(from_pair.at[n, part], pair_recv.at[n, k])
            for i in range(size):
                mine = part_ref[par, first + i, :, columns(2 * line + core, width)]
                total = mine.astype(jnp.float32) + from_pair[n, first + i].astype(jnp.float32)
                summed[n, first + i] = total.astype(jnp.bfloat16)
            if n < 3:
                send(summed.at[n, part], from_chips.at[n, part], chip_send.at[n, k],
                     chip_recv.at[n, k], chips[n])
    for k in order:
        first = first_of(k)
        part = pl.ds(first, size)
        for n in range(3):
            wait_arrival(from_chips.at[n, part], chip_recv.at[n, k])
        for i in range(size):
            target = first + i
            total = summed[3, target].astype(jnp.float32)
            for n in range(3):
                total = total + from_chips[n, target].astype(jnp.float32)
            final[target] = total.astype(jnp.bfloat16)
            away = target != expert
            copy = pltpu.make_async_remote_copy(
                src_ref=final.at[target], dst_ref=out_ref.at[expert],
                send_sem=z_send.at[target], recv_sem=z_recv.at[expert],
                device_id=(2 * target + parity, tp), device_id_type=MESH,
            )
            if size == 1 and k:
                copy.start()
                started.append(copy)
                continue
            if size == 1:
                out_ref[expert] = final[target]
                continue

            @pl.when(away)
            def _(copy=copy):
                copy.start()

            @pl.when(jnp.logical_not(away))
            def _():
                out_ref[expert] = final[expert]

            guarded.append((away, copy))
    for d in range(1, experts):
        source = lax.rem(expert + experts - d, experts)
        wait_arrival(out_ref.at[source], z_recv.at[source])
    for copy in started:
        copy.wait_send()
    for away, copy in guarded:
        pl.when(away)(copy.wait_send)


def give_back(part, n_sp, n_tp):
    _, experts, capacity, model_width = part.shape
    width = model_width // n_tp
    dma = pltpu.SemaphoreType.DMA
    block = (experts, capacity, width)
    chunks = min(experts, 4)
    return pl.pallas_call(
        functools.partial(return_kernel, n_sp, n_tp, chunks),
        out_shape=jax.ShapeDtypeStruct(block, jnp.bfloat16),
        in_specs=[VMEM],
        out_specs=VMEM,
        scratch_shapes=[
            pltpu.VMEM((4,) + block, jnp.bfloat16), pltpu.VMEM((4,) + block, jnp.bfloat16),
            pltpu.VMEM((3,) + block, jnp.bfloat16), pltpu.VMEM(block, jnp.bfloat16),
            dma((4, chunks)), dma((4, chunks)), dma((3, chunks)), dma((3, chunks)),
            dma((experts,)), dma((experts,)),
        ],
        compiler_params=pltpu.CompilerParams(
            collective_id=1, has_side_effects=True, vmem_limit_bytes=48 * 1024 * 1024
        ),
    )(part)


def dot(left, right, left_dim, right_dim):
    return lax.dot_general(
        left, right, (((left_dim,), (right_dim,)), ((), ())), preferred_element_type=jnp.float32
    )


def flipped(index, bits):
    bit = 1
    while bit <= bits:
        if bits & bit:
            index = index + bit - 2 * bit * lax.rem(index // bit, 2)
        bit *= 2
    return index


PLAN_CHUNKS = (1, 3, 2)
PLAN_OVER_X = (0, 4,)
PLAN = (
    ("depart", 1), ("cross", 0, 1), ("cross", 0, 0), ("depart", 2), ("own", 1), ("cross", 1, 1),
    ("depart", 0), ("depart", 3), ("own", 0), ("across", 0, 0), ("depart", 4), ("own", 2), ("near_y", 0),
    ("near_x", 1), ("near_x", 0), ("own", 3), ("across", 0, 1), ("depart", 5), ("near_y", 1),
    ("across", 1, 1), ("far", 1), ("near_x", 2), ("far", 0), ("own", 4), ("pre", 1), ("near_y", 2),
    ("near_x", 3), ("hidden", 1), ("far", 2), ("own", 5), ("pre", 0), ("near_x", 4), ("back", 1),
    ("near_y", 4), ("pre", 3), ("near_y", 3), ("cross", 1, 0), ("far", 3), ("near_x", 5), ("pair", 1),
    ("hidden", 3), ("far", 4), ("back", 3), ("pre", 2), ("near_y", 5), ("far", 5), ("pair", 3), ("hidden", 2),
    ("fold_x", 1), ("across", 1, 0), ("fold_y", 1), ("back", 2), ("fold_x", 3), ("fold_y", 3), ("pair", 2),
    ("home", 1), ("hidden", 0), ("back", 0), ("home", 3), ("fold_y", 2), ("fold_x", 2), ("grad", 6),
    ("pair", 0), ("grad", 5), ("grad", 8), ("home", 2), ("grad", 2), ("grad", 3), ("grad", 0), ("grad", 9),
    ("fold_x", 0), ("fold_y", 0), ("grad", 11), ("grad", 7), ("grad", 4), ("grad", 10), ("grad", 1),
    ("home", 0),
)


def expert_kernel(
    n_sp, n_tp,
    chosen_ref, weight_ref, token_x, token_g, gate_b, conv_out, gate_ref, up_ref, down_ref,
    stream_ref, block_ref, out_b, out_head, out_gate, out_up, out_down,
    sent_x, sent_g, out_back, part_ref,
    rows_x, rows_g, act, dup, dgt, part_out, part_mine, from_pair, summed,
    near_x, near_y, passed, far_x, far_y, final, wg, wu, wd, gate_pre, up_pre,
    w_sem, z_send, z_recv, own_send, own_recv, line_send, line_recv, relay_send, relay_recv,
    pair_send, pair_recv, own_pair_send, own_pair_recv, b_send, b_recv, h_send, h_recv,
    rp_send, rp_recv, near_send, near_recv, far_send, far_recv, back_send, back_recv,
    gather_send, gather_recv, halo_send, halo_recv, place_send, place_recv, held_send, held_recv,
):
    experts = n_sp // 2
    sp, tp, expert, parity, row, core = place(n_tp)
    capacity, width = sent_x.shape[1:]
    tokens, model_width = token_x.shape
    half = width // 2
    halo = out_head.shape[0]
    x_side = (2 * expert + 1 - parity, tp)
    y_side = (sp, 2 * (1 - row) + core)
    pair = (sp, 2 * row + 1 - core)
    other_quarter = 2 * (1 - row) + core
    sources, rows = (sent_x, sent_g), (rows_x, rows_g)
    started = []

    def send(src, dst, send_sem, recv_sem, device):
        copy = pltpu.make_async_remote_copy(
            src_ref=src, dst_ref=dst, send_sem=send_sem, recv_sem=recv_sem,
            device_id=device, device_id_type=MESH,
        )
        copy.start()
        started.append(copy)

    def spot(t, j, par, quarter):
        return rows[t].at[flipped(expert, j), par, :, columns(quarter, width)]

    loads = [
        pltpu.make_async_copy(src, dst, w_sem.at[n])
        for n, (src, dst) in enumerate(((gate_ref, wg), (up_ref, wu), (down_ref, wd)))
    ]
    for load in loads:
        load.start()
    before, after = lax.rem(sp + n_sp - 1, n_sp), lax.rem(sp + 1, n_sp)
    fixed = [x_side, y_side, pair] + [(2 * flipped(expert, j) + parity, tp) for j in PLAN_CHUNKS]
    fixed += [(near, (lax.rem(tp + n, n_tp))) for near in (before, after) for n in range(n_tp)]
    targets = [(2 * (core + 2 * h) + row, expert) for h in range(2)]
    origins = [(2 * tp + par, 2 * parity + lax.rem(expert, 2)) for par in range(2)]
    barrier = pltpu.get_barrier_semaphore()
    for peer in fixed:
        pl.semaphore_signal(barrier, inc=1, device_id=peer, device_id_type=MESH)
    expected = len(fixed)
    for peer in targets + origins:
        away = jnp.logical_or(peer[0] != sp, peer[1] != tp)

        @pl.when(away)
        def _(peer=peer):
            pl.semaphore_signal(barrier, inc=1, device_id=peer, device_id_type=MESH)

        expected = expected + away.astype(jnp.int32)
    out_b[parity, expert] = (
        gate_b[...].astype(jnp.float32) * conv_out[...].astype(jnp.float32)
    ).astype(jnp.bfloat16)
    slot_weight = jnp.sum(weight_ref[...], axis=2, keepdims=True)
    mine = columns(tp, width)
    one_hot = chosen_ref[...].reshape(experts * capacity, tokens)
    sent_x[...] = dot(one_hot, token_x[:, mine], 1, 0).astype(jnp.bfloat16).reshape(sent_x.shape)
    scaled = slot_weight * dot(one_hot, token_g[:, mine], 1, 0).reshape(sent_g.shape)
    sent_g[...] = scaled.astype(jnp.bfloat16)
    one_hot = chosen_ref[expert]
    slot_weight = jnp.sum(weight_ref[expert], axis=1, keepdims=True)
    rows_x[expert, parity] = dot(one_hot, token_x[...], 1, 0).astype(jnp.bfloat16)
    rows_g[expert, parity] = (slot_weight * dot(one_hot, token_g[...], 1, 0)).astype(jnp.bfloat16)
    pl.semaphore_wait(barrier, expected)
    steps = [(j, t) for j in PLAN_CHUNKS for t in range(2)]

    def depart(n):
        j, t = steps[n]
        target = flipped(expert, j)
        send(sources[t].at[target], rows[t].at[expert, parity, :, columns(tp, width)],
             z_send.at[t, j], z_recv.at[t, j], (2 * target + parity, tp))

    def piece(t, par, which, part):
        return rows[t].at[expert, par, :, columns(2 * which + part, width)]

    def cross(t, part):
        block = piece(t, parity, core, part)
        send(block, block, own_send.at[t, part], own_recv.at[t, part], x_side)

    def own_stage(n):
        j, t = steps[n]
        block = spot(t, j, parity, tp)
        wait_arrival(block, z_recv.at[t, j])
        send(block, block, line_send.at[t, j, 0], line_recv.at[t, j, 0], x_side)
        send(block, block, line_send.at[t, j, 1], line_recv.at[t, j, 1], y_side)
        send(block, block, pair_send.at[t, j, 0], pair_recv.at[t, j, 0], pair)

    def across_stage(t, part):
        block = piece(t, 1 - parity, core, part)
        wait_arrival(block, own_recv.at[t, part])
        send(block, block, own_pair_send.at[t, part], own_pair_recv.at[t, part], pair)

    def near_x_stage(n):
        j, t = steps[n]
        block = spot(t, j, 1 - parity, tp)
        wait_arrival(block, line_recv.at[t, j, 0])
        if n not in PLAN_OVER_X:
            send(block, block, relay_send.at[t, j], relay_recv.at[t, j], y_side)
        send(block, block, pair_send.at[t, j, 1], pair_recv.at[t, j, 1], pair)

    def near_y_stage(n):
        j, t = steps[n]
        block = spot(t, j, parity, other_quarter)
        wait_arrival(block, line_recv.at[t, j, 1])
        if n in PLAN_OVER_X:
            send(block, block, relay_send.at[t, j], relay_recv.at[t, j], x_side)
        send(block, block, pair_send.at[t, j, 2], pair_recv.at[t, j, 2], pair)

    def far_stage(n):
        j, t = steps[n]
        block = spot(t, j, 1 - parity, other_quarter)
        wait_arrival(block, relay_recv.at[t, j])
        send(block, block, pair_send.at[t, j, 3], pair_recv.at[t, j, 3], pair)

    def arrived(j, t):
        if j == 0:
            for part in range(2):
                wait_arrival(piece(t, 1 - parity, 1 - core, part), own_pair_recv.at[t, part])
            return
        quarters = (2 * row + 1 - core, 2 * (1 - row) + 1 - core)
        spots = ((parity, quarters[0]), (1 - parity, quarters[0]),
                 (parity, quarters[1]), (1 - parity, quarters[1]))
        for n, (par, quarter) in enumerate(spots):
            wait_arrival(spot(t, j, par, quarter), pair_recv.at[t, j, n])

    def pre_stage(j):
        arrived(j, 0)
        if waiting:
            for load in waiting:
                load.wait()
            waiting.clear()
        x = rows_x[flipped(expert, j)].reshape(2 * capacity, model_width)
        gate_pre[j] = dot(x, wg[...], 1, 1)
        up_pre[j] = dot(x, wu[...], 1, 1)

    def hidden_stage(j):
        arrived(j, 1)
        source = flipped(expert, j)
        g = rows_g[source].reshape(2 * capacity, model_width)
        d_act = dot(g, wd[...], 1, 1)
        gate, up = gate_pre[j], up_pre[j]
        s = jax.nn.sigmoid(gate)
        silu = gate * s
        act[source] = (silu * up).astype(jnp.bfloat16)
        dup[source] = (d_act * silu).astype(jnp.bfloat16)
        dgt[source] = (d_act * up * s * (1.0 + gate * (1.0 - s))).astype(jnp.bfloat16)

    def backward(j):
        source = flipped(expert, j)
        for kept in range(2):
            side_core = core if kept else 1 - core
            store = part_mine if kept else part_out
            for h in range(2):
                cols = columns(2 * h + side_core, width)
                value = (
                    dot(dgt[source], wg[:, cols], 1, 0) + dot(dup[source], wu[:, cols], 1, 0)
                ).astype(jnp.bfloat16)
                for par in range(2):
                    piece = value[par * capacity : (par + 1) * capacity]
                    store[j, h, par, 0] = piece[:, :half]
                    store[j, h, par, 1] = piece[:, half:]
            if not kept:
                send(part_out.at[j], from_pair.at[j], rp_send.at[j], rp_recv.at[j], pair)

    def reduce_pair(j):
        wait_arrival(from_pair.at[j], rp_recv.at[j])
        total = part_mine[j].astype(jnp.float32) + from_pair[j].astype(jnp.float32)
        summed[j] = total.astype(jnp.bfloat16)
        send(summed.at[j, 0, 1 - parity], near_x.at[j], near_send.at[j, 0], near_recv.at[j, 0], x_side)
        send(summed.at[j, 1, :, 1 - row], near_y.at[j], near_send.at[j, 1], near_recv.at[j, 1], y_side)

    def fold_x(j):
        wait_arrival(near_x.at[j], near_recv.at[j, 0])
        total = summed[j, 0, parity, 1 - row].astype(jnp.float32) + near_x[j, 1 - row].astype(jnp.float32)
        passed[j, 0] = total.astype(jnp.bfloat16)
        send(passed.at[j, 0], far_y.at[j], far_send.at[j, 0], far_recv.at[j, 0], y_side)

    def fold_y(j):
        wait_arrival(near_y.at[j], near_recv.at[j, 1])
        total = summed[j, 1, 1 - parity, row].astype(jnp.float32) + near_y[j, 1 - parity].astype(jnp.float32)
        passed[j, 1] = total.astype(jnp.bfloat16)
        send(passed.at[j, 1], far_x.at[j], far_send.at[j, 1], far_recv.at[j, 1], x_side)

    def reduce_far(j):
        wait_arrival(far_y.at[j], far_recv.at[j, 0])
        wait_arrival(far_x.at[j], far_recv.at[j, 1])
        left = summed[j, 0, parity, row].astype(jnp.float32) + near_x[j, row].astype(jnp.float32)
        left = (left + far_y[j].astype(jnp.float32)).astype(jnp.bfloat16)
        right = summed[j, 1, parity, row].astype(jnp.float32) + near_y[j, parity].astype(jnp.float32)
        right = (right + far_x[j].astype(jnp.float32)).astype(jnp.bfloat16)
        if j == 0:
            out_back[expert, :, :half] = left
            out_back[expert, :, half:] = right
            return
        final[j, :, :half] = left
        final[j, :, half:] = right
        target = flipped(expert, j)
        send(final.at[j], out_back.at[expert], back_send.at[j], back_recv.at[j], (2 * target + parity, tp))

    def weight_grad(n):
        out, left, right = (
            (out_down, act, rows_g), (out_gate, dgt, rows_x), (out_up, dup, rows_x)
        )[n // 4]
        tile = model_width // 4
        cols = slice(n % 4 * tile, (n % 4 + 1) * tile)
        lhs = left[...].reshape(-1, left.shape[-1])
        rhs = right[:, :, :, cols].reshape(-1, tile)
        out[:, cols] = dot(lhs, rhs, 0, 0).astype(jnp.bfloat16)

    def share_branch():
        block = out_b.at[parity, expert]
        for j in PLAN_CHUNKS:
            send(block, block, b_send.at[j], b_recv.at[j], (2 * flipped(expert, j) + parity, tp))
        send(gate_b.at[pl.ds(0, halo)], out_head, h_send.at[0], h_recv.at[0], (before, tp))

    stages = {
        "depart": depart, "cross": cross, "own": own_stage, "across": across_stage,
        "near_x": near_x_stage, "near_y": near_y_stage, "far": far_stage,
        "pre": pre_stage, "hidden": hidden_stage, "back": backward, "pair": reduce_pair,
        "fold_x": fold_x, "fold_y": fold_y, "home": reduce_far, "grad": weight_grad,
    }
    waiting = list(loads)
    owns = [n for n, stage in enumerate(PLAN) if stage[0] == "own"]
    for n, (name, *numbers) in enumerate(PLAN):
        stages[name](*numbers)
        if n == owns[-1]:
            share_branch()

    def block_columns(h, line, side_core):
        return columns(4 * h + 2 * side_core + line, half)

    for j in PLAN_CHUNKS:
        wait_arrival(out_b.at[parity, flipped(expert, j)], b_recv.at[j])
    send(out_b.at[parity], out_b.at[parity], b_send.at[0], b_recv.at[0], x_side)
    for j in PLAN_CHUNKS:
        wait_arrival(out_back.at[flipped(expert, j)], back_recv.at[j])
    one_hot = chosen_ref[...].reshape(experts * capacity, tokens)
    total = dot(one_hot, out_back[...].reshape(experts * capacity, width), 0, 0)
    guarded = []
    for h in range(2):
        cols = block_columns(h, row, core)
        base = token_g[:, cols].astype(jnp.float32)
        value = (base + total[:, h * half : (h + 1) * half]).astype(jnp.bfloat16)
        part_ref[h] = value
        stream_ref[pl.ds(0, tokens), cols] = value
    for h in range(2):
        src, dst, recv = part_ref.at[h], block_ref.at[parity, expert], place_recv.at[parity]
        away = jnp.logical_or(targets[h][0] != sp, targets[h][1] != tp)
        copy = pltpu.make_async_remote_copy(
            src_ref=src, dst_ref=dst, send_sem=place_send.at[h], recv_sem=recv,
            device_id=targets[h], device_id_type=MESH,
        )

        @pl.when(away)
        def _(copy=copy):
            copy.start()

        @pl.when(jnp.logical_not(away))
        def _(src=src, dst=dst, recv=recv):
            pltpu.make_async_copy(src, dst, recv).start()

        guarded.append((away, copy))
        cols = block_columns(h, row, core)
        dst = stream_ref.at[pl.ds(0, tokens), cols]
        send(src, dst, gather_send.at[h, 0], gather_recv.at[h, 0], y_side)
        send(src, dst, gather_send.at[h, 1], gather_recv.at[h, 1], pair)
        for n in range(n_tp):
            send(src.at[pl.ds(0, halo)], stream_ref.at[pl.ds(tokens, halo), cols],
                 halo_send.at[h, n], halo_recv.at[h, n], (before, lax.rem(tp + n, n_tp)))
    for h in range(2):
        block = stream_ref.at[pl.ds(0, tokens), block_columns(h, 1 - row, core)]
        wait_arrival(block, gather_recv.at[h, 0])
        send(block, block, gather_send.at[h, 2], gather_recv.at[h, 2], pair)
    for par in range(2):
        block = block_ref.at[par, tp]
        wait_arrival(block, place_recv.at[par])
        send(block, block, held_send.at[par, 0], held_recv.at[par, 0], y_side)
        send(block, block, held_send.at[par, 1], held_recv.at[par, 1], pair)
    for par in range(2):
        block = block_ref.at[par, other_quarter]
        wait_arrival(block, held_recv.at[par, 0])
        send(block, block, held_send.at[par, 2], held_recv.at[par, 2], pair)
    wait_arrival(out_b.at[1 - parity], b_recv.at[0])
    wait_arrival(out_head, h_recv.at[0])
    for h in range(2):
        for line, slot in ((row, 1), (1 - row, 2)):
            wait_arrival(
                stream_ref.at[pl.ds(0, tokens), block_columns(h, line, 1 - core)], gather_recv.at[h, slot]
            )
        for n in range(n_tp):
            source = lax.rem(tp + n_tp - n, n_tp)
            cols = block_columns(h, source // 2, lax.rem(source, 2))
            wait_arrival(stream_ref.at[pl.ds(tokens, halo), cols], halo_recv.at[h, n])
    for par in range(2):
        for line, slot in ((row, 1), (1 - row, 2)):
            wait_arrival(block_ref.at[par, 2 * line + 1 - core], held_recv.at[par, slot])
    for copy in started:
        copy.wait_send()
    for away, copy in guarded:
        pl.when(away)(copy.wait_send)


def run_experts(
    chosen, weight_of, token_x, token_g, gate_b, conv_out, wg, wu, wd, halo, n_sp, n_tp
):
    experts, capacity, tokens = chosen.shape
    model_width = token_x.shape[1]
    width = model_width // n_tp
    units = wg.shape[0]
    half = width // 2
    channels = gate_b.shape[1]
    dma = pltpu.SemaphoreType.DMA
    bf16 = jnp.bfloat16

    def vmem(*shape):
        return pltpu.VMEM(shape, bf16)

    rows = vmem(experts, 2, capacity, model_width)
    hidden = vmem(experts, 2 * capacity, units)
    blocks = vmem(experts, 2, 2, 2, capacity, half)
    near = vmem(experts, 2, capacity, half)
    far = vmem(experts, capacity, half)
    routed = vmem(experts, capacity, width)
    weight = vmem(units, model_width)
    pre = pltpu.VMEM((experts, 2 * capacity, units), jnp.float32)
    return pl.pallas_call(
        functools.partial(expert_kernel, n_sp, n_tp),
        out_shape=(
            vmem(tokens + halo, model_width), vmem(2, experts, tokens, half),
            vmem(2, experts, tokens, channels), vmem(halo, channels),
            weight, weight, weight,
        ),
        in_specs=[VMEM] * 6 + [ANY] * 3,
        out_specs=(VMEM,) * 7,
        scratch_shapes=[
            routed, routed, routed, vmem(2, tokens, half),
            rows, rows, hidden, hidden, hidden, blocks, blocks, blocks, blocks,
            near, near, near, far, far, routed,
            weight, weight, weight, pre, pre,
            dma((3,)), dma((2, experts)), dma((2, experts)), dma((2, 2)), dma((2, 2)),
            dma((2, experts, 2)), dma((2, experts, 2)), dma((2, experts)), dma((2, experts)),
            dma((2, experts, 4)), dma((2, experts, 4)), dma((2, 2)), dma((2, 2)),
            dma((experts,)), dma((experts,)), dma((1,)), dma((1,)),
            dma((experts,)), dma((experts,)), dma((experts, 2)), dma((experts, 2)),
            dma((experts, 2)), dma((experts, 2)), dma((experts,)), dma((experts,)),
            dma((2, 3)), dma((2, 3)), dma((2, n_tp)), dma((2, n_tp)),
            dma((2,)), dma((2,)), dma((2, 3)), dma((2, 3)),
        ],
        compiler_params=pltpu.CompilerParams(
            collective_id=3, has_side_effects=True, vmem_limit_bytes=48 * 1024 * 1024
        ),
    )(chosen, weight_of, token_x, token_g, gate_b, conv_out, wg, wu, wd)


def tail_kernel(
    n_sp, stream, blocks, branches, next_gate, out_proj, conv_out, gate_b, gate_c, hidden_h, taps,
    grad_gate, grad_up, grad_down,
    out_gate, out_up, out_down, out_p, out_hidden, out_gate_b, out_gate_c,
    extended, sems,
):
    tokens, channels = conv_out.shape
    moves = [
        pltpu.make_async_copy(src, dst, sems.at[n])
        for n, (src, dst) in enumerate(
            ((grad_gate, out_gate), (grad_up, out_up), (grad_down, out_down))
        )
    ]
    for move in moves:
        move.start()
    reach = taps.shape[0] - 1
    d_branch = dot(stream[...], out_proj[...], 1, 0)
    last = lax.axis_index("sp") == n_sp - 1
    following = jnp.where(last, 0.0, d_branch[tokens:] * next_gate[...].astype(jnp.float32))
    d_branch = d_branch[:tokens]
    out_gate_b[...] = (d_branch * conv_out[...].astype(jnp.float32)).astype(jnp.bfloat16)
    extended[pl.ds(0, tokens)] = d_branch * gate_b[...].astype(jnp.float32)
    extended[pl.ds(tokens, next_gate.shape[0])] = following
    d_input = jnp.zeros((tokens, channels), jnp.float32)
    for tap in range(reach + 1):
        d_input = d_input + taps[tap : tap + 1] * extended[pl.ds(reach - tap, tokens)]
    out_hidden[...] = (d_input * gate_c[...].astype(jnp.float32)).astype(jnp.bfloat16)
    out_gate_c[...] = (d_input * hidden_h[...].astype(jnp.float32)).astype(jnp.bfloat16)
    out_p[...] = dot(
        blocks[...].reshape(-1, blocks.shape[-1]), branches[...].reshape(-1, channels), 0, 0
    )
    for move in moves:
        move.wait()


def run_tail(stream, blocks, branches, next_gate, out_proj, conv_out, gate_b, gate_c, hidden_h, taps, grads, n_sp):
    tokens, channels = conv_out.shape
    halo = next_gate.shape[0]
    small = jax.ShapeDtypeStruct((tokens, channels), jnp.bfloat16)
    grad = jax.ShapeDtypeStruct(grads[0].shape, jnp.bfloat16)
    return pl.pallas_call(
        functools.partial(tail_kernel, n_sp),
        out_shape=(
            grad, grad, grad,
            jax.ShapeDtypeStruct((blocks.shape[-1], channels), jnp.float32), small, small, small,
        ),
        in_specs=[VMEM] * 13,
        out_specs=(ANY,) * 3 + (VMEM,) * 4,
        scratch_shapes=[
            pltpu.VMEM((tokens + halo, channels), jnp.float32), pltpu.SemaphoreType.DMA((3,)),
        ],
        compiler_params=pltpu.CompilerParams(vmem_limit_bytes=24 * 1024 * 1024),
    )(stream, blocks, branches, next_gate, out_proj, conv_out, gate_b, gate_c, hidden_h, taps, *grads)


def stream_kernel(
    n_sp, n_tp, part_ref, stream_ref, block_ref,
    tp_send, tp_recv, h_send, h_recv, b_send, b_recv, s_send, s_recv,
):
    sp, tp = lax.axis_index("sp"), lax.axis_index("tp")
    tokens, width = part_ref.shape
    block = block_ref.shape[2]
    halo = stream_ref.shape[0] - tokens
    per_part, per_peer = width // block, n_sp // n_tp
    greet([
        (lax.rem(sp + i, n_sp), lax.rem(tp + j, n_tp))
        for i in range(n_sp) for j in range(n_tp) if i or j
    ])
    started = []

    def send(src, dst, send_sem, recv_sem, device):
        copy = pltpu.make_async_remote_copy(
            src_ref=src, dst_ref=dst, send_sem=send_sem, recv_sem=recv_sem,
            device_id=device, device_id_type=MESH,
        )
        copy.start()
        started.append((None, copy))

    keeper = sp // per_peer
    for b in range(per_part):
        target = tp * per_part + b
        src = part_ref.at[:, b * block : (b + 1) * block]
        dst = block_ref.at[sp]
        away = jnp.logical_or(target != sp, keeper != tp)
        copy = pltpu.make_async_remote_copy(
            src_ref=src, dst_ref=dst, send_sem=b_send.at[b], recv_sem=b_recv.at[lax.rem(sp, per_peer)],
            device_id=(target, keeper), device_id_type=MESH,
        )

        @pl.when(away)
        def _(copy=copy):
            copy.start()

        @pl.when(jnp.logical_not(away))
        def _(src=src, dst=dst):
            pltpu.make_async_copy(src, dst, b_recv.at[lax.rem(sp, per_peer)]).start()

        started.append((away, copy))
    mine = stream_ref.at[pl.ds(0, tokens), columns(tp, width)]
    edge = stream_ref.at[pl.ds(tokens, halo), columns(tp, width)]
    before = lax.rem(sp + n_sp - 1, n_sp)
    pltpu.make_async_copy(part_ref, mine, tp_recv.at[0]).start()
    for j in range(n_tp):
        peer = lax.rem(tp + j, n_tp)
        if j:
            send(part_ref, mine, tp_send.at[j], tp_recv.at[j], (sp, peer))
        send(part_ref.at[pl.ds(0, halo)], edge, h_send.at[j], h_recv.at[j], (before, peer))
    for n in range(per_peer):
        held = block_ref.at[tp * per_peer + n]
        wait_arrival(held, b_recv.at[n])
        for j in range(1, n_tp):
            send(held, held, s_send.at[n, j], s_recv.at[n, j], (sp, lax.rem(tp + j, n_tp)))
    for j in range(n_tp):
        source = lax.rem(tp + n_tp - j, n_tp)
        wait_arrival(stream_ref.at[pl.ds(0, tokens), columns(source, width)], tp_recv.at[j])
        wait_arrival(stream_ref.at[pl.ds(tokens, halo), columns(source, width)], h_recv.at[j])
        for n in range(per_peer):
            if j:
                wait_arrival(block_ref.at[source * per_peer + n], s_recv.at[n, j])
    for away, copy in started:
        if away is None:
            copy.wait_send()
        else:
            pl.when(away)(copy.wait_send)


def share_stream(part, halo, n_sp, n_tp):
    tokens, width = part.shape
    dma = pltpu.SemaphoreType.DMA
    block = width * n_tp // n_sp
    per_peer = n_sp // n_tp
    return pl.pallas_call(
        functools.partial(stream_kernel, n_sp, n_tp),
        out_shape=(
            jax.ShapeDtypeStruct((tokens + halo, width * n_tp), jnp.bfloat16),
            jax.ShapeDtypeStruct((n_sp, tokens, block), jnp.bfloat16),
        ),
        in_specs=[VMEM],
        out_specs=(VMEM, VMEM),
        scratch_shapes=[
            dma((n_tp,)), dma((n_tp,)), dma((n_tp,)), dma((n_tp,)),
            dma((width // block,)), dma((per_peer,)), dma((per_peer, n_tp)), dma((per_peer, n_tp)),
        ],
        compiler_params=pltpu.CompilerParams(collective_id=2, has_side_effects=True),
    )(part)


def slot_choice(routes, experts, capacity):
    flat_ids = routes.reshape(-1)
    one_hot = (flat_ids[:, None] == jnp.arange(experts, dtype=jnp.int32)[None, :])
    count = flat_ids.shape[0]
    before = jnp.arange(count)[:, None] > jnp.arange(count)[None, :]
    earlier = jnp.dot(
        before.astype(jnp.bfloat16), one_hot.astype(jnp.bfloat16), preferred_element_type=jnp.float32
    )
    ranked = jnp.sum(jnp.where(one_hot, earlier, 0.0), axis=1).astype(jnp.int32)
    return (flat_ids * capacity + ranked).reshape(routes.shape)


def contract_rows(left_side, right_side):
    return lax.dot_general(
        left_side, right_side, (((0,), (0,)), ((), ())), preferred_element_type=jnp.float32
    )


def contract_cols(left_side, right_side):
    return lax.dot_general(
        left_side, right_side, (((1,), (1,)), ((), ())), preferred_element_type=jnp.float32
    )


def per_device(
    moe_input,
    out_grad,
    routes,
    route_weights,
    gate_cols,
    up_cols,
    down_rows,
    out_proj,
    conv_out,
    gate_b,
    gate_c,
    hidden_h,
    conv_taps,
):
    seq_devices = lax.axis_size("sp")
    experts = seq_devices // 2
    tokens_here, model_width = moe_input.shape
    top_count = routes.shape[1]
    half_cap = 3 * tokens_here // seq_devices
    capacity = 2 * half_cap
    slot_count = experts * capacity
    n_tp = lax.axis_size("tp")
    positions = slot_choice(routes, experts, capacity)
    slots = jnp.arange(slot_count, dtype=jnp.int32)
    hits = slots[:, None, None] == positions[None]
    chosen = jnp.any(hits, axis=2).astype(jnp.bfloat16)
    halo = 16
    aligned = model_width % (seq_devices * 128) == 0
    planned = aligned and experts == len(PLAN_CHUNKS) + 1 and n_tp == experts
    if planned:
        weight_of = jnp.sum(jnp.where(hits, route_weights[None], 0.0), axis=2)
        stream, blocks, branches, next_gate, *grads = run_experts(
            chosen.reshape(experts, capacity, tokens_here),
            weight_of.reshape(experts, capacity, tokens_here),
            moe_input, out_grad, gate_b, conv_out, gate_cols.T, up_cols.T, down_rows,
            halo, seq_devices, n_tp,
        )
        grad_gate, grad_up, *rest = run_tail(
            stream, blocks, branches, next_gate, out_proj, conv_out, gate_b, gate_c, hidden_h,
            conv_taps, grads, seq_devices,
        )
        return (grad_gate.T, grad_up.T, *rest[:2], rest[2], rest[3], rest[4])
    slot_weight = jnp.sum(jnp.where(hits, route_weights[None], 0.0), axis=(1, 2))
    quarter = model_width // n_tp
    column_start = lax.axis_index("tp") * quarter
    source_x = lax.dynamic_slice_in_dim(moe_input, column_start, quarter, 1)
    source_g = lax.dynamic_slice_in_dim(out_grad, column_start, quarter, 1)
    sent_x = jnp.dot(chosen, source_x, preferred_element_type=jnp.float32).astype(jnp.bfloat16)
    sent_g = jnp.dot(chosen, source_g, preferred_element_type=jnp.float32)
    sent_g = (slot_weight[:, None] * sent_g).astype(jnp.bfloat16)
    branch = (gate_b.astype(jnp.float32) * conv_out.astype(jnp.float32)).astype(jnp.bfloat16)
    rows_x, rows_g, all_branch, next_gate_b = dispatch(
        sent_x.reshape(experts, capacity, quarter),
        sent_g.reshape(experts, capacity, quarter),
        branch,
        gate_b[:halo],
        seq_devices,
        n_tp,
    )
    rows_x = rows_x.reshape(-1, model_width)
    rows_g = rows_g.reshape(-1, model_width)
    gate_pre = jnp.dot(rows_x, gate_cols, preferred_element_type=jnp.float32)
    up_pre = jnp.dot(rows_x, up_cols, preferred_element_type=jnp.float32)
    sigmoid_g = jax.nn.sigmoid(gate_pre)
    silu_g = gate_pre * sigmoid_g
    activation = (silu_g * up_pre).astype(jnp.bfloat16)
    grad_down = contract_rows(activation, rows_g).astype(jnp.bfloat16)
    d_act = contract_cols(rows_g, down_rows)
    d_up = (d_act * silu_g).astype(jnp.bfloat16)
    d_gate = (d_act * up_pre * sigmoid_g * (1.0 + gate_pre * (1.0 - sigmoid_g))).astype(
        jnp.bfloat16
    )
    grad_gate = contract_rows(rows_x, d_gate).astype(jnp.bfloat16)
    grad_up = contract_rows(rows_x, d_up).astype(jnp.bfloat16)
    partial_value = (contract_cols(d_gate, gate_cols) + contract_cols(d_up, up_cols)).astype(
        jnp.bfloat16
    )
    returned = give_back(
        partial_value.reshape(2, experts, capacity, model_width), seq_devices, n_tp
    ).reshape(slot_count, quarter)
    stream_part = (source_g.astype(jnp.float32) + contract_rows(chosen, returned)).astype(
        jnp.bfloat16
    )
    if aligned:
        stream, stream_block = share_stream(stream_part, halo, seq_devices, n_tp)
        grad_proj = contract_rows(
            stream_block.reshape(-1, stream_block.shape[2]),
            all_branch.reshape(-1, all_branch.shape[2]),
        )
    else:
        stream = lax.all_gather(stream_part, "tp", axis=1, tiled=True)
        grad_proj = lax.psum_scatter(
            contract_rows(stream, branch), "sp", scatter_dimension=0, tiled=True
        )
    d_branch = jnp.dot(stream, out_proj, preferred_element_type=jnp.float32)
    d_after = d_branch[tokens_here:]
    d_branch = d_branch[:tokens_here]
    grad_gate_b = (d_branch * conv_out.astype(jnp.float32)).astype(jnp.bfloat16)
    d_conv = d_branch * gate_b.astype(jnp.float32)
    kernel_taps = conv_taps.shape[0]
    kernel_reach = kernel_taps - 1
    if aligned:
        last = lax.axis_index("sp") == seq_devices - 1
        next_rows_in = jnp.where(last, 0.0, d_after * next_gate_b.astype(jnp.float32))[:kernel_reach]
    else:
        next_rows_in = from_behind(d_conv[:kernel_reach], "sp", -1)
    extended = jnp.concatenate([d_conv, next_rows_in], axis=0)
    d_input = jnp.zeros_like(d_conv)
    for tap_index in range(kernel_taps):
        offset = kernel_reach - tap_index
        d_input = d_input + conv_taps[tap_index][None, :] * extended[offset : offset + tokens_here]
    grad_hidden = (d_input * gate_c.astype(jnp.float32)).astype(jnp.bfloat16)
    grad_gate_c = (d_input * hidden_h.astype(jnp.float32)).astype(jnp.bfloat16)
    return (grad_gate, grad_up, grad_down, grad_proj, grad_hidden, grad_gate_b, grad_gate_c)


def solution(mesh):
    placed = (
        P("sp", None),
        P("sp", None),
        P("sp", None),
        P("sp", None),
        P(None, ("sp", "tp")),
        P(None, ("sp", "tp")),
        P(("sp", "tp"), None),
        P(None, "tp"),
        P("sp", "tp"),
        P("sp", "tp"),
        P("sp", "tp"),
        P("sp", "tp"),
        P(None, "tp"),
    )
    return jax.shard_map(
        per_device,
        mesh=mesh,
        in_specs=placed,
        out_specs=(
            P(None, ("sp", "tp")),
            P(None, ("sp", "tp")),
            P(("sp", "tp"), None),
            P("sp", "tp"),
            P("sp", "tp"),
            P("sp", "tp"),
            P("sp", "tp"),
        ),
        check_vma=False,
    )
```

```python
import functools

import jax
import jax.numpy as jnp
from jax import lax
from jax.experimental import pallas as pl
from jax.experimental.pallas import tpu as pltpu
from jax.sharding import PartitionSpec as P


def from_behind(block, axis, distance):
    devices = range(lax.axis_size(axis))
    route = [(i - distance, i) for i in devices if i - distance in devices]
    return lax.ppermute(block, axis, route)


MESH = pl.DeviceIdType.MESH
VMEM = pl.BlockSpec(memory_space=pltpu.VMEM)
HBM = pl.BlockSpec(memory_space=pltpu.HBM)


def columns(index, width):
    return pl.ds(pl.multiple_of(index * width, width), width)


def wait_arrival(ref, sem):
    pltpu.make_async_copy(ref, ref, sem).wait()


def greet(peers):
    barrier = pltpu.get_barrier_semaphore()
    for peer in peers:
        pl.semaphore_signal(barrier, inc=1, device_id=peer, device_id_type=MESH)
    pl.semaphore_wait(barrier, len(peers))


def place(n_tp):
    sp, tp = lax.axis_index("sp"), lax.axis_index("tp")
    expert, parity = sp // 2, lax.rem(sp, 2)
    row, core = tp // 2, lax.rem(tp, 2)
    return sp, tp, expert, parity, row, core


def dispatch_kernel(
    n_sp, n_tp, chunks,
    x_ref, g_ref, branch_ref, head_ref,
    out_x, out_g, out_b, out_head,
    z_send, z_recv, own_send, relay_send, near_recv, diag_recv, pair_send, pair_recv, b_send, b_recv, h_send, h_recv,
):
    experts = n_sp // 2
    sp, tp, expert, parity, row, core = place(n_tp)
    width = x_ref.shape[-1]
    size = experts // chunks
    x_side = (2 * expert + 1 - parity, tp)
    y_side = (sp, 2 * (1 - row) + core)
    pair = (sp, 2 * row + 1 - core)
    greet([(lax.rem(sp + d, n_sp), tp) for d in range(1, n_sp)] + [y_side, pair])
    started = []
    sources, outs = (x_ref, g_ref), (out_x, out_g)

    def spot(t, par, first, quarter, count):
        return outs[t].at[par, pl.ds(first, count), :, columns(quarter, width)]

    def send(src, device, send_sem, recv_sem):
        copy = pltpu.make_async_remote_copy(
            src_ref=src, dst_ref=src, send_sem=send_sem, recv_sem=recv_sem,
            device_id=device, device_id_type=MESH,
        )
        copy.start()
        started.append(copy)

    for t in range(2):
        for d in range(experts):
            target = lax.rem(expert + d, experts)
            src = sources[t].at[pl.ds(target, 1)]
            dst = spot(t, parity, expert, tp, 1)
            if d == 0:
                pltpu.make_async_copy(src, dst, z_recv.at[t, 0]).start()
                continue
            copy = pltpu.make_async_remote_copy(
                src_ref=src, dst_ref=dst, send_sem=z_send.at[t, d], recv_sem=z_recv.at[t, d],
                device_id=(2 * target + parity, tp), device_id_type=MESH,
            )
            copy.start()
            started.append(copy)
    for d in range(n_sp):
        dst = out_b.at[sp]
        if d == 0:
            pltpu.make_async_copy(branch_ref, dst, b_recv.at[0]).start()
            continue
        copy = pltpu.make_async_remote_copy(
            src_ref=branch_ref, dst_ref=dst, send_sem=b_send.at[d], recv_sem=b_recv.at[d],
            device_id=(lax.rem(sp + d, n_sp), tp), device_id_type=MESH,
        )
        copy.start()
        started.append(copy)

    copy = pltpu.make_async_remote_copy(
        src_ref=head_ref, dst_ref=out_head, send_sem=h_send.at[0], recv_sem=h_recv.at[0],
        device_id=(lax.rem(sp + n_sp - 1, n_sp), tp), device_id_type=MESH,
    )
    copy.start()
    started.append(copy)

    own_chunk = expert // size
    other_quarter = 2 * (1 - row) + core

    def first_of(k):
        return lax.rem(own_chunk + chunks - k, chunks) * size

    def own_stage(k, t):
        first = first_of(k)
        for i in range(size):
            source = first + i
            d = lax.rem(expert + experts - source, experts)
            wait_arrival(spot(t, parity, source, tp, 1), z_recv.at[t, d])
        block = spot(t, parity, first, tp, size)
        send(block, x_side, own_send.at[t, k, 0], near_recv.at[t, k, 0])
        send(block, y_side, own_send.at[t, k, 1], near_recv.at[t, k, 1])
        send(block, pair, pair_send.at[t, k, 0], pair_recv.at[t, k, 0])

    def near_stage(k, t):
        first = first_of(k)
        from_x = spot(t, 1 - parity, first, tp, size)
        from_y = spot(t, parity, first, other_quarter, size)
        wait_arrival(from_x, near_recv.at[t, k, 0])
        if (k + t) % 2 == 0:
            send(from_x, y_side, relay_send.at[t, k], diag_recv.at[t, k])
        send(from_x, pair, pair_send.at[t, k, 1], pair_recv.at[t, k, 1])
        wait_arrival(from_y, near_recv.at[t, k, 1])
        if (k + t) % 2 == 1:
            send(from_y, x_side, relay_send.at[t, k], diag_recv.at[t, k])
        send(from_y, pair, pair_send.at[t, k, 2], pair_recv.at[t, k, 2])

    def far_stage(k, t):
        block = spot(t, 1 - parity, first_of(k), other_quarter, size)
        wait_arrival(block, diag_recv.at[t, k])
        send(block, pair, pair_send.at[t, k, 3], pair_recv.at[t, k, 3])

    order = [0] + [k for n in range(1, chunks // 2 + 1) for k in dict.fromkeys((n, chunks - n))]
    steps = [(k, t) for k in order for t in range(2)]
    for n in range(len(steps) + 3):
        if n < len(steps):
            own_stage(*steps[n])
        if 1 <= n < len(steps) + 1:
            near_stage(*steps[n - 1])
        if 3 <= n < len(steps) + 3:
            far_stage(*steps[n - 3])
    for k, t in steps:
        first = first_of(k)
        quarters = (2 * row + 1 - core, 2 * (1 - row) + 1 - core)
        spots = ((parity, quarters[0]), (1 - parity, quarters[0]),
                 (parity, quarters[1]), (1 - parity, quarters[1]))
        for j, (par, quarter) in enumerate(spots):
            wait_arrival(spot(t, par, first, quarter, size), pair_recv.at[t, k, j])
    for d in range(n_sp):
        wait_arrival(out_b.at[lax.rem(sp + n_sp - d, n_sp)], b_recv.at[d])
    wait_arrival(out_head, h_recv.at[0])
    for copy in started:
        copy.wait_send()


def dispatch(x, g, branch, head, n_sp, n_tp):
    experts, capacity, width = x.shape
    chunks = min(experts, 4)
    dma = pltpu.SemaphoreType.DMA
    rows = jax.ShapeDtypeStruct((2, experts, capacity, width * n_tp), jnp.bfloat16)
    return pl.pallas_call(
        functools.partial(dispatch_kernel, n_sp, n_tp, chunks),
        out_shape=(
            rows, rows, jax.ShapeDtypeStruct((n_sp,) + branch.shape, branch.dtype),
            jax.ShapeDtypeStruct(head.shape, head.dtype),
        ),
        in_specs=[VMEM] * 4,
        out_specs=(VMEM,) * 4,
        scratch_shapes=[
            dma((2, experts)), dma((2, experts)), dma((2, chunks, 2)), dma((2, chunks)),
            dma((2, chunks, 2)), dma((2, chunks)), dma((2, chunks, 4)), dma((2, chunks, 4)),
            dma((n_sp,)), dma((n_sp,)), dma((1,)), dma((1,)),
        ],
        compiler_params=pltpu.CompilerParams(
            collective_id=0, has_side_effects=True, vmem_limit_bytes=48 * 1024 * 1024
        ),
    )(x, g, branch, head)


def return_kernel(
    n_sp, n_tp, chunks,
    part_ref, out_ref,
    from_pair, summed, from_chips, final,
    pair_send, pair_recv, chip_send, chip_recv, z_send, z_recv,
):
    experts = n_sp // 2
    sp, tp, expert, parity, row, core = place(n_tp)
    width = out_ref.shape[-1]
    pair = (sp, 2 * row + 1 - core)
    offsets = ((1, 1), (1, 0), (0, 1), (0, 0))

    def other(dp, dr):
        return lax.rem(parity + dp, 2), lax.rem(row + dr, 2)

    chips = [(2 * expert + other(dp, dr)[0], 2 * other(dp, dr)[1] + core) for dp, dr in offsets[:3]]
    along = [(2 * lax.rem(expert + d, experts) + parity, tp) for d in range(1, experts)]
    greet([pair] + chips + along)
    started, guarded = [], []

    def send(src, dst, send_sem, recv_sem, device):
        copy = pltpu.make_async_remote_copy(
            src_ref=src, dst_ref=dst, send_sem=send_sem, recv_sem=recv_sem,
            device_id=device, device_id_type=MESH,
        )
        copy.start()
        started.append(copy)

    size = experts // chunks
    own_chunk = expert // size
    order = [chunks // 2] if chunks > 1 else []
    order += [k for k in range(1, chunks) if k not in order] + [0]

    def first_of(k):
        return lax.rem(own_chunk + k, chunks) * size

    for k in order:
        part = pl.ds(first_of(k), size)
        for n, (dp, dr) in enumerate(offsets):
            par, line = other(dp, dr)
            src = part_ref.at[par, part, :, columns(2 * line + 1 - core, width)]
            send(src, from_pair.at[n, part], pair_send.at[n, k], pair_recv.at[n, k], pair)
    for k in order:
        first = first_of(k)
        part = pl.ds(first, size)
        for n, (dp, dr) in enumerate(offsets):
            par, line = other(dp, dr)
            wait_arrival(from_pair.at[n, part], pair_recv.at[n, k])
            for i in range(size):
                mine = part_ref[par, first + i, :, columns(2 * line + core, width)]
                total = mine.astype(jnp.float32) + from_pair[n, first + i].astype(jnp.float32)
                summed[n, first + i] = total.astype(jnp.bfloat16)
            if n < 3:
                send(summed.at[n, part], from_chips.at[n, part], chip_send.at[n, k],
                     chip_recv.at[n, k], chips[n])
    for k in order:
        first = first_of(k)
        part = pl.ds(first, size)
        for n in range(3):
            wait_arrival(from_chips.at[n, part], chip_recv.at[n, k])
        for i in range(size):
            target = first + i
            total = summed[3, target].astype(jnp.float32)
            for n in range(3):
                total = total + from_chips[n, target].astype(jnp.float32)
            final[target] = total.astype(jnp.bfloat16)
            away = target != expert
            copy = pltpu.make_async_remote_copy(
                src_ref=final.at[target], dst_ref=out_ref.at[expert],
                send_sem=z_send.at[target], recv_sem=z_recv.at[expert],
                device_id=(2 * target + parity, tp), device_id_type=MESH,
            )
            if size == 1 and k:
                copy.start()
                started.append(copy)
                continue
            if size == 1:
                out_ref[expert] = final[target]
                continue

            @pl.when(away)
            def _(copy=copy):
                copy.start()

            @pl.when(jnp.logical_not(away))
            def _():
                out_ref[expert] = final[expert]

            guarded.append((away, copy))
    for d in range(1, experts):
        source = lax.rem(expert + experts - d, experts)
        wait_arrival(out_ref.at[source], z_recv.at[source])
    for copy in started:
        copy.wait_send()
    for away, copy in guarded:
        pl.when(away)(copy.wait_send)


def give_back(part, n_sp, n_tp):
    _, experts, capacity, model_width = part.shape
    width = model_width // n_tp
    dma = pltpu.SemaphoreType.DMA
    block = (experts, capacity, width)
    chunks = min(experts, 4)
    return pl.pallas_call(
        functools.partial(return_kernel, n_sp, n_tp, chunks),
        out_shape=jax.ShapeDtypeStruct(block, jnp.bfloat16),
        in_specs=[VMEM],
        out_specs=VMEM,
        scratch_shapes=[
            pltpu.VMEM((4,) + block, jnp.bfloat16), pltpu.VMEM((4,) + block, jnp.bfloat16),
            pltpu.VMEM((3,) + block, jnp.bfloat16), pltpu.VMEM(block, jnp.bfloat16),
            dma((4, chunks)), dma((4, chunks)), dma((3, chunks)), dma((3, chunks)),
            dma((experts,)), dma((experts,)),
        ],
        compiler_params=pltpu.CompilerParams(
            collective_id=1, has_side_effects=True, vmem_limit_bytes=48 * 1024 * 1024
        ),
    )(part)


def dot(left, right, left_dim, right_dim):
    return lax.dot_general(
        left, right, (((left_dim,), (right_dim,)), ((), ())), preferred_element_type=jnp.float32
    )


def flipped(index, bits):
    bit = 1
    while bit <= bits:
        if bits & bit:
            index = index + bit - 2 * bit * lax.rem(index // bit, 2)
        bit *= 2
    return index


PLAN_CHUNKS = (1, 3, 2)
PLAN_OVER_X = (0, 4,)
PLAN = (
    ("depart", 1), ("cross", 0, 1), ("cross", 0, 0), ("depart", 2), ("own", 1), ("cross", 1, 1),
    ("depart", 0), ("depart", 3), ("own", 0), ("across", 0, 0), ("depart", 4), ("own", 2), ("near_y", 0),
    ("near_x", 1), ("near_x", 0), ("own", 3), ("across", 0, 1), ("depart", 5), ("near_y", 1),
    ("across", 1, 1), ("far", 1), ("near_x", 2), ("far", 0), ("own", 4), ("pre", 1), ("near_y", 2),
    ("near_x", 3), ("hidden", 1), ("far", 2), ("own", 5), ("pre", 0), ("near_x", 4), ("back", 1),
    ("near_y", 4), ("pre", 3), ("near_y", 3), ("cross", 1, 0), ("far", 3), ("near_x", 5), ("pair", 1),
    ("hidden", 3), ("far", 4), ("back", 3), ("pre", 2), ("near_y", 5), ("far", 5), ("pair", 3), ("hidden", 2),
    ("fold_x", 1), ("across", 1, 0), ("fold_y", 1), ("back", 2), ("fold_x", 3), ("fold_y", 3), ("pair", 2),
    ("home", 1), ("hidden", 0), ("back", 0), ("home", 3), ("fold_y", 2), ("fold_x", 2), ("grad", 6),
    ("pair", 0), ("grad", 5), ("grad", 8), ("home", 2), ("grad", 2), ("grad", 3), ("grad", 0), ("grad", 9),
    ("fold_x", 0), ("fold_y", 0), ("grad", 11), ("grad", 7), ("grad", 4), ("grad", 10), ("grad", 1),
    ("home", 0),
)


def expert_kernel(
    n_sp, n_tp, *refs,
):
    hbm, refs = refs[:13], refs[13:]
    out_gate, out_up, out_down, out_proj_grad, out_hidden, out_gate_b, out_gate_c = refs[:7]
    vmem, refs = refs[7:20], refs[20:]
    routes, route_weights, token_x, token_g, gate_b, conv_out, *vmem_rest = vmem
    gate_c, hidden_h, wg, wu, wd, out_proj, taps = vmem_rest
    (
        stream_ref, block_ref, out_b, out_head, chosen_ref, weight_ref, extended,
        sent_x, sent_g, out_back, part_ref,
        rows_x, rows_g, act, dup, dgt, part_out, part_mine, from_pair, summed,
        near_x, near_y, passed, far_x, far_y, final, gate_pre, up_pre,
        load_sem, z_send, z_recv, own_send, own_recv, line_send, line_recv, relay_send, relay_recv,
        pair_send, pair_recv, own_pair_send, own_pair_recv, b_send, b_recv, h_send, h_recv,
        rp_send, rp_recv, near_send, near_recv, far_send, far_recv, back_send, back_recv,
        gather_send, gather_recv, halo_send, halo_recv, place_send, place_recv, held_send, held_recv,
    ) = refs
    experts = n_sp // 2
    sp, tp, expert, parity, row, core = place(n_tp)
    capacity, width = sent_x.shape[1:]
    tokens, model_width = token_x.shape
    half = width // 2
    halo = out_head.shape[0]
    x_side = (2 * expert + 1 - parity, tp)
    y_side = (sp, 2 * (1 - row) + core)
    pair = (sp, 2 * row + 1 - core)
    other_quarter = 2 * (1 - row) + core
    sources, rows = (sent_x, sent_g), (rows_x, rows_g)
    started = []

    def send(src, dst, send_sem, recv_sem, device):
        copy = pltpu.make_async_remote_copy(
            src_ref=src, dst_ref=dst, send_sem=send_sem, recv_sem=recv_sem,
            device_id=device, device_id_type=MESH,
        )
        copy.start()
        started.append(copy)

    def spot(t, j, par, quarter):
        return rows[t].at[flipped(expert, j), par, :, columns(quarter, width)]

    loads = [
        pltpu.make_async_copy(src, dst, load_sem.at[n]) for n, (src, dst) in enumerate(zip(hbm, vmem))
    ]
    for load in loads:
        load.start()
    before, after = lax.rem(sp + n_sp - 1, n_sp), lax.rem(sp + 1, n_sp)
    fixed = [x_side, y_side, pair] + [(2 * flipped(expert, j) + parity, tp) for j in PLAN_CHUNKS]
    fixed += [(near, (lax.rem(tp + n, n_tp))) for near in (before, after) for n in range(n_tp)]
    targets = [(2 * (core + 2 * h) + row, expert) for h in range(2)]
    origins = [(2 * tp + par, 2 * parity + lax.rem(expert, 2)) for par in range(2)]
    barrier = pltpu.get_barrier_semaphore()
    for peer in fixed:
        pl.semaphore_signal(barrier, inc=1, device_id=peer, device_id_type=MESH)
    expected = len(fixed)
    for peer in targets + origins:
        away = jnp.logical_or(peer[0] != sp, peer[1] != tp)

        @pl.when(away)
        def _(peer=peer):
            pl.semaphore_signal(barrier, inc=1, device_id=peer, device_id_type=MESH)

        expected = expected + away.astype(jnp.int32)
    for load in loads[:2]:
        load.wait()
    lanes = lax.broadcasted_iota(jnp.int32, (tokens, tokens), 1)
    below = lax.broadcasted_iota(jnp.int32, (tokens, tokens), 0) < lanes
    first, second = routes[0:1], routes[1:2]
    ids = lax.broadcasted_iota(jnp.int32, (16, tokens), 0)
    first_hot = (ids == first).astype(jnp.float32)
    count = first_hot + (ids == second).astype(jnp.float32)
    earlier = dot(count.astype(jnp.bfloat16), below.astype(jnp.bfloat16), 1, 0)
    slot = lax.broadcasted_iota(jnp.int32, (capacity, tokens), 0)
    for e in range(experts):
        rank = earlier[e : e + 1].astype(jnp.int32)
        again = rank + first_hot[e : e + 1].astype(jnp.int32)
        hit = slot == jnp.where(first == e, rank, -1)
        hit_again = slot == jnp.where(second == e, again, -1)
        chosen_ref[e] = jnp.logical_or(hit, hit_again).astype(jnp.float32).astype(jnp.bfloat16)
        weight_ref[e] = jnp.where(hit, route_weights[0:1], 0.0) + jnp.where(
            hit_again, route_weights[1:2], 0.0
        )
    for load in loads[2:6]:
        load.wait()
    out_b[parity, expert] = (
        gate_b[...].astype(jnp.float32) * conv_out[...].astype(jnp.float32)
    ).astype(jnp.bfloat16)
    slot_weight = jnp.sum(weight_ref[...], axis=2, keepdims=True)
    mine = columns(tp, width)
    one_hot = chosen_ref[...].reshape(experts * capacity, tokens)
    sent_x[...] = dot(one_hot, token_x[:, mine], 1, 0).astype(jnp.bfloat16).reshape(sent_x.shape)
    scaled = slot_weight * dot(one_hot, token_g[:, mine], 1, 0).reshape(sent_g.shape)
    sent_g[...] = scaled.astype(jnp.bfloat16)
    one_hot = chosen_ref[expert]
    slot_weight = jnp.sum(weight_ref[expert], axis=1, keepdims=True)
    rows_x[expert, parity] = dot(one_hot, token_x[...], 1, 0).astype(jnp.bfloat16)
    rows_g[expert, parity] = (slot_weight * dot(one_hot, token_g[...], 1, 0)).astype(jnp.bfloat16)
    pl.semaphore_wait(barrier, expected)
    steps = [(j, t) for j in PLAN_CHUNKS for t in range(2)]

    def depart(n):
        j, t = steps[n]
        target = flipped(expert, j)
        send(sources[t].at[target], rows[t].at[expert, parity, :, columns(tp, width)],
             z_send.at[t, j], z_recv.at[t, j], (2 * target + parity, tp))

    def piece(t, par, which, part):
        return rows[t].at[expert, par, :, columns(2 * which + part, width)]

    def cross(t, part):
        block = piece(t, parity, core, part)
        send(block, block, own_send.at[t, part], own_recv.at[t, part], x_side)

    def own_stage(n):
        j, t = steps[n]
        block = spot(t, j, parity, tp)
        wait_arrival(block, z_recv.at[t, j])
        send(block, block, line_send.at[t, j, 0], line_recv.at[t, j, 0], x_side)
        send(block, block, line_send.at[t, j, 1], line_recv.at[t, j, 1], y_side)
        send(block, block, pair_send.at[t, j, 0], pair_recv.at[t, j, 0], pair)

    def across_stage(t, part):
        block = piece(t, 1 - parity, core, part)
        wait_arrival(block, own_recv.at[t, part])
        send(block, block, own_pair_send.at[t, part], own_pair_recv.at[t, part], pair)

    def near_x_stage(n):
        j, t = steps[n]
        block = spot(t, j, 1 - parity, tp)
        wait_arrival(block, line_recv.at[t, j, 0])
        if n not in PLAN_OVER_X:
            send(block, block, relay_send.at[t, j], relay_recv.at[t, j], y_side)
        send(block, block, pair_send.at[t, j, 1], pair_recv.at[t, j, 1], pair)

    def near_y_stage(n):
        j, t = steps[n]
        block = spot(t, j, parity, other_quarter)
        wait_arrival(block, line_recv.at[t, j, 1])
        if n in PLAN_OVER_X:
            send(block, block, relay_send.at[t, j], relay_recv.at[t, j], x_side)
        send(block, block, pair_send.at[t, j, 2], pair_recv.at[t, j, 2], pair)

    def far_stage(n):
        j, t = steps[n]
        block = spot(t, j, 1 - parity, other_quarter)
        wait_arrival(block, relay_recv.at[t, j])
        send(block, block, pair_send.at[t, j, 3], pair_recv.at[t, j, 3], pair)

    def arrived(j, t):
        if j == 0:
            for part in range(2):
                wait_arrival(piece(t, 1 - parity, 1 - core, part), own_pair_recv.at[t, part])
            return
        quarters = (2 * row + 1 - core, 2 * (1 - row) + 1 - core)
        spots = ((parity, quarters[0]), (1 - parity, quarters[0]),
                 (parity, quarters[1]), (1 - parity, quarters[1]))
        for n, (par, quarter) in enumerate(spots):
            wait_arrival(spot(t, j, par, quarter), pair_recv.at[t, j, n])

    def pre_stage(j):
        arrived(j, 0)
        if waiting:
            for load in waiting:
                load.wait()
            waiting.clear()
        x = rows_x[flipped(expert, j)].reshape(2 * capacity, model_width)
        gate_pre[j] = dot(x, wg[...], 1, 1)
        up_pre[j] = dot(x, wu[...], 1, 1)

    def hidden_stage(j):
        arrived(j, 1)
        source = flipped(expert, j)
        g = rows_g[source].reshape(2 * capacity, model_width)
        d_act = dot(g, wd[...], 1, 1)
        gate, up = gate_pre[j], up_pre[j]
        s = jax.nn.sigmoid(gate)
        silu = gate * s
        act[source] = (silu * up).astype(jnp.bfloat16)
        dup[source] = (d_act * silu).astype(jnp.bfloat16)
        dgt[source] = (d_act * up * s * (1.0 + gate * (1.0 - s))).astype(jnp.bfloat16)

    def backward(j):
        source = flipped(expert, j)
        for kept in range(2):
            side_core = core if kept else 1 - core
            store = part_mine if kept else part_out
            for h in range(2):
                cols = columns(2 * h + side_core, width)
                value = (
                    dot(dgt[source], wg[:, cols], 1, 0) + dot(dup[source], wu[:, cols], 1, 0)
                ).astype(jnp.bfloat16)
                for par in range(2):
                    piece = value[par * capacity : (par + 1) * capacity]
                    store[j, h, par, 0] = piece[:, :half]
                    store[j, h, par, 1] = piece[:, half:]
            if not kept:
                send(part_out.at[j], from_pair.at[j], rp_send.at[j], rp_recv.at[j], pair)

    def reduce_pair(j):
        wait_arrival(from_pair.at[j], rp_recv.at[j])
        total = part_mine[j].astype(jnp.float32) + from_pair[j].astype(jnp.float32)
        summed[j] = total.astype(jnp.bfloat16)
        send(summed.at[j, 0, 1 - parity], near_x.at[j], near_send.at[j, 0], near_recv.at[j, 0], x_side)
        send(summed.at[j, 1, :, 1 - row], near_y.at[j], near_send.at[j, 1], near_recv.at[j, 1], y_side)

    def fold_x(j):
        wait_arrival(near_x.at[j], near_recv.at[j, 0])
        total = summed[j, 0, parity, 1 - row].astype(jnp.float32) + near_x[j, 1 - row].astype(jnp.float32)
        passed[j, 0] = total.astype(jnp.bfloat16)
        send(passed.at[j, 0], far_y.at[j], far_send.at[j, 0], far_recv.at[j, 0], y_side)

    def fold_y(j):
        wait_arrival(near_y.at[j], near_recv.at[j, 1])
        total = summed[j, 1, 1 - parity, row].astype(jnp.float32) + near_y[j, 1 - parity].astype(jnp.float32)
        passed[j, 1] = total.astype(jnp.bfloat16)
        send(passed.at[j, 1], far_x.at[j], far_send.at[j, 1], far_recv.at[j, 1], x_side)

    def reduce_far(j):
        wait_arrival(far_y.at[j], far_recv.at[j, 0])
        wait_arrival(far_x.at[j], far_recv.at[j, 1])
        left = summed[j, 0, parity, row].astype(jnp.float32) + near_x[j, row].astype(jnp.float32)
        left = (left + far_y[j].astype(jnp.float32)).astype(jnp.bfloat16)
        right = summed[j, 1, parity, row].astype(jnp.float32) + near_y[j, parity].astype(jnp.float32)
        right = (right + far_x[j].astype(jnp.float32)).astype(jnp.bfloat16)
        if j == 0:
            out_back[expert, :, :half] = left
            out_back[expert, :, half:] = right
            return
        final[j, :, :half] = left
        final[j, :, half:] = right
        target = flipped(expert, j)
        send(final.at[j], out_back.at[expert], back_send.at[j], back_recv.at[j], (2 * target + parity, tp))

    def weight_grad(n):
        out, left, right = (
            (out_down, act, rows_g), (out_gate, dgt, rows_x), (out_up, dup, rows_x)
        )[n // 4]
        tile = model_width // 4
        cols = slice(n % 4 * tile, (n % 4 + 1) * tile)
        lhs = left[...].reshape(-1, left.shape[-1])
        rhs = right[:, :, :, cols].reshape(-1, tile)
        out[:, cols] = dot(lhs, rhs, 0, 0).astype(jnp.bfloat16)

    def share_branch():
        block = out_b.at[parity, expert]
        for j in PLAN_CHUNKS:
            send(block, block, b_send.at[j], b_recv.at[j], (2 * flipped(expert, j) + parity, tp))
        send(gate_b.at[pl.ds(0, halo)], out_head, h_send.at[0], h_recv.at[0], (before, tp))

    stages = {
        "depart": depart, "cross": cross, "own": own_stage, "across": across_stage,
        "near_x": near_x_stage, "near_y": near_y_stage, "far": far_stage,
        "pre": pre_stage, "hidden": hidden_stage, "back": backward, "pair": reduce_pair,
        "fold_x": fold_x, "fold_y": fold_y, "home": reduce_far, "grad": weight_grad,
    }
    waiting = loads[6:]
    owns = [n for n, stage in enumerate(PLAN) if stage[0] == "own"]
    for n, (name, *numbers) in enumerate(PLAN):
        stages[name](*numbers)
        if n == owns[-1]:
            share_branch()

    def block_columns(h, line, side_core):
        return columns(4 * h + 2 * side_core + line, half)

    for j in PLAN_CHUNKS:
        wait_arrival(out_b.at[parity, flipped(expert, j)], b_recv.at[j])
    send(out_b.at[parity], out_b.at[parity], b_send.at[0], b_recv.at[0], x_side)
    for j in PLAN_CHUNKS:
        wait_arrival(out_back.at[flipped(expert, j)], back_recv.at[j])
    one_hot = chosen_ref[...].reshape(experts * capacity, tokens)
    total = dot(one_hot, out_back[...].reshape(experts * capacity, width), 0, 0)
    guarded = []
    for h in range(2):
        cols = block_columns(h, row, core)
        base = token_g[:, cols].astype(jnp.float32)
        value = (base + total[:, h * half : (h + 1) * half]).astype(jnp.bfloat16)
        part_ref[h] = value
        stream_ref[pl.ds(0, tokens), cols] = value
    for h in range(2):
        src, dst, recv = part_ref.at[h], block_ref.at[parity, expert], place_recv.at[parity]
        away = jnp.logical_or(targets[h][0] != sp, targets[h][1] != tp)
        copy = pltpu.make_async_remote_copy(
            src_ref=src, dst_ref=dst, send_sem=place_send.at[h], recv_sem=recv,
            device_id=targets[h], device_id_type=MESH,
        )

        @pl.when(away)
        def _(copy=copy):
            copy.start()

        @pl.when(jnp.logical_not(away))
        def _(src=src, dst=dst, recv=recv):
            pltpu.make_async_copy(src, dst, recv).start()

        guarded.append((away, copy))
        cols = block_columns(h, row, core)
        dst = stream_ref.at[pl.ds(0, tokens), cols]
        send(src, dst, gather_send.at[h, 0], gather_recv.at[h, 0], y_side)
        send(src, dst, gather_send.at[h, 1], gather_recv.at[h, 1], pair)
        for n in range(n_tp):
            send(src.at[pl.ds(0, halo)], stream_ref.at[pl.ds(tokens, halo), cols],
                 halo_send.at[h, n], halo_recv.at[h, n], (before, lax.rem(tp + n, n_tp)))
    for h in range(2):
        block = stream_ref.at[pl.ds(0, tokens), block_columns(h, 1 - row, core)]
        wait_arrival(block, gather_recv.at[h, 0])
        send(block, block, gather_send.at[h, 2], gather_recv.at[h, 2], pair)
    for par in range(2):
        block = block_ref.at[par, tp]
        wait_arrival(block, place_recv.at[par])
        send(block, block, held_send.at[par, 0], held_recv.at[par, 0], y_side)
        send(block, block, held_send.at[par, 1], held_recv.at[par, 1], pair)
    for h in range(2):
        for line, slot in ((row, 1), (1 - row, 2)):
            wait_arrival(
                stream_ref.at[pl.ds(0, tokens), block_columns(h, line, 1 - core)], gather_recv.at[h, slot]
            )
        for n in range(n_tp):
            source = lax.rem(tp + n_tp - n, n_tp)
            cols = block_columns(h, source // 2, lax.rem(source, 2))
            wait_arrival(stream_ref.at[pl.ds(tokens, halo), cols], halo_recv.at[h, n])
    wait_arrival(out_head, h_recv.at[0])
    channels = conv_out.shape[1]
    reach = taps.shape[0] - 1
    d_branch = dot(stream_ref[...], out_proj[...], 1, 0)
    following = jnp.where(sp == n_sp - 1, 0.0, d_branch[tokens:] * out_head[...].astype(jnp.float32))
    d_branch = d_branch[:tokens]
    out_gate_b[...] = (d_branch * conv_out[...].astype(jnp.float32)).astype(jnp.bfloat16)
    extended[pl.ds(0, tokens)] = d_branch * gate_b[...].astype(jnp.float32)
    extended[pl.ds(tokens, halo)] = following
    d_input = jnp.zeros((tokens, channels), jnp.float32)
    for tap in range(reach + 1):
        d_input = d_input + taps[tap : tap + 1] * extended[pl.ds(reach - tap, tokens)]
    out_hidden[...] = (d_input * gate_c[...].astype(jnp.float32)).astype(jnp.bfloat16)
    out_gate_c[...] = (d_input * hidden_h[...].astype(jnp.float32)).astype(jnp.bfloat16)
    for par in range(2):
        block = block_ref.at[par, other_quarter]
        wait_arrival(block, held_recv.at[par, 0])
        send(block, block, held_send.at[par, 2], held_recv.at[par, 2], pair)
    wait_arrival(out_b.at[1 - parity], b_recv.at[0])
    for par in range(2):
        for line, slot in ((row, 1), (1 - row, 2)):
            wait_arrival(block_ref.at[par, 2 * line + 1 - core], held_recv.at[par, slot])
    out_proj_grad[...] = dot(
        block_ref[...].reshape(-1, half), out_b[...].reshape(-1, channels), 0, 0
    )
    for copy in started:
        copy.wait_send()
    for away, copy in guarded:
        pl.when(away)(copy.wait_send)


def run_experts(operands, halo, n_sp):
    _, _, token_x, token_g, gate_b, _, _, _, wg, *_ = operands
    tokens, model_width = token_x.shape
    experts = n_tp = n_sp // 2
    capacity = 2 * (3 * tokens // n_sp)
    width = model_width // n_tp
    units = wg.shape[0]
    half = width // 2
    channels = gate_b.shape[1]
    dma = pltpu.SemaphoreType.DMA

    def vmem(*shape):
        return pltpu.VMEM(shape, jnp.bfloat16)

    def wide(*shape):
        return pltpu.VMEM(shape, jnp.float32)

    rows = vmem(experts, 2, capacity, model_width)
    hidden = vmem(experts, 2 * capacity, units)
    blocks = vmem(experts, 2, 2, 2, capacity, half)
    near = vmem(experts, 2, capacity, half)
    far = vmem(experts, capacity, half)
    routed = vmem(experts, capacity, width)
    weight = vmem(units, model_width)
    pre = wide(experts, 2 * capacity, units)
    small = vmem(tokens, channels)
    return pl.pallas_call(
        functools.partial(expert_kernel, n_sp, n_tp),
        out_shape=(weight, weight, weight, wide(half, channels), small, small, small),
        in_specs=[HBM] * len(operands),
        out_specs=(VMEM,) * 7,
        scratch_shapes=[
            *(pltpu.VMEM(operand.shape, operand.dtype) for operand in operands),
            vmem(tokens + halo, model_width), vmem(2, experts, tokens, half),
            vmem(2, experts, tokens, channels), vmem(halo, channels),
            vmem(experts, capacity, tokens), wide(experts, capacity, tokens),
            wide(tokens + halo, channels),
            routed, routed, routed, vmem(2, tokens, half),
            rows, rows, hidden, hidden, hidden, blocks, blocks, blocks, blocks,
            near, near, near, far, far, routed, pre, pre,
            dma((len(operands),)), dma((2, experts)), dma((2, experts)), dma((2, 2)), dma((2, 2)),
            dma((2, experts, 2)), dma((2, experts, 2)), dma((2, experts)), dma((2, experts)),
            dma((2, experts, 4)), dma((2, experts, 4)), dma((2, 2)), dma((2, 2)),
            dma((experts,)), dma((experts,)), dma((1,)), dma((1,)),
            dma((experts,)), dma((experts,)), dma((experts, 2)), dma((experts, 2)),
            dma((experts, 2)), dma((experts, 2)), dma((experts,)), dma((experts,)),
            dma((2, 3)), dma((2, 3)), dma((2, n_tp)), dma((2, n_tp)),
            dma((2,)), dma((2,)), dma((2, 3)), dma((2, 3)),
        ],
        compiler_params=pltpu.CompilerParams(
            collective_id=3, has_side_effects=True, vmem_limit_bytes=48 * 1024 * 1024
        ),
    )(*operands)


def store_kernel(*refs):
    count = len(refs) // 2
    moves = [
        pltpu.make_async_copy(refs[n], refs[count + n], refs[-1].at[n]) for n in range(count)
    ]
    for move in moves:
        move.start()
    for move in moves:
        move.wait()


def store(arrays):
    return pl.pallas_call(
        store_kernel,
        out_shape=tuple(jax.ShapeDtypeStruct(a.shape, a.dtype) for a in arrays),
        in_specs=[VMEM] * len(arrays),
        out_specs=(HBM,) * len(arrays),
        scratch_shapes=[pltpu.SemaphoreType.DMA((len(arrays),))],
        compiler_params=pltpu.CompilerParams(vmem_limit_bytes=16 * 1024 * 1024),
    )(*arrays)


def stream_kernel(
    n_sp, n_tp, part_ref, stream_ref, block_ref,
    tp_send, tp_recv, h_send, h_recv, b_send, b_recv, s_send, s_recv,
):
    sp, tp = lax.axis_index("sp"), lax.axis_index("tp")
    tokens, width = part_ref.shape
    block = block_ref.shape[2]
    halo = stream_ref.shape[0] - tokens
    per_part, per_peer = width // block, n_sp // n_tp
    greet([
        (lax.rem(sp + i, n_sp), lax.rem(tp + j, n_tp))
        for i in range(n_sp) for j in range(n_tp) if i or j
    ])
    started = []

    def send(src, dst, send_sem, recv_sem, device):
        copy = pltpu.make_async_remote_copy(
            src_ref=src, dst_ref=dst, send_sem=send_sem, recv_sem=recv_sem,
            device_id=device, device_id_type=MESH,
        )
        copy.start()
        started.append((None, copy))

    keeper = sp // per_peer
    for b in range(per_part):
        target = tp * per_part + b
        src = part_ref.at[:, b * block : (b + 1) * block]
        dst = block_ref.at[sp]
        away = jnp.logical_or(target != sp, keeper != tp)
        copy = pltpu.make_async_remote_copy(
            src_ref=src, dst_ref=dst, send_sem=b_send.at[b], recv_sem=b_recv.at[lax.rem(sp, per_peer)],
            device_id=(target, keeper), device_id_type=MESH,
        )

        @pl.when(away)
        def _(copy=copy):
            copy.start()

        @pl.when(jnp.logical_not(away))
        def _(src=src, dst=dst):
            pltpu.make_async_copy(src, dst, b_recv.at[lax.rem(sp, per_peer)]).start()

        started.append((away, copy))
    mine = stream_ref.at[pl.ds(0, tokens), columns(tp, width)]
    edge = stream_ref.at[pl.ds(tokens, halo), columns(tp, width)]
    before = lax.rem(sp + n_sp - 1, n_sp)
    pltpu.make_async_copy(part_ref, mine, tp_recv.at[0]).start()
    for j in range(n_tp):
        peer = lax.rem(tp + j, n_tp)
        if j:
            send(part_ref, mine, tp_send.at[j], tp_recv.at[j], (sp, peer))
        send(part_ref.at[pl.ds(0, halo)], edge, h_send.at[j], h_recv.at[j], (before, peer))
    for n in range(per_peer):
        held = block_ref.at[tp * per_peer + n]
        wait_arrival(held, b_recv.at[n])
        for j in range(1, n_tp):
            send(held, held, s_send.at[n, j], s_recv.at[n, j], (sp, lax.rem(tp + j, n_tp)))
    for j in range(n_tp):
        source = lax.rem(tp + n_tp - j, n_tp)
        wait_arrival(stream_ref.at[pl.ds(0, tokens), columns(source, width)], tp_recv.at[j])
        wait_arrival(stream_ref.at[pl.ds(tokens, halo), columns(source, width)], h_recv.at[j])
        for n in range(per_peer):
            if j:
                wait_arrival(block_ref.at[source * per_peer + n], s_recv.at[n, j])
    for away, copy in started:
        if away is None:
            copy.wait_send()
        else:
            pl.when(away)(copy.wait_send)


def share_stream(part, halo, n_sp, n_tp):
    tokens, width = part.shape
    dma = pltpu.SemaphoreType.DMA
    block = width * n_tp // n_sp
    per_peer = n_sp // n_tp
    return pl.pallas_call(
        functools.partial(stream_kernel, n_sp, n_tp),
        out_shape=(
            jax.ShapeDtypeStruct((tokens + halo, width * n_tp), jnp.bfloat16),
            jax.ShapeDtypeStruct((n_sp, tokens, block), jnp.bfloat16),
        ),
        in_specs=[VMEM],
        out_specs=(VMEM, VMEM),
        scratch_shapes=[
            dma((n_tp,)), dma((n_tp,)), dma((n_tp,)), dma((n_tp,)),
            dma((width // block,)), dma((per_peer,)), dma((per_peer, n_tp)), dma((per_peer, n_tp)),
        ],
        compiler_params=pltpu.CompilerParams(collective_id=2, has_side_effects=True),
    )(part)


def slot_choice(routes, experts, capacity):
    flat_ids = routes.reshape(-1)
    one_hot = (flat_ids[:, None] == jnp.arange(experts, dtype=jnp.int32)[None, :])
    count = flat_ids.shape[0]
    before = jnp.arange(count)[:, None] > jnp.arange(count)[None, :]
    earlier = jnp.dot(
        before.astype(jnp.bfloat16), one_hot.astype(jnp.bfloat16), preferred_element_type=jnp.float32
    )
    ranked = jnp.sum(jnp.where(one_hot, earlier, 0.0), axis=1).astype(jnp.int32)
    return (flat_ids * capacity + ranked).reshape(routes.shape)


def contract_rows(left_side, right_side):
    return lax.dot_general(
        left_side, right_side, (((0,), (0,)), ((), ())), preferred_element_type=jnp.float32
    )


def contract_cols(left_side, right_side):
    return lax.dot_general(
        left_side, right_side, (((1,), (1,)), ((), ())), preferred_element_type=jnp.float32
    )


def per_device(
    moe_input,
    out_grad,
    routes,
    route_weights,
    gate_cols,
    up_cols,
    down_rows,
    out_proj,
    conv_out,
    gate_b,
    gate_c,
    hidden_h,
    conv_taps,
):
    seq_devices = lax.axis_size("sp")
    experts = seq_devices // 2
    tokens_here, model_width = moe_input.shape
    top_count = routes.shape[1]
    half_cap = 3 * tokens_here // seq_devices
    capacity = 2 * half_cap
    slot_count = experts * capacity
    n_tp = lax.axis_size("tp")
    halo = 16
    aligned = model_width % (seq_devices * 128) == 0
    planned = aligned and experts == len(PLAN_CHUNKS) + 1 and n_tp == experts
    if planned and top_count == 2 and conv_taps.shape[0] <= halo:
        operands = (
            routes.T, route_weights.T, moe_input, out_grad, gate_b, conv_out, gate_c, hidden_h,
            gate_cols.T, up_cols.T, down_rows, out_proj, conv_taps,
        )
        operands = tuple(pltpu.with_memory_space_constraint(a, pltpu.HBM) for a in operands)
        grads = run_experts(operands, halo, seq_devices)
        grad_gate, grad_up, *rest = store(grads)
        return (grad_gate.T, grad_up.T, *rest)
    positions = slot_choice(routes, experts, capacity)
    slots = jnp.arange(slot_count, dtype=jnp.int32)
    hits = slots[:, None, None] == positions[None]
    chosen = jnp.any(hits, axis=2).astype(jnp.bfloat16)
    slot_weight = jnp.sum(jnp.where(hits, route_weights[None], 0.0), axis=(1, 2))
    quarter = model_width // n_tp
    column_start = lax.axis_index("tp") * quarter
    source_x = lax.dynamic_slice_in_dim(moe_input, column_start, quarter, 1)
    source_g = lax.dynamic_slice_in_dim(out_grad, column_start, quarter, 1)
    sent_x = jnp.dot(chosen, source_x, preferred_element_type=jnp.float32).astype(jnp.bfloat16)
    sent_g = jnp.dot(chosen, source_g, preferred_element_type=jnp.float32)
    sent_g = (slot_weight[:, None] * sent_g).astype(jnp.bfloat16)
    branch = (gate_b.astype(jnp.float32) * conv_out.astype(jnp.float32)).astype(jnp.bfloat16)
    rows_x, rows_g, all_branch, next_gate_b = dispatch(
        sent_x.reshape(experts, capacity, quarter),
        sent_g.reshape(experts, capacity, quarter),
        branch,
        gate_b[:halo],
        seq_devices,
        n_tp,
    )
    rows_x = rows_x.reshape(-1, model_width)
    rows_g = rows_g.reshape(-1, model_width)
    gate_pre = jnp.dot(rows_x, gate_cols, preferred_element_type=jnp.float32)
    up_pre = jnp.dot(rows_x, up_cols, preferred_element_type=jnp.float32)
    sigmoid_g = jax.nn.sigmoid(gate_pre)
    silu_g = gate_pre * sigmoid_g
    activation = (silu_g * up_pre).astype(jnp.bfloat16)
    grad_down = contract_rows(activation, rows_g).astype(jnp.bfloat16)
    d_act = contract_cols(rows_g, down_rows)
    d_up = (d_act * silu_g).astype(jnp.bfloat16)
    d_gate = (d_act * up_pre * sigmoid_g * (1.0 + gate_pre * (1.0 - sigmoid_g))).astype(
        jnp.bfloat16
    )
    grad_gate = contract_rows(rows_x, d_gate).astype(jnp.bfloat16)
    grad_up = contract_rows(rows_x, d_up).astype(jnp.bfloat16)
    partial_value = (contract_cols(d_gate, gate_cols) + contract_cols(d_up, up_cols)).astype(
        jnp.bfloat16
    )
    returned = give_back(
        partial_value.reshape(2, experts, capacity, model_width), seq_devices, n_tp
    ).reshape(slot_count, quarter)
    stream_part = (source_g.astype(jnp.float32) + contract_rows(chosen, returned)).astype(
        jnp.bfloat16
    )
    if aligned:
        stream, stream_block = share_stream(stream_part, halo, seq_devices, n_tp)
        grad_proj = contract_rows(
            stream_block.reshape(-1, stream_block.shape[2]),
            all_branch.reshape(-1, all_branch.shape[2]),
        )
    else:
        stream = lax.all_gather(stream_part, "tp", axis=1, tiled=True)
        grad_proj = lax.psum_scatter(
            contract_rows(stream, branch), "sp", scatter_dimension=0, tiled=True
        )
    d_branch = jnp.dot(stream, out_proj, preferred_element_type=jnp.float32)
    d_after = d_branch[tokens_here:]
    d_branch = d_branch[:tokens_here]
    grad_gate_b = (d_branch * conv_out.astype(jnp.float32)).astype(jnp.bfloat16)
    d_conv = d_branch * gate_b.astype(jnp.float32)
    kernel_taps = conv_taps.shape[0]
    kernel_reach = kernel_taps - 1
    if aligned:
        last = lax.axis_index("sp") == seq_devices - 1
        next_rows_in = jnp.where(last, 0.0, d_after * next_gate_b.astype(jnp.float32))[:kernel_reach]
    else:
        next_rows_in = from_behind(d_conv[:kernel_reach], "sp", -1)
    extended = jnp.concatenate([d_conv, next_rows_in], axis=0)
    d_input = jnp.zeros_like(d_conv)
    for tap_index in range(kernel_taps):
        offset = kernel_reach - tap_index
        d_input = d_input + conv_taps[tap_index][None, :] * extended[offset : offset + tokens_here]
    grad_hidden = (d_input * gate_c.astype(jnp.float32)).astype(jnp.bfloat16)
    grad_gate_c = (d_input * hidden_h.astype(jnp.float32)).astype(jnp.bfloat16)
    return (grad_gate, grad_up, grad_down, grad_proj, grad_hidden, grad_gate_b, grad_gate_c)


def solution(mesh):
    placed = (
        P("sp", None),
        P("sp", None),
        P("sp", None),
        P("sp", None),
        P(None, ("sp", "tp")),
        P(None, ("sp", "tp")),
        P(("sp", "tp"), None),
        P(None, "tp"),
        P("sp", "tp"),
        P("sp", "tp"),
        P("sp", "tp"),
        P("sp", "tp"),
        P(None, "tp"),
    )
    return jax.shard_map(
        per_device,
        mesh=mesh,
        in_specs=placed,
        out_specs=(
            P(None, ("sp", "tp")),
            P(None, ("sp", "tp")),
            P(("sp", "tp"), None),
            P("sp", "tp"),
            P("sp", "tp"),
            P("sp", "tp"),
            P("sp", "tp"),
        ),
        check_vma=False,
    )
```

```python
import functools

import jax
import jax.numpy as jnp
from jax import lax
from jax.experimental import pallas as pl
from jax.experimental.pallas import tpu as pltpu
from jax.sharding import PartitionSpec as P


def from_behind(block, axis, distance):
    devices = range(lax.axis_size(axis))
    route = [(i - distance, i) for i in devices if i - distance in devices]
    return lax.ppermute(block, axis, route)


MESH = pl.DeviceIdType.MESH
VMEM = pl.BlockSpec(memory_space=pltpu.VMEM)
HBM = pl.BlockSpec(memory_space=pltpu.HBM)


def columns(index, width):
    return pl.ds(pl.multiple_of(index * width, width), width)


def wait_arrival(ref, sem):
    pltpu.make_async_copy(ref, ref, sem).wait()


def greet(peers):
    barrier = pltpu.get_barrier_semaphore()
    for peer in peers:
        pl.semaphore_signal(barrier, inc=1, device_id=peer, device_id_type=MESH)
    pl.semaphore_wait(barrier, len(peers))


def place(n_tp):
    sp, tp = lax.axis_index("sp"), lax.axis_index("tp")
    expert, parity = sp // 2, lax.rem(sp, 2)
    row, core = tp // 2, lax.rem(tp, 2)
    return sp, tp, expert, parity, row, core


def dispatch_kernel(
    n_sp, n_tp, chunks,
    x_ref, g_ref, branch_ref, head_ref,
    out_x, out_g, out_b, out_head,
    z_send, z_recv, own_send, relay_send, near_recv, diag_recv, pair_send, pair_recv, b_send, b_recv, h_send, h_recv,
):
    experts = n_sp // 2
    sp, tp, expert, parity, row, core = place(n_tp)
    width = x_ref.shape[-1]
    size = experts // chunks
    x_side = (2 * expert + 1 - parity, tp)
    y_side = (sp, 2 * (1 - row) + core)
    pair = (sp, 2 * row + 1 - core)
    greet([(lax.rem(sp + d, n_sp), tp) for d in range(1, n_sp)] + [y_side, pair])
    started = []
    sources, outs = (x_ref, g_ref), (out_x, out_g)

    def spot(t, par, first, quarter, count):
        return outs[t].at[par, pl.ds(first, count), :, columns(quarter, width)]

    def send(src, device, send_sem, recv_sem):
        copy = pltpu.make_async_remote_copy(
            src_ref=src, dst_ref=src, send_sem=send_sem, recv_sem=recv_sem,
            device_id=device, device_id_type=MESH,
        )
        copy.start()
        started.append(copy)

    for t in range(2):
        for d in range(experts):
            target = lax.rem(expert + d, experts)
            src = sources[t].at[pl.ds(target, 1)]
            dst = spot(t, parity, expert, tp, 1)
            if d == 0:
                pltpu.make_async_copy(src, dst, z_recv.at[t, 0]).start()
                continue
            copy = pltpu.make_async_remote_copy(
                src_ref=src, dst_ref=dst, send_sem=z_send.at[t, d], recv_sem=z_recv.at[t, d],
                device_id=(2 * target + parity, tp), device_id_type=MESH,
            )
            copy.start()
            started.append(copy)
    for d in range(n_sp):
        dst = out_b.at[sp]
        if d == 0:
            pltpu.make_async_copy(branch_ref, dst, b_recv.at[0]).start()
            continue
        copy = pltpu.make_async_remote_copy(
            src_ref=branch_ref, dst_ref=dst, send_sem=b_send.at[d], recv_sem=b_recv.at[d],
            device_id=(lax.rem(sp + d, n_sp), tp), device_id_type=MESH,
        )
        copy.start()
        started.append(copy)

    copy = pltpu.make_async_remote_copy(
        src_ref=head_ref, dst_ref=out_head, send_sem=h_send.at[0], recv_sem=h_recv.at[0],
        device_id=(lax.rem(sp + n_sp - 1, n_sp), tp), device_id_type=MESH,
    )
    copy.start()
    started.append(copy)

    own_chunk = expert // size
    other_quarter = 2 * (1 - row) + core

    def first_of(k):
        return lax.rem(own_chunk + chunks - k, chunks) * size

    def own_stage(k, t):
        first = first_of(k)
        for i in range(size):
            source = first + i
            d = lax.rem(expert + experts - source, experts)
            wait_arrival(spot(t, parity, source, tp, 1), z_recv.at[t, d])
        block = spot(t, parity, first, tp, size)
        send(block, x_side, own_send.at[t, k, 0], near_recv.at[t, k, 0])
        send(block, y_side, own_send.at[t, k, 1], near_recv.at[t, k, 1])
        send(block, pair, pair_send.at[t, k, 0], pair_recv.at[t, k, 0])

    def near_stage(k, t):
        first = first_of(k)
        from_x = spot(t, 1 - parity, first, tp, size)
        from_y = spot(t, parity, first, other_quarter, size)
        wait_arrival(from_x, near_recv.at[t, k, 0])
        if (k + t) % 2 == 0:
            send(from_x, y_side, relay_send.at[t, k], diag_recv.at[t, k])
        send(from_x, pair, pair_send.at[t, k, 1], pair_recv.at[t, k, 1])
        wait_arrival(from_y, near_recv.at[t, k, 1])
        if (k + t) % 2 == 1:
            send(from_y, x_side, relay_send.at[t, k], diag_recv.at[t, k])
        send(from_y, pair, pair_send.at[t, k, 2], pair_recv.at[t, k, 2])

    def far_stage(k, t):
        block = spot(t, 1 - parity, first_of(k), other_quarter, size)
        wait_arrival(block, diag_recv.at[t, k])
        send(block, pair, pair_send.at[t, k, 3], pair_recv.at[t, k, 3])

    order = [0] + [k for n in range(1, chunks // 2 + 1) for k in dict.fromkeys((n, chunks - n))]
    steps = [(k, t) for k in order for t in range(2)]
    for n in range(len(steps) + 3):
        if n < len(steps):
            own_stage(*steps[n])
        if 1 <= n < len(steps) + 1:
            near_stage(*steps[n - 1])
        if 3 <= n < len(steps) + 3:
            far_stage(*steps[n - 3])
    for k, t in steps:
        first = first_of(k)
        quarters = (2 * row + 1 - core, 2 * (1 - row) + 1 - core)
        spots = ((parity, quarters[0]), (1 - parity, quarters[0]),
                 (parity, quarters[1]), (1 - parity, quarters[1]))
        for j, (par, quarter) in enumerate(spots):
            wait_arrival(spot(t, par, first, quarter, size), pair_recv.at[t, k, j])
    for d in range(n_sp):
        wait_arrival(out_b.at[lax.rem(sp + n_sp - d, n_sp)], b_recv.at[d])
    wait_arrival(out_head, h_recv.at[0])
    for copy in started:
        copy.wait_send()


def dispatch(x, g, branch, head, n_sp, n_tp):
    experts, capacity, width = x.shape
    chunks = min(experts, 4)
    dma = pltpu.SemaphoreType.DMA
    rows = jax.ShapeDtypeStruct((2, experts, capacity, width * n_tp), jnp.bfloat16)
    return pl.pallas_call(
        functools.partial(dispatch_kernel, n_sp, n_tp, chunks),
        out_shape=(
            rows, rows, jax.ShapeDtypeStruct((n_sp,) + branch.shape, branch.dtype),
            jax.ShapeDtypeStruct(head.shape, head.dtype),
        ),
        in_specs=[VMEM] * 4,
        out_specs=(VMEM,) * 4,
        scratch_shapes=[
            dma((2, experts)), dma((2, experts)), dma((2, chunks, 2)), dma((2, chunks)),
            dma((2, chunks, 2)), dma((2, chunks)), dma((2, chunks, 4)), dma((2, chunks, 4)),
            dma((n_sp,)), dma((n_sp,)), dma((1,)), dma((1,)),
        ],
        compiler_params=pltpu.CompilerParams(
            collective_id=0, has_side_effects=True, vmem_limit_bytes=48 * 1024 * 1024
        ),
    )(x, g, branch, head)


def return_kernel(
    n_sp, n_tp, chunks,
    part_ref, out_ref,
    from_pair, summed, from_chips, final,
    pair_send, pair_recv, chip_send, chip_recv, z_send, z_recv,
):
    experts = n_sp // 2
    sp, tp, expert, parity, row, core = place(n_tp)
    width = out_ref.shape[-1]
    pair = (sp, 2 * row + 1 - core)
    offsets = ((1, 1), (1, 0), (0, 1), (0, 0))

    def other(dp, dr):
        return lax.rem(parity + dp, 2), lax.rem(row + dr, 2)

    chips = [(2 * expert + other(dp, dr)[0], 2 * other(dp, dr)[1] + core) for dp, dr in offsets[:3]]
    along = [(2 * lax.rem(expert + d, experts) + parity, tp) for d in range(1, experts)]
    greet([pair] + chips + along)
    started, guarded = [], []

    def send(src, dst, send_sem, recv_sem, device):
        copy = pltpu.make_async_remote_copy(
            src_ref=src, dst_ref=dst, send_sem=send_sem, recv_sem=recv_sem,
            device_id=device, device_id_type=MESH,
        )
        copy.start()
        started.append(copy)

    size = experts // chunks
    own_chunk = expert // size
    order = [chunks // 2] if chunks > 1 else []
    order += [k for k in range(1, chunks) if k not in order] + [0]

    def first_of(k):
        return lax.rem(own_chunk + k, chunks) * size

    for k in order:
        part = pl.ds(first_of(k), size)
        for n, (dp, dr) in enumerate(offsets):
            par, line = other(dp, dr)
            src = part_ref.at[par, part, :, columns(2 * line + 1 - core, width)]
            send(src, from_pair.at[n, part], pair_send.at[n, k], pair_recv.at[n, k], pair)
    for k in order:
        first = first_of(k)
        part = pl.ds(first, size)
        for n, (dp, dr) in enumerate(offsets):
            par, line = other(dp, dr)
            wait_arrival(from_pair.at[n, part], pair_recv.at[n, k])
            for i in range(size):
                mine = part_ref[par, first + i, :, columns(2 * line + core, width)]
                total = mine.astype(jnp.float32) + from_pair[n, first + i].astype(jnp.float32)
                summed[n, first + i] = total.astype(jnp.bfloat16)
            if n < 3:
                send(summed.at[n, part], from_chips.at[n, part], chip_send.at[n, k],
                     chip_recv.at[n, k], chips[n])
    for k in order:
        first = first_of(k)
        part = pl.ds(first, size)
        for n in range(3):
            wait_arrival(from_chips.at[n, part], chip_recv.at[n, k])
        for i in range(size):
            target = first + i
            total = summed[3, target].astype(jnp.float32)
            for n in range(3):
                total = total + from_chips[n, target].astype(jnp.float32)
            final[target] = total.astype(jnp.bfloat16)
            away = target != expert
            copy = pltpu.make_async_remote_copy(
                src_ref=final.at[target], dst_ref=out_ref.at[expert],
                send_sem=z_send.at[target], recv_sem=z_recv.at[expert],
                device_id=(2 * target + parity, tp), device_id_type=MESH,
            )
            if size == 1 and k:
                copy.start()
                started.append(copy)
                continue
            if size == 1:
                out_ref[expert] = final[target]
                continue

            @pl.when(away)
            def _(copy=copy):
                copy.start()

            @pl.when(jnp.logical_not(away))
            def _():
                out_ref[expert] = final[expert]

            guarded.append((away, copy))
    for d in range(1, experts):
        source = lax.rem(expert + experts - d, experts)
        wait_arrival(out_ref.at[source], z_recv.at[source])
    for copy in started:
        copy.wait_send()
    for away, copy in guarded:
        pl.when(away)(copy.wait_send)


def give_back(part, n_sp, n_tp):
    _, experts, capacity, model_width = part.shape
    width = model_width // n_tp
    dma = pltpu.SemaphoreType.DMA
    block = (experts, capacity, width)
    chunks = min(experts, 4)
    return pl.pallas_call(
        functools.partial(return_kernel, n_sp, n_tp, chunks),
        out_shape=jax.ShapeDtypeStruct(block, jnp.bfloat16),
        in_specs=[VMEM],
        out_specs=VMEM,
        scratch_shapes=[
            pltpu.VMEM((4,) + block, jnp.bfloat16), pltpu.VMEM((4,) + block, jnp.bfloat16),
            pltpu.VMEM((3,) + block, jnp.bfloat16), pltpu.VMEM(block, jnp.bfloat16),
            dma((4, chunks)), dma((4, chunks)), dma((3, chunks)), dma((3, chunks)),
            dma((experts,)), dma((experts,)),
        ],
        compiler_params=pltpu.CompilerParams(
            collective_id=1, has_side_effects=True, vmem_limit_bytes=48 * 1024 * 1024
        ),
    )(part)


def dot(left, right, left_dim, right_dim):
    return lax.dot_general(
        left, right, (((left_dim,), (right_dim,)), ((), ())), preferred_element_type=jnp.float32
    )


def flipped(index, bits):
    bit = 1
    while bit <= bits:
        if bits & bit:
            index = index + bit - 2 * bit * lax.rem(index // bit, 2)
        bit *= 2
    return index


PLAN_CHUNKS = (1, 3, 2)
PLAN_OVER_X = (2, 4)
PLAN_EXTRA = (0, 1)
PLAN_RELAYED = (0, 1)
PLAN = (
    ("depart", 3), ("depart", 0), ("cross", 1, 0), ("depart", 2), ("cross", 0, 0), ("depart", 1),
    ("depart", 4), ("across", 1, 0), ("across", 0, 0), ("own", 3), ("own", 0), ("aside", 0), ("own", 2),
    ("near_x", 3), ("extra", 0), ("near_y", 3), ("own", 1), ("aside", 1), ("near_x", 0), ("depart", 5),
    ("pre", 0), ("near_y", 2), ("near_y", 0), ("share",), ("own", 4), ("hidden", 0), ("far", 3),
    ("near_x", 1), ("near_x", 2), ("own", 5), ("extra", 1), ("far", 2), ("back", 0), ("pre", 3),
    ("near_y", 4), ("hidden", 3), ("far", 0), ("near_x", 4), ("near_x", 5), ("back", 3), ("pair_x", 0),
    ("near_y", 1), ("pre", 1), ("far", 4), ("pair_y", 3), ("pair_x", 3), ("near_y", 5), ("far", 1),
    ("pair_y", 0), ("far", 5), ("pre", 2), ("hidden", 2), ("back", 2), ("hidden", 1), ("fold_x", 3),
    ("fold_y", 3), ("back", 1), ("pair_y", 2), ("pair_x", 2), ("pair_x", 1), ("grad", 11), ("grad", 6),
    ("pair_y", 1), ("home", 3), ("fold_y", 2), ("fold_x", 2), ("fold_y", 1), ("fold_x", 1), ("grad", 8),
    ("grad", 5), ("home", 2), ("grad", 9), ("fold_y", 0), ("grad", 7), ("fold_x", 0), ("grad", 1),
    ("home", 1), ("grad", 2), ("grad", 0), ("home", 0), ("grad", 10), ("grad", 4), ("grad", 3),
)


def expert_kernel(
    n_sp, n_tp, *refs,
):
    hbm, refs = refs[:13], refs[13:]
    out_gate, out_up, out_down, out_proj_grad, out_hidden, out_gate_b, out_gate_c = refs[:7]
    vmem, refs = refs[7:20], refs[20:]
    routes, route_weights, token_x, token_g, gate_b, conv_out, *vmem_rest = vmem
    gate_c, hidden_h, wg, wu, wd, out_proj, taps = vmem_rest
    (
        stream_ref, block_ref, out_b, out_head, chosen_ref, weight_ref, extended,
        sent_x, sent_g, extra, out_back, part_ref,
        rows_x, rows_g, act, dup, dgt, part_out, part_mine, from_pair, summed,
        near_x, near_y, passed, far_x, far_y, final, gate_pre, up_pre,
        load_sem, z_send, z_recv, own_send, own_recv, line_send, line_recv, relay_send, relay_recv,
        pair_send, pair_recv, own_pair_send, own_pair_recv, b_send, b_recv, h_send, h_recv,
        rp_send, rp_recv, near_send, near_recv, far_send, far_recv, back_send, back_recv,
        gather_send, gather_recv, halo_send, halo_recv, place_send, place_recv, held_send, held_recv,
    ) = refs
    experts = n_sp // 2
    sp, tp, expert, parity, row, core = place(n_tp)
    capacity, width = sent_x.shape[1:]
    tokens, model_width = token_x.shape
    half = width // 2
    halo = out_head.shape[0]
    x_side = (2 * expert + 1 - parity, tp)
    y_side = (sp, 2 * (1 - row) + core)
    pair = (sp, 2 * row + 1 - core)
    other_quarter = 2 * (1 - row) + core
    sources, rows = (sent_x, sent_g), (rows_x, rows_g)
    started = []

    def send(src, dst, send_sem, recv_sem, device):
        copy = pltpu.make_async_remote_copy(
            src_ref=src, dst_ref=dst, send_sem=send_sem, recv_sem=recv_sem,
            device_id=device, device_id_type=MESH,
        )
        copy.start()
        started.append(copy)

    def spot(t, j, par, quarter):
        return rows[t].at[flipped(expert, j), par, :, columns(quarter, width)]

    loads = [
        pltpu.make_async_copy(src, dst, load_sem.at[n]) for n, (src, dst) in enumerate(zip(hbm, vmem))
    ]
    for load in loads[:6]:
        load.start()
    before, after = lax.rem(sp + n_sp - 1, n_sp), lax.rem(sp + 1, n_sp)
    fixed = [x_side, y_side, pair] + [(2 * flipped(expert, j) + parity, tp) for j in PLAN_CHUNKS]
    fixed += [(near, (lax.rem(tp + n, n_tp))) for near in (before, after) for n in range(n_tp)]
    targets = [(2 * (core + 2 * h) + row, expert) for h in range(2)]
    origins = [(2 * tp + par, 2 * parity + lax.rem(expert, 2)) for par in range(2)]
    barrier = pltpu.get_barrier_semaphore()
    for peer in fixed:
        pl.semaphore_signal(barrier, inc=1, device_id=peer, device_id_type=MESH)
    expected = len(fixed)
    for peer in targets + origins:
        away = jnp.logical_or(peer[0] != sp, peer[1] != tp)

        @pl.when(away)
        def _(peer=peer):
            pl.semaphore_signal(barrier, inc=1, device_id=peer, device_id_type=MESH)

        expected = expected + away.astype(jnp.int32)
    for load in loads[:2]:
        load.wait()
    lanes = lax.broadcasted_iota(jnp.int32, (tokens, tokens), 1)
    below = lax.broadcasted_iota(jnp.int32, (tokens, tokens), 0) < lanes
    first, second = routes[0:1], routes[1:2]
    ids = lax.broadcasted_iota(jnp.int32, (16, tokens), 0)
    first_hot = (ids == first).astype(jnp.float32)
    count = first_hot + (ids == second).astype(jnp.float32)
    earlier = dot(count.astype(jnp.bfloat16), below.astype(jnp.bfloat16), 1, 0)
    slot = lax.broadcasted_iota(jnp.int32, (capacity, tokens), 0)
    for e in range(experts):
        rank = earlier[e : e + 1].astype(jnp.int32)
        again = rank + first_hot[e : e + 1].astype(jnp.int32)
        hit = slot == jnp.where(first == e, rank, -1)
        hit_again = slot == jnp.where(second == e, again, -1)
        chosen_ref[e] = jnp.logical_or(hit, hit_again).astype(jnp.float32).astype(jnp.bfloat16)
        weight_ref[e] = jnp.where(hit, route_weights[0:1], 0.0) + jnp.where(
            hit_again, route_weights[1:2], 0.0
        )
    for load in loads[2:6]:
        load.wait()
    for load in loads[6:]:
        load.start()
    out_b[parity, expert] = (
        gate_b[...].astype(jnp.float32) * conv_out[...].astype(jnp.float32)
    ).astype(jnp.bfloat16)
    tokens_in, prepared = (token_x, token_g), []

    def select(t, one_hot, weight, cols):
        value = dot(one_hot, tokens_in[t][:, cols], 1, 0)
        return (weight * value if t else value).astype(jnp.bfloat16)

    def prepare(kind, t):
        if (kind, t) not in prepared:
            prepared.append((kind, t))
            if kind == "own":
                weight = jnp.sum(weight_ref[expert], axis=1, keepdims=True)
                rows[t][expert, parity] = select(t, chosen_ref[expert], weight, slice(None))
            elif kind == "sent":
                weight = jnp.sum(weight_ref[...].reshape(-1, tokens), axis=1, keepdims=True)
                one_hot = chosen_ref[...].reshape(-1, tokens)
                value = select(t, one_hot, weight, columns(tp, width))
                sources[t][...] = value.reshape(experts, capacity, width)
            else:
                target = flipped(expert, 1)
                weight = jnp.sum(weight_ref[target], axis=1, keepdims=True)
                extra[t] = select(t, chosen_ref[target], weight, columns(other_quarter, width))

    for t in range(2):
        prepare("own", t)
        prepare("sent", t)
    for n in PLAN_EXTRA:
        prepare("extra", n % 2)
    pl.semaphore_wait(barrier, expected)
    steps = [(j, t) for j in PLAN_CHUNKS for t in range(2)]

    def depart(n):
        j, t = steps[n]
        target = flipped(expert, j)
        prepare("sent", t)
        send(sources[t].at[target], rows[t].at[expert, parity, :, columns(tp, width)],
             z_send.at[t, j], z_recv.at[t, j], (2 * target + parity, tp))

    def piece(t, par, which, part):
        return rows[t].at[expert, par, :, columns(2 * which + part, width)]

    def depart_extra(n):
        j, t = steps[n]
        prepare("extra", t)
        send(extra.at[t], rows[t].at[expert, parity, :, columns(other_quarter, width)],
             line_send.at[t, j, 1], line_recv.at[t, j, 1], (2 * flipped(expert, j) + parity, tp))

    def cross(t, part):
        prepare("own", t)
        block = piece(t, parity, core, row if t in PLAN_RELAYED else part)
        send(block, block, own_send.at[t, part], own_recv.at[t, part], x_side)

    def own_stage(n):
        j, t = steps[n]
        block = spot(t, j, parity, tp)
        wait_arrival(block, z_recv.at[t, j])
        send(block, block, line_send.at[t, j, 0], line_recv.at[t, j, 0], x_side)
        if n not in PLAN_EXTRA:
            send(block, block, line_send.at[t, j, 1], line_recv.at[t, j, 1], y_side)
        send(block, block, pair_send.at[t, j, 0], pair_recv.at[t, j, 0], pair)

    def across_stage(t, part):
        block = piece(t, 1 - parity, core, row if t in PLAN_RELAYED else part)
        wait_arrival(block, own_recv.at[t, part])
        if t in PLAN_RELAYED:
            send(block, block, own_send.at[t, 1], own_recv.at[t, 1], y_side)
        send(block, block, own_pair_send.at[t, part], own_pair_recv.at[t, part], pair)

    def aside_stage(t):
        block = piece(t, 1 - parity, core, 1 - row)
        wait_arrival(block, own_recv.at[t, 1])
        send(block, block, own_pair_send.at[t, 1], own_pair_recv.at[t, 1], pair)

    def near_x_stage(n):
        j, t = steps[n]
        block = spot(t, j, 1 - parity, tp)
        wait_arrival(block, line_recv.at[t, j, 0])
        if n not in PLAN_OVER_X:
            send(block, block, relay_send.at[t, j], relay_recv.at[t, j], y_side)
        send(block, block, pair_send.at[t, j, 1], pair_recv.at[t, j, 1], pair)

    def near_y_stage(n):
        j, t = steps[n]
        block = spot(t, j, parity, other_quarter)
        wait_arrival(block, line_recv.at[t, j, 1])
        if n in PLAN_OVER_X:
            send(block, block, relay_send.at[t, j], relay_recv.at[t, j], x_side)
        send(block, block, pair_send.at[t, j, 2], pair_recv.at[t, j, 2], pair)

    def far_stage(n):
        j, t = steps[n]
        block = spot(t, j, 1 - parity, other_quarter)
        wait_arrival(block, relay_recv.at[t, j])
        send(block, block, pair_send.at[t, j, 3], pair_recv.at[t, j, 3], pair)

    def arrived(j, t):
        if j == 0:
            for part in range(2):
                which = lax.rem(row + part, 2) if t in PLAN_RELAYED else part
                wait_arrival(piece(t, 1 - parity, 1 - core, which), own_pair_recv.at[t, part])
            return
        quarters = (2 * row + 1 - core, 2 * (1 - row) + 1 - core)
        spots = ((parity, quarters[0]), (1 - parity, quarters[0]),
                 (parity, quarters[1]), (1 - parity, quarters[1]))
        for n, (par, quarter) in enumerate(spots):
            wait_arrival(spot(t, j, par, quarter), pair_recv.at[t, j, n])

    def pre_stage(j):
        arrived(j, 0)
        if waiting:
            for load in waiting:
                load.wait()
            waiting.clear()
        x = rows_x[flipped(expert, j)].reshape(2 * capacity, model_width)
        gate_pre[j] = dot(x, wg[...], 1, 1)
        up_pre[j] = dot(x, wu[...], 1, 1)

    def hidden_stage(j):
        arrived(j, 1)
        source = flipped(expert, j)
        g = rows_g[source].reshape(2 * capacity, model_width)
        d_act = dot(g, wd[...], 1, 1)
        gate, up = gate_pre[j], up_pre[j]
        s = jax.nn.sigmoid(gate)
        silu = gate * s
        act[source] = (silu * up).astype(jnp.bfloat16)
        dup[source] = (d_act * silu).astype(jnp.bfloat16)
        dgt[source] = (d_act * up * s * (1.0 + gate * (1.0 - s))).astype(jnp.bfloat16)

    def backward(j):
        source = flipped(expert, j)
        for kept in range(2):
            side_core = core if kept else 1 - core
            store = part_mine if kept else part_out
            for h in range(2):
                cols = columns(2 * h + side_core, width)
                value = (
                    dot(dgt[source], wg[:, cols], 1, 0) + dot(dup[source], wu[:, cols], 1, 0)
                ).astype(jnp.bfloat16)
                for par in range(2):
                    piece = value[par * capacity : (par + 1) * capacity]
                    store[j, h, par, 0] = piece[:, :half]
                    store[j, h, par, 1] = piece[:, half:]
                if not kept:
                    send(part_out.at[j, h], from_pair.at[j, h], rp_send.at[j, h], rp_recv.at[j, h], pair)

    def add_pair(j, h):
        wait_arrival(from_pair.at[j, h], rp_recv.at[j, h])
        total = part_mine[j, h].astype(jnp.float32) + from_pair[j, h].astype(jnp.float32)
        summed[j, h] = total.astype(jnp.bfloat16)

    def pair_x(j):
        add_pair(j, 0)
        send(summed.at[j, 0, 1 - parity], near_x.at[j], near_send.at[j, 0], near_recv.at[j, 0], x_side)

    def pair_y(j):
        add_pair(j, 1)
        send(summed.at[j, 1, :, 1 - row], near_y.at[j], near_send.at[j, 1], near_recv.at[j, 1], y_side)

    def fold_x(j):
        wait_arrival(near_x.at[j], near_recv.at[j, 0])
        total = summed[j, 0, parity, 1 - row].astype(jnp.float32) + near_x[j, 1 - row].astype(jnp.float32)
        passed[j, 0] = total.astype(jnp.bfloat16)
        send(passed.at[j, 0], far_y.at[j], far_send.at[j, 0], far_recv.at[j, 0], y_side)

    def fold_y(j):
        wait_arrival(near_y.at[j], near_recv.at[j, 1])
        total = summed[j, 1, 1 - parity, row].astype(jnp.float32) + near_y[j, 1 - parity].astype(jnp.float32)
        passed[j, 1] = total.astype(jnp.bfloat16)
        send(passed.at[j, 1], far_x.at[j], far_send.at[j, 1], far_recv.at[j, 1], x_side)

    def reduce_far(j):
        wait_arrival(far_y.at[j], far_recv.at[j, 0])
        wait_arrival(far_x.at[j], far_recv.at[j, 1])
        left = summed[j, 0, parity, row].astype(jnp.float32) + near_x[j, row].astype(jnp.float32)
        left = (left + far_y[j].astype(jnp.float32)).astype(jnp.bfloat16)
        right = summed[j, 1, parity, row].astype(jnp.float32) + near_y[j, parity].astype(jnp.float32)
        right = (right + far_x[j].astype(jnp.float32)).astype(jnp.bfloat16)
        if j == 0:
            out_back[expert, :, :half] = left
            out_back[expert, :, half:] = right
            return
        final[j, :, :half] = left
        final[j, :, half:] = right
        target = flipped(expert, j)
        send(final.at[j], out_back.at[expert], back_send.at[j], back_recv.at[j], (2 * target + parity, tp))

    def weight_grad(n):
        out, left, right = (
            (out_down, act, rows_g), (out_gate, dgt, rows_x), (out_up, dup, rows_x)
        )[n // 4]
        tile = model_width // 4
        cols = slice(n % 4 * tile, (n % 4 + 1) * tile)
        lhs = left[...].reshape(-1, left.shape[-1])
        rhs = right[:, :, :, cols].reshape(-1, tile)
        out[:, cols] = dot(lhs, rhs, 0, 0).astype(jnp.bfloat16)

    def share_branch():
        block = out_b.at[parity, expert]
        for j in PLAN_CHUNKS:
            send(block, block, b_send.at[j], b_recv.at[j], (2 * flipped(expert, j) + parity, tp))
        send(gate_b.at[pl.ds(0, halo)], out_head, h_send.at[0], h_recv.at[0], (before, tp))

    stages = {
        "depart": depart, "extra": depart_extra, "cross": cross, "own": own_stage,
        "across": across_stage, "aside": aside_stage,
        "near_x": near_x_stage, "near_y": near_y_stage, "far": far_stage,
        "pre": pre_stage, "hidden": hidden_stage, "back": backward, "pair_x": pair_x, "pair_y": pair_y,
        "fold_x": fold_x, "fold_y": fold_y, "home": reduce_far, "grad": weight_grad,
        "share": share_branch,
    }
    waiting = loads[6:]
    for name, *numbers in PLAN:
        stages[name](*numbers)

    def block_columns(h, line, side_core):
        return columns(4 * h + 2 * side_core + line, half)

    for j in PLAN_CHUNKS:
        wait_arrival(out_b.at[parity, flipped(expert, j)], b_recv.at[j])
    send(out_b.at[parity], out_b.at[parity], b_send.at[0], b_recv.at[0], x_side)
    for j in PLAN_CHUNKS:
        wait_arrival(out_back.at[flipped(expert, j)], back_recv.at[j])
    one_hot = chosen_ref[...].reshape(experts * capacity, tokens)
    total = dot(one_hot, out_back[...].reshape(experts * capacity, width), 0, 0)
    guarded = []
    for h in range(2):
        cols = block_columns(h, row, core)
        base = token_g[:, cols].astype(jnp.float32)
        value = (base + total[:, h * half : (h + 1) * half]).astype(jnp.bfloat16)
        part_ref[h] = value
        stream_ref[pl.ds(0, tokens), cols] = value
    for h in range(2):
        src, dst, recv = part_ref.at[h], block_ref.at[parity, expert], place_recv.at[parity]
        away = jnp.logical_or(targets[h][0] != sp, targets[h][1] != tp)
        copy = pltpu.make_async_remote_copy(
            src_ref=src, dst_ref=dst, send_sem=place_send.at[h], recv_sem=recv,
            device_id=targets[h], device_id_type=MESH,
        )

        @pl.when(away)
        def _(copy=copy):
            copy.start()

        @pl.when(jnp.logical_not(away))
        def _(src=src, dst=dst, recv=recv):
            pltpu.make_async_copy(src, dst, recv).start()

        guarded.append((away, copy))
        cols = block_columns(h, row, core)
        dst = stream_ref.at[pl.ds(0, tokens), cols]
        send(src, dst, gather_send.at[h, 0], gather_recv.at[h, 0], y_side)
        send(src, dst, gather_send.at[h, 1], gather_recv.at[h, 1], pair)
        for n in range(n_tp):
            send(src.at[pl.ds(0, halo)], stream_ref.at[pl.ds(tokens, halo), cols],
                 halo_send.at[h, n], halo_recv.at[h, n], (before, lax.rem(tp + n, n_tp)))
    for h in range(2):
        block = stream_ref.at[pl.ds(0, tokens), block_columns(h, 1 - row, core)]
        wait_arrival(block, gather_recv.at[h, 0])
        send(block, block, gather_send.at[h, 2], gather_recv.at[h, 2], pair)
    for par in range(2):
        block = block_ref.at[par, tp]
        wait_arrival(block, place_recv.at[par])
        send(block, block, held_send.at[par, 0], held_recv.at[par, 0], y_side)
        send(block, block, held_send.at[par, 1], held_recv.at[par, 1], pair)
    for h in range(2):
        for line, slot in ((row, 1), (1 - row, 2)):
            wait_arrival(
                stream_ref.at[pl.ds(0, tokens), block_columns(h, line, 1 - core)], gather_recv.at[h, slot]
            )
        for n in range(n_tp):
            source = lax.rem(tp + n_tp - n, n_tp)
            cols = block_columns(h, source // 2, lax.rem(source, 2))
            wait_arrival(stream_ref.at[pl.ds(tokens, halo), cols], halo_recv.at[h, n])
    wait_arrival(out_head, h_recv.at[0])
    channels = conv_out.shape[1]
    reach = taps.shape[0] - 1
    d_branch = dot(stream_ref[...], out_proj[...], 1, 0)
    following = jnp.where(sp == n_sp - 1, 0.0, d_branch[tokens:] * out_head[...].astype(jnp.float32))
    d_branch = d_branch[:tokens]
    out_gate_b[...] = (d_branch * conv_out[...].astype(jnp.float32)).astype(jnp.bfloat16)
    extended[pl.ds(0, tokens)] = d_branch * gate_b[...].astype(jnp.float32)
    extended[pl.ds(tokens, halo)] = following
    d_input = jnp.zeros((tokens, channels), jnp.float32)
    for tap in range(reach + 1):
        d_input = d_input + taps[tap : tap + 1] * extended[pl.ds(reach - tap, tokens)]
    out_hidden[...] = (d_input * gate_c[...].astype(jnp.float32)).astype(jnp.bfloat16)
    out_gate_c[...] = (d_input * hidden_h[...].astype(jnp.float32)).astype(jnp.bfloat16)
    for par in range(2):
        block = block_ref.at[par, other_quarter]
        wait_arrival(block, held_recv.at[par, 0])
        send(block, block, held_send.at[par, 2], held_recv.at[par, 2], pair)
    wait_arrival(out_b.at[1 - parity], b_recv.at[0])
    for par in range(2):
        for line, slot in ((row, 1), (1 - row, 2)):
            wait_arrival(block_ref.at[par, 2 * line + 1 - core], held_recv.at[par, slot])
    out_proj_grad[...] = dot(
        block_ref[...].reshape(-1, half), out_b[...].reshape(-1, channels), 0, 0
    )
    for copy in started:
        copy.wait_send()
    for away, copy in guarded:
        pl.when(away)(copy.wait_send)


def run_experts(operands, halo, n_sp):
    _, _, token_x, token_g, gate_b, _, _, _, wg, *_ = operands
    tokens, model_width = token_x.shape
    experts = n_tp = n_sp // 2
    capacity = 2 * (3 * tokens // n_sp)
    width = model_width // n_tp
    units = wg.shape[0]
    half = width // 2
    channels = gate_b.shape[1]
    dma = pltpu.SemaphoreType.DMA

    def vmem(*shape):
        return pltpu.VMEM(shape, jnp.bfloat16)

    def wide(*shape):
        return pltpu.VMEM(shape, jnp.float32)

    rows = vmem(experts, 2, capacity, model_width)
    hidden = vmem(experts, 2 * capacity, units)
    blocks = vmem(experts, 2, 2, 2, capacity, half)
    near = vmem(experts, 2, capacity, half)
    far = vmem(experts, capacity, half)
    routed = vmem(experts, capacity, width)
    weight = vmem(units, model_width)
    pre = wide(experts, 2 * capacity, units)
    small = vmem(tokens, channels)
    return pl.pallas_call(
        functools.partial(expert_kernel, n_sp, n_tp),
        out_shape=(weight, weight, weight, wide(half, channels), small, small, small),
        in_specs=[HBM] * len(operands),
        out_specs=(VMEM,) * 7,
        scratch_shapes=[
            *(pltpu.VMEM(operand.shape, operand.dtype) for operand in operands),
            vmem(tokens + halo, model_width), vmem(2, experts, tokens, half),
            vmem(2, experts, tokens, channels), vmem(halo, channels),
            vmem(experts, capacity, tokens), wide(experts, capacity, tokens),
            wide(tokens + halo, channels),
            routed, routed, vmem(2, capacity, width), routed, vmem(2, tokens, half),
            rows, rows, hidden, hidden, hidden, blocks, blocks, blocks, blocks,
            near, near, near, far, far, routed, pre, pre,
            dma((len(operands),)), dma((2, experts)), dma((2, experts)), dma((2, 2)), dma((2, 2)),
            dma((2, experts, 2)), dma((2, experts, 2)), dma((2, experts)), dma((2, experts)),
            dma((2, experts, 4)), dma((2, experts, 4)), dma((2, 2)), dma((2, 2)),
            dma((experts,)), dma((experts,)), dma((1,)), dma((1,)),
            dma((experts, 2)), dma((experts, 2)), dma((experts, 2)), dma((experts, 2)),
            dma((experts, 2)), dma((experts, 2)), dma((experts,)), dma((experts,)),
            dma((2, 3)), dma((2, 3)), dma((2, n_tp)), dma((2, n_tp)),
            dma((2,)), dma((2,)), dma((2, 3)), dma((2, 3)),
        ],
        compiler_params=pltpu.CompilerParams(
            collective_id=3, has_side_effects=True, vmem_limit_bytes=48 * 1024 * 1024
        ),
    )(*operands)


def store_kernel(*refs):
    count = len(refs) // 2
    moves = [
        pltpu.make_async_copy(refs[n], refs[count + n], refs[-1].at[n]) for n in range(count)
    ]
    for move in moves:
        move.start()
    for move in moves:
        move.wait()


def store(arrays):
    return pl.pallas_call(
        store_kernel,
        out_shape=tuple(jax.ShapeDtypeStruct(a.shape, a.dtype) for a in arrays),
        in_specs=[VMEM] * len(arrays),
        out_specs=(HBM,) * len(arrays),
        scratch_shapes=[pltpu.SemaphoreType.DMA((len(arrays),))],
        compiler_params=pltpu.CompilerParams(vmem_limit_bytes=16 * 1024 * 1024),
    )(*arrays)


def stream_kernel(
    n_sp, n_tp, part_ref, stream_ref, block_ref,
    tp_send, tp_recv, h_send, h_recv, b_send, b_recv, s_send, s_recv,
):
    sp, tp = lax.axis_index("sp"), lax.axis_index("tp")
    tokens, width = part_ref.shape
    block = block_ref.shape[2]
    halo = stream_ref.shape[0] - tokens
    per_part, per_peer = width // block, n_sp // n_tp
    greet([
        (lax.rem(sp + i, n_sp), lax.rem(tp + j, n_tp))
        for i in range(n_sp) for j in range(n_tp) if i or j
    ])
    started = []

    def send(src, dst, send_sem, recv_sem, device):
        copy = pltpu.make_async_remote_copy(
            src_ref=src, dst_ref=dst, send_sem=send_sem, recv_sem=recv_sem,
            device_id=device, device_id_type=MESH,
        )
        copy.start()
        started.append((None, copy))

    keeper = sp // per_peer
    for b in range(per_part):
        target = tp * per_part + b
        src = part_ref.at[:, b * block : (b + 1) * block]
        dst = block_ref.at[sp]
        away = jnp.logical_or(target != sp, keeper != tp)
        copy = pltpu.make_async_remote_copy(
            src_ref=src, dst_ref=dst, send_sem=b_send.at[b], recv_sem=b_recv.at[lax.rem(sp, per_peer)],
            device_id=(target, keeper), device_id_type=MESH,
        )

        @pl.when(away)
        def _(copy=copy):
            copy.start()

        @pl.when(jnp.logical_not(away))
        def _(src=src, dst=dst):
            pltpu.make_async_copy(src, dst, b_recv.at[lax.rem(sp, per_peer)]).start()

        started.append((away, copy))
    mine = stream_ref.at[pl.ds(0, tokens), columns(tp, width)]
    edge = stream_ref.at[pl.ds(tokens, halo), columns(tp, width)]
    before = lax.rem(sp + n_sp - 1, n_sp)
    pltpu.make_async_copy(part_ref, mine, tp_recv.at[0]).start()
    for j in range(n_tp):
        peer = lax.rem(tp + j, n_tp)
        if j:
            send(part_ref, mine, tp_send.at[j], tp_recv.at[j], (sp, peer))
        send(part_ref.at[pl.ds(0, halo)], edge, h_send.at[j], h_recv.at[j], (before, peer))
    for n in range(per_peer):
        held = block_ref.at[tp * per_peer + n]
        wait_arrival(held, b_recv.at[n])
        for j in range(1, n_tp):
            send(held, held, s_send.at[n, j], s_recv.at[n, j], (sp, lax.rem(tp + j, n_tp)))
    for j in range(n_tp):
        source = lax.rem(tp + n_tp - j, n_tp)
        wait_arrival(stream_ref.at[pl.ds(0, tokens), columns(source, width)], tp_recv.at[j])
        wait_arrival(stream_ref.at[pl.ds(tokens, halo), columns(source, width)], h_recv.at[j])
        for n in range(per_peer):
            if j:
                wait_arrival(block_ref.at[source * per_peer + n], s_recv.at[n, j])
    for away, copy in started:
        if away is None:
            copy.wait_send()
        else:
            pl.when(away)(copy.wait_send)


def share_stream(part, halo, n_sp, n_tp):
    tokens, width = part.shape
    dma = pltpu.SemaphoreType.DMA
    block = width * n_tp // n_sp
    per_peer = n_sp // n_tp
    return pl.pallas_call(
        functools.partial(stream_kernel, n_sp, n_tp),
        out_shape=(
            jax.ShapeDtypeStruct((tokens + halo, width * n_tp), jnp.bfloat16),
            jax.ShapeDtypeStruct((n_sp, tokens, block), jnp.bfloat16),
        ),
        in_specs=[VMEM],
        out_specs=(VMEM, VMEM),
        scratch_shapes=[
            dma((n_tp,)), dma((n_tp,)), dma((n_tp,)), dma((n_tp,)),
            dma((width // block,)), dma((per_peer,)), dma((per_peer, n_tp)), dma((per_peer, n_tp)),
        ],
        compiler_params=pltpu.CompilerParams(collective_id=2, has_side_effects=True),
    )(part)


def slot_choice(routes, experts, capacity):
    flat_ids = routes.reshape(-1)
    one_hot = (flat_ids[:, None] == jnp.arange(experts, dtype=jnp.int32)[None, :])
    count = flat_ids.shape[0]
    before = jnp.arange(count)[:, None] > jnp.arange(count)[None, :]
    earlier = jnp.dot(
        before.astype(jnp.bfloat16), one_hot.astype(jnp.bfloat16), preferred_element_type=jnp.float32
    )
    ranked = jnp.sum(jnp.where(one_hot, earlier, 0.0), axis=1).astype(jnp.int32)
    return (flat_ids * capacity + ranked).reshape(routes.shape)


def contract_rows(left_side, right_side):
    return lax.dot_general(
        left_side, right_side, (((0,), (0,)), ((), ())), preferred_element_type=jnp.float32
    )


def contract_cols(left_side, right_side):
    return lax.dot_general(
        left_side, right_side, (((1,), (1,)), ((), ())), preferred_element_type=jnp.float32
    )


def per_device(
    moe_input,
    out_grad,
    routes,
    route_weights,
    gate_cols,
    up_cols,
    down_rows,
    out_proj,
    conv_out,
    gate_b,
    gate_c,
    hidden_h,
    conv_taps,
):
    seq_devices = lax.axis_size("sp")
    experts = seq_devices // 2
    tokens_here, model_width = moe_input.shape
    top_count = routes.shape[1]
    half_cap = 3 * tokens_here // seq_devices
    capacity = 2 * half_cap
    slot_count = experts * capacity
    n_tp = lax.axis_size("tp")
    halo = 16
    aligned = model_width % (seq_devices * 128) == 0
    planned = aligned and experts == len(PLAN_CHUNKS) + 1 and n_tp == experts
    if planned and top_count == 2 and conv_taps.shape[0] <= halo:
        operands = (
            routes.T, route_weights.T, moe_input, out_grad, gate_b, conv_out, gate_c, hidden_h,
            gate_cols.T, up_cols.T, down_rows, out_proj, conv_taps,
        )
        operands = tuple(pltpu.with_memory_space_constraint(a, pltpu.HBM) for a in operands)
        grads = run_experts(operands, halo, seq_devices)
        grad_gate, grad_up, *rest = store(grads)
        return (grad_gate.T, grad_up.T, *rest)
    positions = slot_choice(routes, experts, capacity)
    slots = jnp.arange(slot_count, dtype=jnp.int32)
    hits = slots[:, None, None] == positions[None]
    chosen = jnp.any(hits, axis=2).astype(jnp.bfloat16)
    slot_weight = jnp.sum(jnp.where(hits, route_weights[None], 0.0), axis=(1, 2))
    quarter = model_width // n_tp
    column_start = lax.axis_index("tp") * quarter
    source_x = lax.dynamic_slice_in_dim(moe_input, column_start, quarter, 1)
    source_g = lax.dynamic_slice_in_dim(out_grad, column_start, quarter, 1)
    sent_x = jnp.dot(chosen, source_x, preferred_element_type=jnp.float32).astype(jnp.bfloat16)
    sent_g = jnp.dot(chosen, source_g, preferred_element_type=jnp.float32)
    sent_g = (slot_weight[:, None] * sent_g).astype(jnp.bfloat16)
    branch = (gate_b.astype(jnp.float32) * conv_out.astype(jnp.float32)).astype(jnp.bfloat16)
    rows_x, rows_g, all_branch, next_gate_b = dispatch(
        sent_x.reshape(experts, capacity, quarter),
        sent_g.reshape(experts, capacity, quarter),
        branch,
        gate_b[:halo],
        seq_devices,
        n_tp,
    )
    rows_x = rows_x.reshape(-1, model_width)
    rows_g = rows_g.reshape(-1, model_width)
    gate_pre = jnp.dot(rows_x, gate_cols, preferred_element_type=jnp.float32)
    up_pre = jnp.dot(rows_x, up_cols, preferred_element_type=jnp.float32)
    sigmoid_g = jax.nn.sigmoid(gate_pre)
    silu_g = gate_pre * sigmoid_g
    activation = (silu_g * up_pre).astype(jnp.bfloat16)
    grad_down = contract_rows(activation, rows_g).astype(jnp.bfloat16)
    d_act = contract_cols(rows_g, down_rows)
    d_up = (d_act * silu_g).astype(jnp.bfloat16)
    d_gate = (d_act * up_pre * sigmoid_g * (1.0 + gate_pre * (1.0 - sigmoid_g))).astype(
        jnp.bfloat16
    )
    grad_gate = contract_rows(rows_x, d_gate).astype(jnp.bfloat16)
    grad_up = contract_rows(rows_x, d_up).astype(jnp.bfloat16)
    partial_value = (contract_cols(d_gate, gate_cols) + contract_cols(d_up, up_cols)).astype(
        jnp.bfloat16
    )
    returned = give_back(
        partial_value.reshape(2, experts, capacity, model_width), seq_devices, n_tp
    ).reshape(slot_count, quarter)
    stream_part = (source_g.astype(jnp.float32) + contract_rows(chosen, returned)).astype(
        jnp.bfloat16
    )
    if aligned:
        stream, stream_block = share_stream(stream_part, halo, seq_devices, n_tp)
        grad_proj = contract_rows(
            stream_block.reshape(-1, stream_block.shape[2]),
            all_branch.reshape(-1, all_branch.shape[2]),
        )
    else:
        stream = lax.all_gather(stream_part, "tp", axis=1, tiled=True)
        grad_proj = lax.psum_scatter(
            contract_rows(stream, branch), "sp", scatter_dimension=0, tiled=True
        )
    d_branch = jnp.dot(stream, out_proj, preferred_element_type=jnp.float32)
    d_after = d_branch[tokens_here:]
    d_branch = d_branch[:tokens_here]
    grad_gate_b = (d_branch * conv_out.astype(jnp.float32)).astype(jnp.bfloat16)
    d_conv = d_branch * gate_b.astype(jnp.float32)
    kernel_taps = conv_taps.shape[0]
    kernel_reach = kernel_taps - 1
    if aligned:
        last = lax.axis_index("sp") == seq_devices - 1
        next_rows_in = jnp.where(last, 0.0, d_after * next_gate_b.astype(jnp.float32))[:kernel_reach]
    else:
        next_rows_in = from_behind(d_conv[:kernel_reach], "sp", -1)
    extended = jnp.concatenate([d_conv, next_rows_in], axis=0)
    d_input = jnp.zeros_like(d_conv)
    for tap_index in range(kernel_taps):
        offset = kernel_reach - tap_index
        d_input = d_input + conv_taps[tap_index][None, :] * extended[offset : offset + tokens_here]
    grad_hidden = (d_input * gate_c.astype(jnp.float32)).astype(jnp.bfloat16)
    grad_gate_c = (d_input * hidden_h.astype(jnp.float32)).astype(jnp.bfloat16)
    return (grad_gate, grad_up, grad_down, grad_proj, grad_hidden, grad_gate_b, grad_gate_c)


def solution(mesh):
    placed = (
        P("sp", None),
        P("sp", None),
        P("sp", None),
        P("sp", None),
        P(None, ("sp", "tp")),
        P(None, ("sp", "tp")),
        P(("sp", "tp"), None),
        P(None, "tp"),
        P("sp", "tp"),
        P("sp", "tp"),
        P("sp", "tp"),
        P("sp", "tp"),
        P(None, "tp"),
    )
    return jax.shard_map(
        per_device,
        mesh=mesh,
        in_specs=placed,
        out_specs=(
            P(None, ("sp", "tp")),
            P(None, ("sp", "tp")),
            P(("sp", "tp"), None),
            P("sp", "tp"),
            P("sp", "tp"),
            P("sp", "tp"),
            P("sp", "tp"),
        ),
        check_vma=False,
    )
```

```python
import functools

import jax
import jax.numpy as jnp
from jax import lax
from jax.experimental import pallas as pl
from jax.experimental.pallas import tpu as pltpu
from jax.sharding import PartitionSpec as P


def from_behind(block, axis, distance):
    devices = range(lax.axis_size(axis))
    route = [(i - distance, i) for i in devices if i - distance in devices]
    return lax.ppermute(block, axis, route)


MESH = pl.DeviceIdType.MESH
VMEM = pl.BlockSpec(memory_space=pltpu.VMEM)
HBM = pl.BlockSpec(memory_space=pltpu.HBM)


def columns(index, width):
    return pl.ds(pl.multiple_of(index * width, width), width)


def wait_arrival(ref, sem):
    pltpu.make_async_copy(ref, ref, sem).wait()


def greet(peers):
    barrier = pltpu.get_barrier_semaphore()
    for peer in peers:
        pl.semaphore_signal(barrier, inc=1, device_id=peer, device_id_type=MESH)
    pl.semaphore_wait(barrier, len(peers))


def place(n_tp):
    sp, tp = lax.axis_index("sp"), lax.axis_index("tp")
    expert, parity = sp // 2, lax.rem(sp, 2)
    row, core = tp // 2, lax.rem(tp, 2)
    return sp, tp, expert, parity, row, core


def dispatch_kernel(
    n_sp, n_tp, chunks,
    x_ref, g_ref, branch_ref, head_ref,
    out_x, out_g, out_b, out_head,
    z_send, z_recv, own_send, relay_send, near_recv, diag_recv, pair_send, pair_recv, b_send, b_recv, h_send, h_recv,
):
    experts = n_sp // 2
    sp, tp, expert, parity, row, core = place(n_tp)
    width = x_ref.shape[-1]
    size = experts // chunks
    x_side = (2 * expert + 1 - parity, tp)
    y_side = (sp, 2 * (1 - row) + core)
    pair = (sp, 2 * row + 1 - core)
    greet([(lax.rem(sp + d, n_sp), tp) for d in range(1, n_sp)] + [y_side, pair])
    started = []
    sources, outs = (x_ref, g_ref), (out_x, out_g)

    def spot(t, par, first, quarter, count):
        return outs[t].at[par, pl.ds(first, count), :, columns(quarter, width)]

    def send(src, device, send_sem, recv_sem):
        copy = pltpu.make_async_remote_copy(
            src_ref=src, dst_ref=src, send_sem=send_sem, recv_sem=recv_sem,
            device_id=device, device_id_type=MESH,
        )
        copy.start()
        started.append(copy)

    for t in range(2):
        for d in range(experts):
            target = lax.rem(expert + d, experts)
            src = sources[t].at[pl.ds(target, 1)]
            dst = spot(t, parity, expert, tp, 1)
            if d == 0:
                pltpu.make_async_copy(src, dst, z_recv.at[t, 0]).start()
                continue
            copy = pltpu.make_async_remote_copy(
                src_ref=src, dst_ref=dst, send_sem=z_send.at[t, d], recv_sem=z_recv.at[t, d],
                device_id=(2 * target + parity, tp), device_id_type=MESH,
            )
            copy.start()
            started.append(copy)
    for d in range(n_sp):
        dst = out_b.at[sp]
        if d == 0:
            pltpu.make_async_copy(branch_ref, dst, b_recv.at[0]).start()
            continue
        copy = pltpu.make_async_remote_copy(
            src_ref=branch_ref, dst_ref=dst, send_sem=b_send.at[d], recv_sem=b_recv.at[d],
            device_id=(lax.rem(sp + d, n_sp), tp), device_id_type=MESH,
        )
        copy.start()
        started.append(copy)

    copy = pltpu.make_async_remote_copy(
        src_ref=head_ref, dst_ref=out_head, send_sem=h_send.at[0], recv_sem=h_recv.at[0],
        device_id=(lax.rem(sp + n_sp - 1, n_sp), tp), device_id_type=MESH,
    )
    copy.start()
    started.append(copy)

    own_chunk = expert // size
    other_quarter = 2 * (1 - row) + core

    def first_of(k):
        return lax.rem(own_chunk + chunks - k, chunks) * size

    def own_stage(k, t):
        first = first_of(k)
        for i in range(size):
            source = first + i
            d = lax.rem(expert + experts - source, experts)
            wait_arrival(spot(t, parity, source, tp, 1), z_recv.at[t, d])
        block = spot(t, parity, first, tp, size)
        send(block, x_side, own_send.at[t, k, 0], near_recv.at[t, k, 0])
        send(block, y_side, own_send.at[t, k, 1], near_recv.at[t, k, 1])
        send(block, pair, pair_send.at[t, k, 0], pair_recv.at[t, k, 0])

    def near_stage(k, t):
        first = first_of(k)
        from_x = spot(t, 1 - parity, first, tp, size)
        from_y = spot(t, parity, first, other_quarter, size)
        wait_arrival(from_x, near_recv.at[t, k, 0])
        if (k + t) % 2 == 0:
            send(from_x, y_side, relay_send.at[t, k], diag_recv.at[t, k])
        send(from_x, pair, pair_send.at[t, k, 1], pair_recv.at[t, k, 1])
        wait_arrival(from_y, near_recv.at[t, k, 1])
        if (k + t) % 2 == 1:
            send(from_y, x_side, relay_send.at[t, k], diag_recv.at[t, k])
        send(from_y, pair, pair_send.at[t, k, 2], pair_recv.at[t, k, 2])

    def far_stage(k, t):
        block = spot(t, 1 - parity, first_of(k), other_quarter, size)
        wait_arrival(block, diag_recv.at[t, k])
        send(block, pair, pair_send.at[t, k, 3], pair_recv.at[t, k, 3])

    order = [0] + [k for n in range(1, chunks // 2 + 1) for k in dict.fromkeys((n, chunks - n))]
    steps = [(k, t) for k in order for t in range(2)]
    for n in range(len(steps) + 3):
        if n < len(steps):
            own_stage(*steps[n])
        if 1 <= n < len(steps) + 1:
            near_stage(*steps[n - 1])
        if 3 <= n < len(steps) + 3:
            far_stage(*steps[n - 3])
    for k, t in steps:
        first = first_of(k)
        quarters = (2 * row + 1 - core, 2 * (1 - row) + 1 - core)
        spots = ((parity, quarters[0]), (1 - parity, quarters[0]),
                 (parity, quarters[1]), (1 - parity, quarters[1]))
        for j, (par, quarter) in enumerate(spots):
            wait_arrival(spot(t, par, first, quarter, size), pair_recv.at[t, k, j])
    for d in range(n_sp):
        wait_arrival(out_b.at[lax.rem(sp + n_sp - d, n_sp)], b_recv.at[d])
    wait_arrival(out_head, h_recv.at[0])
    for copy in started:
        copy.wait_send()


def dispatch(x, g, branch, head, n_sp, n_tp):
    experts, capacity, width = x.shape
    chunks = min(experts, 4)
    dma = pltpu.SemaphoreType.DMA
    rows = jax.ShapeDtypeStruct((2, experts, capacity, width * n_tp), jnp.bfloat16)
    return pl.pallas_call(
        functools.partial(dispatch_kernel, n_sp, n_tp, chunks),
        out_shape=(
            rows, rows, jax.ShapeDtypeStruct((n_sp,) + branch.shape, branch.dtype),
            jax.ShapeDtypeStruct(head.shape, head.dtype),
        ),
        in_specs=[VMEM] * 4,
        out_specs=(VMEM,) * 4,
        scratch_shapes=[
            dma((2, experts)), dma((2, experts)), dma((2, chunks, 2)), dma((2, chunks)),
            dma((2, chunks, 2)), dma((2, chunks)), dma((2, chunks, 4)), dma((2, chunks, 4)),
            dma((n_sp,)), dma((n_sp,)), dma((1,)), dma((1,)),
        ],
        compiler_params=pltpu.CompilerParams(
            collective_id=0, has_side_effects=True, vmem_limit_bytes=48 * 1024 * 1024
        ),
    )(x, g, branch, head)


def return_kernel(
    n_sp, n_tp, chunks,
    part_ref, out_ref,
    from_pair, summed, from_chips, final,
    pair_send, pair_recv, chip_send, chip_recv, z_send, z_recv,
):
    experts = n_sp // 2
    sp, tp, expert, parity, row, core = place(n_tp)
    width = out_ref.shape[-1]
    pair = (sp, 2 * row + 1 - core)
    offsets = ((1, 1), (1, 0), (0, 1), (0, 0))

    def other(dp, dr):
        return lax.rem(parity + dp, 2), lax.rem(row + dr, 2)

    chips = [(2 * expert + other(dp, dr)[0], 2 * other(dp, dr)[1] + core) for dp, dr in offsets[:3]]
    along = [(2 * lax.rem(expert + d, experts) + parity, tp) for d in range(1, experts)]
    greet([pair] + chips + along)
    started, guarded = [], []

    def send(src, dst, send_sem, recv_sem, device):
        copy = pltpu.make_async_remote_copy(
            src_ref=src, dst_ref=dst, send_sem=send_sem, recv_sem=recv_sem,
            device_id=device, device_id_type=MESH,
        )
        copy.start()
        started.append(copy)

    size = experts // chunks
    own_chunk = expert // size
    order = [chunks // 2] if chunks > 1 else []
    order += [k for k in range(1, chunks) if k not in order] + [0]

    def first_of(k):
        return lax.rem(own_chunk + k, chunks) * size

    for k in order:
        part = pl.ds(first_of(k), size)
        for n, (dp, dr) in enumerate(offsets):
            par, line = other(dp, dr)
            src = part_ref.at[par, part, :, columns(2 * line + 1 - core, width)]
            send(src, from_pair.at[n, part], pair_send.at[n, k], pair_recv.at[n, k], pair)
    for k in order:
        first = first_of(k)
        part = pl.ds(first, size)
        for n, (dp, dr) in enumerate(offsets):
            par, line = other(dp, dr)
            wait_arrival(from_pair.at[n, part], pair_recv.at[n, k])
            for i in range(size):
                mine = part_ref[par, first + i, :, columns(2 * line + core, width)]
                total = mine.astype(jnp.float32) + from_pair[n, first + i].astype(jnp.float32)
                summed[n, first + i] = total.astype(jnp.bfloat16)
            if n < 3:
                send(summed.at[n, part], from_chips.at[n, part], chip_send.at[n, k],
                     chip_recv.at[n, k], chips[n])
    for k in order:
        first = first_of(k)
        part = pl.ds(first, size)
        for n in range(3):
            wait_arrival(from_chips.at[n, part], chip_recv.at[n, k])
        for i in range(size):
            target = first + i
            total = summed[3, target].astype(jnp.float32)
            for n in range(3):
                total = total + from_chips[n, target].astype(jnp.float32)
            final[target] = total.astype(jnp.bfloat16)
            away = target != expert
            copy = pltpu.make_async_remote_copy(
                src_ref=final.at[target], dst_ref=out_ref.at[expert],
                send_sem=z_send.at[target], recv_sem=z_recv.at[expert],
                device_id=(2 * target + parity, tp), device_id_type=MESH,
            )
            if size == 1 and k:
                copy.start()
                started.append(copy)
                continue
            if size == 1:
                out_ref[expert] = final[target]
                continue

            @pl.when(away)
            def _(copy=copy):
                copy.start()

            @pl.when(jnp.logical_not(away))
            def _():
                out_ref[expert] = final[expert]

            guarded.append((away, copy))
    for d in range(1, experts):
        source = lax.rem(expert + experts - d, experts)
        wait_arrival(out_ref.at[source], z_recv.at[source])
    for copy in started:
        copy.wait_send()
    for away, copy in guarded:
        pl.when(away)(copy.wait_send)


def give_back(part, n_sp, n_tp):
    _, experts, capacity, model_width = part.shape
    width = model_width // n_tp
    dma = pltpu.SemaphoreType.DMA
    block = (experts, capacity, width)
    chunks = min(experts, 4)
    return pl.pallas_call(
        functools.partial(return_kernel, n_sp, n_tp, chunks),
        out_shape=jax.ShapeDtypeStruct(block, jnp.bfloat16),
        in_specs=[VMEM],
        out_specs=VMEM,
        scratch_shapes=[
            pltpu.VMEM((4,) + block, jnp.bfloat16), pltpu.VMEM((4,) + block, jnp.bfloat16),
            pltpu.VMEM((3,) + block, jnp.bfloat16), pltpu.VMEM(block, jnp.bfloat16),
            dma((4, chunks)), dma((4, chunks)), dma((3, chunks)), dma((3, chunks)),
            dma((experts,)), dma((experts,)),
        ],
        compiler_params=pltpu.CompilerParams(
            collective_id=1, has_side_effects=True, vmem_limit_bytes=48 * 1024 * 1024
        ),
    )(part)


def dot(left, right, left_dim, right_dim):
    return lax.dot_general(
        left, right, (((left_dim,), (right_dim,)), ((), ())), preferred_element_type=jnp.float32
    )


def flipped(index, bits):
    bit = 1
    while bit <= bits:
        if bits & bit:
            index = index + bit - 2 * bit * lax.rem(index // bit, 2)
        bit *= 2
    return index


PLAN_CHUNKS = (1, 3, 2)
PLAN_OVER_X = (0, 5)
PLAN_EXTRA = (0, 1)
PLAN = (
    ("depart", 3), ("cross", 0, 0), ("cross", 0, 1), ("cross", 1, 0), ("cross", 1, 1), ("depart", 0),
    ("depart", 2), ("depart", 1), ("across", 0, 0), ("across", 0, 1), ("across", 1, 0), ("across", 1, 1),
    ("depart", 4), ("extra", 0), ("depart", 5), ("own", 3), ("own", 0), ("near_x", 3), ("own", 2),
    ("aside", 0, 0), ("aside", 0, 1), ("near_y", 3), ("own", 1), ("aside", 1, 0), ("aside", 1, 1),
    ("near_x", 2), ("far", 3), ("extra", 1), ("own", 4), ("share",), ("near_y", 2), ("pre", 0), ("near_y", 0),
    ("own", 5), ("far", 2), ("hidden", 0), ("near_x", 4), ("back", 0), ("near_y", 4), ("pre", 3),
    ("near_x", 1), ("near_y", 1), ("far", 0), ("hidden", 3), ("near_y", 5), ("back", 3), ("near_x", 0),
    ("near_x", 5), ("pair_x", 3), ("far", 4), ("pair_x", 0), ("pair_y", 3), ("pair_y", 0), ("pre", 1),
    ("far", 5), ("pre", 2), ("far", 1), ("hidden", 2), ("back", 2), ("fold_y", 3), ("fold_x", 3),
    ("hidden", 1), ("pair_x", 2), ("pair_y", 2), ("back", 1), ("grad", 3), ("pair_x", 1), ("left", 3),
    ("right", 3), ("pair_y", 1), ("grad", 5), ("grad", 11), ("grad", 8), ("fold_x", 2), ("grad", 10),
    ("fold_y", 2), ("fold_y", 0), ("fold_x", 1), ("grad", 9), ("fold_y", 1), ("left", 2), ("right", 2),
    ("fold_x", 0), ("left", 1), ("right", 1), ("grad", 7), ("grad", 2), ("grad", 4), ("left", 0),
    ("right", 0), ("grad", 0), ("grad", 1), ("grad", 6),
)


def expert_kernel(
    n_sp, n_tp, *refs,
):
    hbm, refs = refs[:13], refs[13:]
    out_gate, out_up, out_down, out_proj_grad, out_hidden, out_gate_b, out_gate_c = refs[:7]
    vmem, refs = refs[7:20], refs[20:]
    routes, route_weights, token_x, token_g, gate_b, conv_out, *vmem_rest = vmem
    gate_c, hidden_h, wg, wu, wd, out_proj, taps = vmem_rest
    (
        stream_ref, block_ref, out_b, out_head, chosen_ref, weight_ref, extended,
        sent_x, sent_g, extra, out_back, part_ref,
        rows_x, rows_g, act, dup, dgt, part_out, part_mine, from_pair, summed,
        near_x, near_y, passed, far_x, far_y, final, gate_pre, up_pre,
        load_sem, z_send, z_recv, own_send, own_recv, line_send, line_recv, relay_send, relay_recv,
        pair_send, pair_recv, own_pair_send, own_pair_recv, b_send, b_recv, h_send, h_recv,
        rp_send, rp_recv, near_send, near_recv, far_send, far_recv, back_send, back_recv,
        gather_send, gather_recv, halo_send, halo_recv, place_send, place_recv, held_send, held_recv,
    ) = refs
    experts = n_sp // 2
    sp, tp, expert, parity, row, core = place(n_tp)
    capacity, width = sent_x.shape[1:]
    tokens, model_width = token_x.shape
    half = width // 2
    halo = out_head.shape[0]
    x_side = (2 * expert + 1 - parity, tp)
    y_side = (sp, 2 * (1 - row) + core)
    pair = (sp, 2 * row + 1 - core)
    other_quarter = 2 * (1 - row) + core
    sources, rows = (sent_x, sent_g), (rows_x, rows_g)
    started = []

    def send(src, dst, send_sem, recv_sem, device):
        copy = pltpu.make_async_remote_copy(
            src_ref=src, dst_ref=dst, send_sem=send_sem, recv_sem=recv_sem,
            device_id=device, device_id_type=MESH,
        )
        copy.start()
        started.append(copy)

    def spot(t, j, par, quarter):
        return rows[t].at[flipped(expert, j), par, :, columns(quarter, width)]

    loads = [
        pltpu.make_async_copy(src, dst, load_sem.at[n]) for n, (src, dst) in enumerate(zip(hbm, vmem))
    ]
    for load in loads[:6]:
        load.start()
    before, after = lax.rem(sp + n_sp - 1, n_sp), lax.rem(sp + 1, n_sp)
    fixed = [x_side, y_side, pair] + [(2 * flipped(expert, j) + parity, tp) for j in PLAN_CHUNKS]
    fixed += [(near, (lax.rem(tp + n, n_tp))) for near in (before, after) for n in range(n_tp)]
    targets = [(2 * (core + 2 * h) + row, expert) for h in range(2)]
    origins = [(2 * tp + par, 2 * parity + lax.rem(expert, 2)) for par in range(2)]
    barrier = pltpu.get_barrier_semaphore()
    for peer in fixed:
        pl.semaphore_signal(barrier, inc=1, device_id=peer, device_id_type=MESH)
    expected = len(fixed)
    for peer in targets + origins:
        away = jnp.logical_or(peer[0] != sp, peer[1] != tp)

        @pl.when(away)
        def _(peer=peer):
            pl.semaphore_signal(barrier, inc=1, device_id=peer, device_id_type=MESH)

        expected = expected + away.astype(jnp.int32)
    for load in loads[:2]:
        load.wait()
    lanes = lax.broadcasted_iota(jnp.int32, (tokens, tokens), 1)
    below = lax.broadcasted_iota(jnp.int32, (tokens, tokens), 0) < lanes
    first, second = routes[0:1], routes[1:2]
    ids = lax.broadcasted_iota(jnp.int32, (16, tokens), 0)
    first_hot = (ids == first).astype(jnp.float32)
    count = first_hot + (ids == second).astype(jnp.float32)
    earlier = dot(count.astype(jnp.bfloat16), below.astype(jnp.bfloat16), 1, 0)
    slot = lax.broadcasted_iota(jnp.int32, (capacity, tokens), 0)
    for e in range(experts):
        rank = earlier[e : e + 1].astype(jnp.int32)
        again = rank + first_hot[e : e + 1].astype(jnp.int32)
        hit = slot == jnp.where(first == e, rank, -1)
        hit_again = slot == jnp.where(second == e, again, -1)
        chosen_ref[e] = jnp.logical_or(hit, hit_again).astype(jnp.float32).astype(jnp.bfloat16)
        weight_ref[e] = jnp.where(hit, route_weights[0:1], 0.0) + jnp.where(
            hit_again, route_weights[1:2], 0.0
        )
    for load in loads[2:6]:
        load.wait()
    for load in loads[6:]:
        load.start()
    out_b[parity, expert] = (
        gate_b[...].astype(jnp.float32) * conv_out[...].astype(jnp.float32)
    ).astype(jnp.bfloat16)
    tokens_in, prepared = (token_x, token_g), []

    def select(t, one_hot, weight, cols):
        value = dot(one_hot, tokens_in[t][:, cols], 1, 0)
        return (weight * value if t else value).astype(jnp.bfloat16)

    def prepare(kind, t):
        if (kind, t) not in prepared:
            prepared.append((kind, t))
            if kind == "own":
                weight = jnp.sum(weight_ref[expert], axis=1, keepdims=True)
                rows[t][expert, parity] = select(t, chosen_ref[expert], weight, slice(None))
            elif kind == "sent":
                weight = jnp.sum(weight_ref[...].reshape(-1, tokens), axis=1, keepdims=True)
                one_hot = chosen_ref[...].reshape(-1, tokens)
                value = select(t, one_hot, weight, columns(tp, width))
                sources[t][...] = value.reshape(experts, capacity, width)
            else:
                target = flipped(expert, 1)
                weight = jnp.sum(weight_ref[target], axis=1, keepdims=True)
                extra[t] = select(t, chosen_ref[target], weight, columns(other_quarter, width))

    for t in range(2):
        prepare("own", t)
        prepare("sent", t)
    for n in PLAN_EXTRA:
        prepare("extra", n % 2)
    pl.semaphore_wait(barrier, expected)
    steps = [(j, t) for j in PLAN_CHUNKS for t in range(2)]

    def depart(n):
        j, t = steps[n]
        target = flipped(expert, j)
        prepare("sent", t)
        send(sources[t].at[target], rows[t].at[expert, parity, :, columns(tp, width)],
             z_send.at[t, j], z_recv.at[t, j], (2 * target + parity, tp))

    def piece(t, par, which, line, part):
        part = pl.ds(part * (capacity // 2), capacity // 2)
        return rows[t].at[expert, par, part, columns(2 * which + line, width)]

    def depart_extra(n):
        j, t = steps[n]
        prepare("extra", t)
        send(extra.at[t], rows[t].at[expert, parity, :, columns(other_quarter, width)],
             line_send.at[t, j, 1], line_recv.at[t, j, 1], (2 * flipped(expert, j) + parity, tp))

    def cross(t, part):
        block = piece(t, parity, core, row, part)
        send(block, block, own_send.at[t, 0, part], own_recv.at[t, 0, part], x_side)

    def own_stage(n):
        j, t = steps[n]
        block = spot(t, j, parity, tp)
        wait_arrival(block, z_recv.at[t, j])
        send(block, block, line_send.at[t, j, 0], line_recv.at[t, j, 0], x_side)
        if n not in PLAN_EXTRA:
            send(block, block, line_send.at[t, j, 1], line_recv.at[t, j, 1], y_side)
        send(block, block, pair_send.at[t, j, 0], pair_recv.at[t, j, 0], pair)

    def across_stage(t, part):
        block = piece(t, 1 - parity, core, row, part)
        wait_arrival(block, own_recv.at[t, 0, part])
        send(block, block, own_send.at[t, 1, part], own_recv.at[t, 1, part], y_side)
        send(block, block, own_pair_send.at[t, 0, part], own_pair_recv.at[t, 0, part], pair)

    def aside_stage(t, part):
        block = piece(t, 1 - parity, core, 1 - row, part)
        wait_arrival(block, own_recv.at[t, 1, part])
        send(block, block, own_pair_send.at[t, 1, part], own_pair_recv.at[t, 1, part], pair)

    def near_x_stage(n):
        j, t = steps[n]
        block = spot(t, j, 1 - parity, tp)
        wait_arrival(block, line_recv.at[t, j, 0])
        if n not in PLAN_OVER_X:
            send(block, block, relay_send.at[t, j], relay_recv.at[t, j], y_side)
        send(block, block, pair_send.at[t, j, 1], pair_recv.at[t, j, 1], pair)

    def near_y_stage(n):
        j, t = steps[n]
        block = spot(t, j, parity, other_quarter)
        wait_arrival(block, line_recv.at[t, j, 1])
        if n in PLAN_OVER_X:
            send(block, block, relay_send.at[t, j], relay_recv.at[t, j], x_side)
        send(block, block, pair_send.at[t, j, 2], pair_recv.at[t, j, 2], pair)

    def far_stage(n):
        j, t = steps[n]
        block = spot(t, j, 1 - parity, other_quarter)
        wait_arrival(block, relay_recv.at[t, j])
        send(block, block, pair_send.at[t, j, 3], pair_recv.at[t, j, 3], pair)

    def arrived(j, t):
        if j == 0:
            for part in range(2):
                for n, line in enumerate((row, 1 - row)):
                    block = piece(t, 1 - parity, 1 - core, line, part)
                    wait_arrival(block, own_pair_recv.at[t, n, part])
            return
        quarters = (2 * row + 1 - core, 2 * (1 - row) + 1 - core)
        spots = ((parity, quarters[0]), (1 - parity, quarters[0]),
                 (parity, quarters[1]), (1 - parity, quarters[1]))
        for n, (par, quarter) in enumerate(spots):
            wait_arrival(spot(t, j, par, quarter), pair_recv.at[t, j, n])

    def pre_stage(j):
        arrived(j, 0)
        if waiting:
            for load in waiting:
                load.wait()
            waiting.clear()
        x = rows_x[flipped(expert, j)].reshape(2 * capacity, model_width)
        gate_pre[j] = dot(x, wg[...], 1, 1)
        up_pre[j] = dot(x, wu[...], 1, 1)

    def hidden_stage(j):
        arrived(j, 1)
        source = flipped(expert, j)
        g = rows_g[source].reshape(2 * capacity, model_width)
        d_act = dot(g, wd[...], 1, 1)
        gate, up = gate_pre[j], up_pre[j]
        s = jax.nn.sigmoid(gate)
        silu = gate * s
        act[source] = (silu * up).astype(jnp.bfloat16)
        dup[source] = (d_act * silu).astype(jnp.bfloat16)
        dgt[source] = (d_act * up * s * (1.0 + gate * (1.0 - s))).astype(jnp.bfloat16)

    def backward(j):
        source = flipped(expert, j)
        for kept in range(2):
            side_core = core if kept else 1 - core
            store = part_mine if kept else part_out
            for h in range(2):
                cols = columns(2 * h + side_core, width)
                value = (
                    dot(dgt[source], wg[:, cols], 1, 0) + dot(dup[source], wu[:, cols], 1, 0)
                ).astype(jnp.bfloat16)
                for par in range(2):
                    piece = value[par * capacity : (par + 1) * capacity]
                    store[j, h, par, 0] = piece[:, :half]
                    store[j, h, par, 1] = piece[:, half:]
                if not kept:
                    send(part_out.at[j, h], from_pair.at[j, h], rp_send.at[j, h], rp_recv.at[j, h], pair)

    def add_pair(j, h):
        wait_arrival(from_pair.at[j, h], rp_recv.at[j, h])
        total = part_mine[j, h].astype(jnp.float32) + from_pair[j, h].astype(jnp.float32)
        summed[j, h] = total.astype(jnp.bfloat16)

    def pair_x(j):
        add_pair(j, 0)
        send(summed.at[j, 0, 1 - parity], near_x.at[j], near_send.at[j, 0], near_recv.at[j, 0], x_side)

    def pair_y(j):
        add_pair(j, 1)
        send(summed.at[j, 1, :, 1 - row], near_y.at[j], near_send.at[j, 1], near_recv.at[j, 1], y_side)

    def fold_x(j):
        wait_arrival(near_x.at[j], near_recv.at[j, 0])
        total = summed[j, 0, parity, 1 - row].astype(jnp.float32) + near_x[j, 1 - row].astype(jnp.float32)
        passed[j, 0] = total.astype(jnp.bfloat16)
        send(passed.at[j, 0], far_y.at[j], far_send.at[j, 0], far_recv.at[j, 0], y_side)

    def fold_y(j):
        wait_arrival(near_y.at[j], near_recv.at[j, 1])
        total = summed[j, 1, 1 - parity, row].astype(jnp.float32) + near_y[j, 1 - parity].astype(jnp.float32)
        passed[j, 1] = total.astype(jnp.bfloat16)
        send(passed.at[j, 1], far_x.at[j], far_send.at[j, 1], far_recv.at[j, 1], x_side)

    def go_home(j, h, value):
        cols = pl.ds(h * half, half)
        if j == 0:
            out_back[expert, :, cols] = value
            return
        final[j, :, cols] = value
        send(final.at[j, :, cols], out_back.at[expert, :, cols], back_send.at[j, h], back_recv.at[j, h],
             (2 * flipped(expert, j) + parity, tp))

    def home_left(j):
        wait_arrival(far_y.at[j], far_recv.at[j, 0])
        total = summed[j, 0, parity, row].astype(jnp.float32) + near_x[j, row].astype(jnp.float32)
        go_home(j, 0, (total + far_y[j].astype(jnp.float32)).astype(jnp.bfloat16))

    def home_right(j):
        wait_arrival(far_x.at[j], far_recv.at[j, 1])
        total = summed[j, 1, parity, row].astype(jnp.float32) + near_y[j, parity].astype(jnp.float32)
        go_home(j, 1, (total + far_x[j].astype(jnp.float32)).astype(jnp.bfloat16))

    def weight_grad(n):
        out, left, right = (
            (out_down, act, rows_g), (out_gate, dgt, rows_x), (out_up, dup, rows_x)
        )[n // 4]
        tile = model_width // 4
        cols = slice(n % 4 * tile, (n % 4 + 1) * tile)
        lhs = left[...].reshape(-1, left.shape[-1])
        rhs = right[:, :, :, cols].reshape(-1, tile)
        out[:, cols] = dot(lhs, rhs, 0, 0).astype(jnp.bfloat16)

    def share_branch():
        block = out_b.at[parity, expert]
        for j in PLAN_CHUNKS:
            send(block, block, b_send.at[j], b_recv.at[j], (2 * flipped(expert, j) + parity, tp))
        send(gate_b.at[pl.ds(0, halo)], out_head, h_send.at[0], h_recv.at[0], (before, tp))

    def cross_branch():
        for j in PLAN_CHUNKS:
            wait_arrival(out_b.at[parity, flipped(expert, j)], b_recv.at[j])
        send(out_b.at[parity], out_b.at[parity], b_send.at[0], b_recv.at[0], x_side)

    stages = {
        "depart": depart, "extra": depart_extra, "cross": cross, "own": own_stage,
        "across": across_stage, "aside": aside_stage,
        "near_x": near_x_stage, "near_y": near_y_stage, "far": far_stage,
        "pre": pre_stage, "hidden": hidden_stage, "back": backward, "pair_x": pair_x, "pair_y": pair_y,
        "fold_x": fold_x, "fold_y": fold_y, "left": home_left, "right": home_right, "grad": weight_grad,
        "share": share_branch,
    }
    waiting = loads[6:]
    folds = [n for n, stage in enumerate(PLAN) if stage[0] in ("fold_x", "fold_y")]
    for n, (name, *numbers) in enumerate(PLAN):
        stages[name](*numbers)
        if n == folds[-1]:
            cross_branch()

    def block_columns(h, line, side_core):
        return columns(4 * h + 2 * side_core + line, half)

    for j in PLAN_CHUNKS:
        for h in range(2):
            block = out_back.at[flipped(expert, j), :, pl.ds(h * half, half)]
            wait_arrival(block, back_recv.at[j, h])
    one_hot = chosen_ref[...].reshape(experts * capacity, tokens)
    total = dot(one_hot, out_back[...].reshape(experts * capacity, width), 0, 0)
    guarded = []
    for h in range(2):
        cols = block_columns(h, row, core)
        base = token_g[:, cols].astype(jnp.float32)
        value = (base + total[:, h * half : (h + 1) * half]).astype(jnp.bfloat16)
        part_ref[h] = value
        stream_ref[pl.ds(0, tokens), cols] = value
    for h in range(2):
        src, dst, recv = part_ref.at[h], block_ref.at[parity, expert], place_recv.at[parity]
        away = jnp.logical_or(targets[h][0] != sp, targets[h][1] != tp)
        copy = pltpu.make_async_remote_copy(
            src_ref=src, dst_ref=dst, send_sem=place_send.at[h], recv_sem=recv,
            device_id=targets[h], device_id_type=MESH,
        )

        @pl.when(away)
        def _(copy=copy):
            copy.start()

        @pl.when(jnp.logical_not(away))
        def _(src=src, dst=dst, recv=recv):
            pltpu.make_async_copy(src, dst, recv).start()

        guarded.append((away, copy))
    for h in range(2):
        src, cols = part_ref.at[h], block_columns(h, row, core)
        dst = stream_ref.at[pl.ds(0, tokens), cols]
        send(src, dst, gather_send.at[h, 0], gather_recv.at[h, 0], y_side)
        send(src, dst, gather_send.at[h, 1], gather_recv.at[h, 1], pair)
    for h in range(2):
        src, cols = part_ref.at[h], block_columns(h, row, core)
        for n in range(n_tp):
            send(src.at[pl.ds(0, halo)], stream_ref.at[pl.ds(tokens, halo), cols],
                 halo_send.at[h, n], halo_recv.at[h, n], (before, lax.rem(tp + n, n_tp)))
    for par in range(2):
        block = block_ref.at[par, tp]
        wait_arrival(block, place_recv.at[par])
        send(block, block, held_send.at[par, 0], held_recv.at[par, 0], y_side)
        send(block, block, held_send.at[par, 1], held_recv.at[par, 1], pair)
    for h in range(2):
        block = stream_ref.at[pl.ds(0, tokens), block_columns(h, 1 - row, core)]
        wait_arrival(block, gather_recv.at[h, 0])
        send(block, block, gather_send.at[h, 2], gather_recv.at[h, 2], pair)
    for h in range(2):
        for line, slot in ((row, 1), (1 - row, 2)):
            wait_arrival(
                stream_ref.at[pl.ds(0, tokens), block_columns(h, line, 1 - core)], gather_recv.at[h, slot]
            )
        for n in range(n_tp):
            source = lax.rem(tp + n_tp - n, n_tp)
            cols = block_columns(h, source // 2, lax.rem(source, 2))
            wait_arrival(stream_ref.at[pl.ds(tokens, halo), cols], halo_recv.at[h, n])
    wait_arrival(out_head, h_recv.at[0])
    channels = conv_out.shape[1]
    reach = taps.shape[0] - 1
    d_branch = dot(stream_ref[...], out_proj[...], 1, 0)
    following = jnp.where(sp == n_sp - 1, 0.0, d_branch[tokens:] * out_head[...].astype(jnp.float32))
    d_branch = d_branch[:tokens]
    out_gate_b[...] = (d_branch * conv_out[...].astype(jnp.float32)).astype(jnp.bfloat16)
    extended[pl.ds(0, tokens)] = d_branch * gate_b[...].astype(jnp.float32)
    extended[pl.ds(tokens, halo)] = following
    d_input = jnp.zeros((tokens, channels), jnp.float32)
    for tap in range(reach + 1):
        d_input = d_input + taps[tap : tap + 1] * extended[pl.ds(reach - tap, tokens)]
    out_hidden[...] = (d_input * gate_c[...].astype(jnp.float32)).astype(jnp.bfloat16)
    out_gate_c[...] = (d_input * hidden_h[...].astype(jnp.float32)).astype(jnp.bfloat16)
    for par in range(2):
        block = block_ref.at[par, other_quarter]
        wait_arrival(block, held_recv.at[par, 0])
        send(block, block, held_send.at[par, 2], held_recv.at[par, 2], pair)
    wait_arrival(out_b.at[1 - parity], b_recv.at[0])
    for par in range(2):
        for line, slot in ((row, 1), (1 - row, 2)):
            wait_arrival(block_ref.at[par, 2 * line + 1 - core], held_recv.at[par, slot])
    out_proj_grad[...] = dot(
        block_ref[...].reshape(-1, half), out_b[...].reshape(-1, channels), 0, 0
    )
    for copy in started:
        copy.wait_send()
    for away, copy in guarded:
        pl.when(away)(copy.wait_send)


def run_experts(operands, halo, n_sp):
    _, _, token_x, token_g, gate_b, _, _, _, wg, *_ = operands
    tokens, model_width = token_x.shape
    experts = n_tp = n_sp // 2
    capacity = 2 * (3 * tokens // n_sp)
    width = model_width // n_tp
    units = wg.shape[0]
    half = width // 2
    channels = gate_b.shape[1]
    dma = pltpu.SemaphoreType.DMA

    def vmem(*shape):
        return pltpu.VMEM(shape, jnp.bfloat16)

    def wide(*shape):
        return pltpu.VMEM(shape, jnp.float32)

    rows = vmem(experts, 2, capacity, model_width)
    hidden = vmem(experts, 2 * capacity, units)
    blocks = vmem(experts, 2, 2, 2, capacity, half)
    near = vmem(experts, 2, capacity, half)
    far = vmem(experts, capacity, half)
    routed = vmem(experts, capacity, width)
    weight = vmem(units, model_width)
    pre = wide(experts, 2 * capacity, units)
    small = vmem(tokens, channels)
    return pl.pallas_call(
        functools.partial(expert_kernel, n_sp, n_tp),
        out_shape=(weight, weight, weight, wide(half, channels), small, small, small),
        in_specs=[HBM] * len(operands),
        out_specs=(VMEM,) * 7,
        scratch_shapes=[
            *(pltpu.VMEM(operand.shape, operand.dtype) for operand in operands),
            vmem(tokens + halo, model_width), vmem(2, experts, tokens, half),
            vmem(2, experts, tokens, channels), vmem(halo, channels),
            vmem(experts, capacity, tokens), wide(experts, capacity, tokens),
            wide(tokens + halo, channels),
            routed, routed, vmem(2, capacity, width), routed, vmem(2, tokens, half),
            rows, rows, hidden, hidden, hidden, blocks, blocks, blocks, blocks,
            near, near, near, far, far, routed, pre, pre,
            dma((len(operands),)), dma((2, experts)), dma((2, experts)), dma((2, 2, 2)), dma((2, 2, 2)),
            dma((2, experts, 2)), dma((2, experts, 2)), dma((2, experts)), dma((2, experts)),
            dma((2, experts, 4)), dma((2, experts, 4)), dma((2, 2, 2)), dma((2, 2, 2)),
            dma((experts,)), dma((experts,)), dma((1,)), dma((1,)),
            dma((experts, 2)), dma((experts, 2)), dma((experts, 2)), dma((experts, 2)),
            dma((experts, 2)), dma((experts, 2)), dma((experts, 2)), dma((experts, 2)),
            dma((2, 3)), dma((2, 3)), dma((2, n_tp)), dma((2, n_tp)),
            dma((2,)), dma((2,)), dma((2, 3)), dma((2, 3)),
        ],
        compiler_params=pltpu.CompilerParams(
            collective_id=3, has_side_effects=True, vmem_limit_bytes=48 * 1024 * 1024
        ),
    )(*operands)


def store_kernel(*refs):
    count = len(refs) // 2
    moves = [
        pltpu.make_async_copy(refs[n], refs[count + n], refs[-1].at[n]) for n in range(count)
    ]
    for move in moves:
        move.start()
    for move in moves:
        move.wait()


def store(arrays):
    return pl.pallas_call(
        store_kernel,
        out_shape=tuple(jax.ShapeDtypeStruct(a.shape, a.dtype) for a in arrays),
        in_specs=[VMEM] * len(arrays),
        out_specs=(HBM,) * len(arrays),
        scratch_shapes=[pltpu.SemaphoreType.DMA((len(arrays),))],
        compiler_params=pltpu.CompilerParams(vmem_limit_bytes=16 * 1024 * 1024),
    )(*arrays)


def stream_kernel(
    n_sp, n_tp, part_ref, stream_ref, block_ref,
    tp_send, tp_recv, h_send, h_recv, b_send, b_recv, s_send, s_recv,
):
    sp, tp = lax.axis_index("sp"), lax.axis_index("tp")
    tokens, width = part_ref.shape
    block = block_ref.shape[2]
    halo = stream_ref.shape[0] - tokens
    per_part, per_peer = width // block, n_sp // n_tp
    greet([
        (lax.rem(sp + i, n_sp), lax.rem(tp + j, n_tp))
        for i in range(n_sp) for j in range(n_tp) if i or j
    ])
    started = []

    def send(src, dst, send_sem, recv_sem, device):
        copy = pltpu.make_async_remote_copy(
            src_ref=src, dst_ref=dst, send_sem=send_sem, recv_sem=recv_sem,
            device_id=device, device_id_type=MESH,
        )
        copy.start()
        started.append((None, copy))

    keeper = sp // per_peer
    for b in range(per_part):
        target = tp * per_part + b
        src = part_ref.at[:, b * block : (b + 1) * block]
        dst = block_ref.at[sp]
        away = jnp.logical_or(target != sp, keeper != tp)
        copy = pltpu.make_async_remote_copy(
            src_ref=src, dst_ref=dst, send_sem=b_send.at[b], recv_sem=b_recv.at[lax.rem(sp, per_peer)],
            device_id=(target, keeper), device_id_type=MESH,
        )

        @pl.when(away)
        def _(copy=copy):
            copy.start()

        @pl.when(jnp.logical_not(away))
        def _(src=src, dst=dst):
            pltpu.make_async_copy(src, dst, b_recv.at[lax.rem(sp, per_peer)]).start()

        started.append((away, copy))
    mine = stream_ref.at[pl.ds(0, tokens), columns(tp, width)]
    edge = stream_ref.at[pl.ds(tokens, halo), columns(tp, width)]
    before = lax.rem(sp + n_sp - 1, n_sp)
    pltpu.make_async_copy(part_ref, mine, tp_recv.at[0]).start()
    for j in range(n_tp):
        peer = lax.rem(tp + j, n_tp)
        if j:
            send(part_ref, mine, tp_send.at[j], tp_recv.at[j], (sp, peer))
        send(part_ref.at[pl.ds(0, halo)], edge, h_send.at[j], h_recv.at[j], (before, peer))
    for n in range(per_peer):
        held = block_ref.at[tp * per_peer + n]
        wait_arrival(held, b_recv.at[n])
        for j in range(1, n_tp):
            send(held, held, s_send.at[n, j], s_recv.at[n, j], (sp, lax.rem(tp + j, n_tp)))
    for j in range(n_tp):
        source = lax.rem(tp + n_tp - j, n_tp)
        wait_arrival(stream_ref.at[pl.ds(0, tokens), columns(source, width)], tp_recv.at[j])
        wait_arrival(stream_ref.at[pl.ds(tokens, halo), columns(source, width)], h_recv.at[j])
        for n in range(per_peer):
            if j:
                wait_arrival(block_ref.at[source * per_peer + n], s_recv.at[n, j])
    for away, copy in started:
        if away is None:
            copy.wait_send()
        else:
            pl.when(away)(copy.wait_send)


def share_stream(part, halo, n_sp, n_tp):
    tokens, width = part.shape
    dma = pltpu.SemaphoreType.DMA
    block = width * n_tp // n_sp
    per_peer = n_sp // n_tp
    return pl.pallas_call(
        functools.partial(stream_kernel, n_sp, n_tp),
        out_shape=(
            jax.ShapeDtypeStruct((tokens + halo, width * n_tp), jnp.bfloat16),
            jax.ShapeDtypeStruct((n_sp, tokens, block), jnp.bfloat16),
        ),
        in_specs=[VMEM],
        out_specs=(VMEM, VMEM),
        scratch_shapes=[
            dma((n_tp,)), dma((n_tp,)), dma((n_tp,)), dma((n_tp,)),
            dma((width // block,)), dma((per_peer,)), dma((per_peer, n_tp)), dma((per_peer, n_tp)),
        ],
        compiler_params=pltpu.CompilerParams(collective_id=2, has_side_effects=True),
    )(part)


def slot_choice(routes, experts, capacity):
    flat_ids = routes.reshape(-1)
    one_hot = (flat_ids[:, None] == jnp.arange(experts, dtype=jnp.int32)[None, :])
    count = flat_ids.shape[0]
    before = jnp.arange(count)[:, None] > jnp.arange(count)[None, :]
    earlier = jnp.dot(
        before.astype(jnp.bfloat16), one_hot.astype(jnp.bfloat16), preferred_element_type=jnp.float32
    )
    ranked = jnp.sum(jnp.where(one_hot, earlier, 0.0), axis=1).astype(jnp.int32)
    return (flat_ids * capacity + ranked).reshape(routes.shape)


def contract_rows(left_side, right_side):
    return lax.dot_general(
        left_side, right_side, (((0,), (0,)), ((), ())), preferred_element_type=jnp.float32
    )


def contract_cols(left_side, right_side):
    return lax.dot_general(
        left_side, right_side, (((1,), (1,)), ((), ())), preferred_element_type=jnp.float32
    )


def per_device(
    moe_input,
    out_grad,
    routes,
    route_weights,
    gate_cols,
    up_cols,
    down_rows,
    out_proj,
    conv_out,
    gate_b,
    gate_c,
    hidden_h,
    conv_taps,
):
    seq_devices = lax.axis_size("sp")
    experts = seq_devices // 2
    tokens_here, model_width = moe_input.shape
    top_count = routes.shape[1]
    half_cap = 3 * tokens_here // seq_devices
    capacity = 2 * half_cap
    slot_count = experts * capacity
    n_tp = lax.axis_size("tp")
    halo = 16
    aligned = model_width % (seq_devices * 128) == 0
    planned = aligned and experts == len(PLAN_CHUNKS) + 1 == n_tp and capacity % 32 == 0
    if planned and top_count == 2 and conv_taps.shape[0] <= halo:
        operands = (
            routes.T, route_weights.T, moe_input, out_grad, gate_b, conv_out, gate_c, hidden_h,
            gate_cols.T, up_cols.T, down_rows, out_proj, conv_taps,
        )
        operands = tuple(pltpu.with_memory_space_constraint(a, pltpu.HBM) for a in operands)
        grads = run_experts(operands, halo, seq_devices)
        grad_gate, grad_up, *rest = store(grads)
        return (grad_gate.T, grad_up.T, *rest)
    positions = slot_choice(routes, experts, capacity)
    slots = jnp.arange(slot_count, dtype=jnp.int32)
    hits = slots[:, None, None] == positions[None]
    chosen = jnp.any(hits, axis=2).astype(jnp.bfloat16)
    slot_weight = jnp.sum(jnp.where(hits, route_weights[None], 0.0), axis=(1, 2))
    quarter = model_width // n_tp
    column_start = lax.axis_index("tp") * quarter
    source_x = lax.dynamic_slice_in_dim(moe_input, column_start, quarter, 1)
    source_g = lax.dynamic_slice_in_dim(out_grad, column_start, quarter, 1)
    sent_x = jnp.dot(chosen, source_x, preferred_element_type=jnp.float32).astype(jnp.bfloat16)
    sent_g = jnp.dot(chosen, source_g, preferred_element_type=jnp.float32)
    sent_g = (slot_weight[:, None] * sent_g).astype(jnp.bfloat16)
    branch = (gate_b.astype(jnp.float32) * conv_out.astype(jnp.float32)).astype(jnp.bfloat16)
    rows_x, rows_g, all_branch, next_gate_b = dispatch(
        sent_x.reshape(experts, capacity, quarter),
        sent_g.reshape(experts, capacity, quarter),
        branch,
        gate_b[:halo],
        seq_devices,
        n_tp,
    )
    rows_x = rows_x.reshape(-1, model_width)
    rows_g = rows_g.reshape(-1, model_width)
    gate_pre = jnp.dot(rows_x, gate_cols, preferred_element_type=jnp.float32)
    up_pre = jnp.dot(rows_x, up_cols, preferred_element_type=jnp.float32)
    sigmoid_g = jax.nn.sigmoid(gate_pre)
    silu_g = gate_pre * sigmoid_g
    activation = (silu_g * up_pre).astype(jnp.bfloat16)
    grad_down = contract_rows(activation, rows_g).astype(jnp.bfloat16)
    d_act = contract_cols(rows_g, down_rows)
    d_up = (d_act * silu_g).astype(jnp.bfloat16)
    d_gate = (d_act * up_pre * sigmoid_g * (1.0 + gate_pre * (1.0 - sigmoid_g))).astype(
        jnp.bfloat16
    )
    grad_gate = contract_rows(rows_x, d_gate).astype(jnp.bfloat16)
    grad_up = contract_rows(rows_x, d_up).astype(jnp.bfloat16)
    partial_value = (contract_cols(d_gate, gate_cols) + contract_cols(d_up, up_cols)).astype(
        jnp.bfloat16
    )
    returned = give_back(
        partial_value.reshape(2, experts, capacity, model_width), seq_devices, n_tp
    ).reshape(slot_count, quarter)
    stream_part = (source_g.astype(jnp.float32) + contract_rows(chosen, returned)).astype(
        jnp.bfloat16
    )
    if aligned:
        stream, stream_block = share_stream(stream_part, halo, seq_devices, n_tp)
        grad_proj = contract_rows(
            stream_block.reshape(-1, stream_block.shape[2]),
            all_branch.reshape(-1, all_branch.shape[2]),
        )
    else:
        stream = lax.all_gather(stream_part, "tp", axis=1, tiled=True)
        grad_proj = lax.psum_scatter(
            contract_rows(stream, branch), "sp", scatter_dimension=0, tiled=True
        )
    d_branch = jnp.dot(stream, out_proj, preferred_element_type=jnp.float32)
    d_after = d_branch[tokens_here:]
    d_branch = d_branch[:tokens_here]
    grad_gate_b = (d_branch * conv_out.astype(jnp.float32)).astype(jnp.bfloat16)
    d_conv = d_branch * gate_b.astype(jnp.float32)
    kernel_taps = conv_taps.shape[0]
    kernel_reach = kernel_taps - 1
    if aligned:
        last = lax.axis_index("sp") == seq_devices - 1
        next_rows_in = jnp.where(last, 0.0, d_after * next_gate_b.astype(jnp.float32))[:kernel_reach]
    else:
        next_rows_in = from_behind(d_conv[:kernel_reach], "sp", -1)
    extended = jnp.concatenate([d_conv, next_rows_in], axis=0)
    d_input = jnp.zeros_like(d_conv)
    for tap_index in range(kernel_taps):
        offset = kernel_reach - tap_index
        d_input = d_input + conv_taps[tap_index][None, :] * extended[offset : offset + tokens_here]
    grad_hidden = (d_input * gate_c.astype(jnp.float32)).astype(jnp.bfloat16)
    grad_gate_c = (d_input * hidden_h.astype(jnp.float32)).astype(jnp.bfloat16)
    return (grad_gate, grad_up, grad_down, grad_proj, grad_hidden, grad_gate_b, grad_gate_c)


def solution(mesh):
    placed = (
        P("sp", None),
        P("sp", None),
        P("sp", None),
        P("sp", None),
        P(None, ("sp", "tp")),
        P(None, ("sp", "tp")),
        P(("sp", "tp"), None),
        P(None, "tp"),
        P("sp", "tp"),
        P("sp", "tp"),
        P("sp", "tp"),
        P("sp", "tp"),
        P(None, "tp"),
    )
    return jax.shard_map(
        per_device,
        mesh=mesh,
        in_specs=placed,
        out_specs=(
            P(None, ("sp", "tp")),
            P(None, ("sp", "tp")),
            P(("sp", "tp"), None),
            P("sp", "tp"),
            P("sp", "tp"),
            P("sp", "tp"),
            P("sp", "tp"),
        ),
        check_vma=False,
    )
```

```python
import functools

import jax
import jax.numpy as jnp
from jax import lax
from jax.experimental import pallas as pl
from jax.experimental.pallas import tpu as pltpu
from jax.sharding import PartitionSpec as P


def from_behind(block, axis, distance):
    devices = range(lax.axis_size(axis))
    route = [(i - distance, i) for i in devices if i - distance in devices]
    return lax.ppermute(block, axis, route)


MESH = pl.DeviceIdType.MESH
VMEM = pl.BlockSpec(memory_space=pltpu.VMEM)
HBM = pl.BlockSpec(memory_space=pltpu.HBM)


def columns(index, width):
    return pl.ds(pl.multiple_of(index * width, width), width)


def wait_arrival(ref, sem):
    pltpu.make_async_copy(ref, ref, sem).wait()


def greet(peers):
    barrier = pltpu.get_barrier_semaphore()
    for peer in peers:
        pl.semaphore_signal(barrier, inc=1, device_id=peer, device_id_type=MESH)
    pl.semaphore_wait(barrier, len(peers))


def place(n_tp):
    sp, tp = lax.axis_index("sp"), lax.axis_index("tp")
    expert, parity = sp // 2, lax.rem(sp, 2)
    row, core = tp // 2, lax.rem(tp, 2)
    return sp, tp, expert, parity, row, core


def dispatch_kernel(
    n_sp, n_tp, chunks,
    x_ref, g_ref, branch_ref, head_ref,
    out_x, out_g, out_b, out_head,
    z_send, z_recv, own_send, relay_send, near_recv, diag_recv, pair_send, pair_recv, b_send, b_recv, h_send, h_recv,
):
    experts = n_sp // 2
    sp, tp, expert, parity, row, core = place(n_tp)
    width = x_ref.shape[-1]
    size = experts // chunks
    x_side = (2 * expert + 1 - parity, tp)
    y_side = (sp, 2 * (1 - row) + core)
    pair = (sp, 2 * row + 1 - core)
    greet([(lax.rem(sp + d, n_sp), tp) for d in range(1, n_sp)] + [y_side, pair])
    started = []
    sources, outs = (x_ref, g_ref), (out_x, out_g)

    def spot(t, par, first, quarter, count):
        return outs[t].at[par, pl.ds(first, count), :, columns(quarter, width)]

    def send(src, device, send_sem, recv_sem):
        copy = pltpu.make_async_remote_copy(
            src_ref=src, dst_ref=src, send_sem=send_sem, recv_sem=recv_sem,
            device_id=device, device_id_type=MESH,
        )
        copy.start()
        started.append(copy)

    for t in range(2):
        for d in range(experts):
            target = lax.rem(expert + d, experts)
            src = sources[t].at[pl.ds(target, 1)]
            dst = spot(t, parity, expert, tp, 1)
            if d == 0:
                pltpu.make_async_copy(src, dst, z_recv.at[t, 0]).start()
                continue
            copy = pltpu.make_async_remote_copy(
                src_ref=src, dst_ref=dst, send_sem=z_send.at[t, d], recv_sem=z_recv.at[t, d],
                device_id=(2 * target + parity, tp), device_id_type=MESH,
            )
            copy.start()
            started.append(copy)
    for d in range(n_sp):
        dst = out_b.at[sp]
        if d == 0:
            pltpu.make_async_copy(branch_ref, dst, b_recv.at[0]).start()
            continue
        copy = pltpu.make_async_remote_copy(
            src_ref=branch_ref, dst_ref=dst, send_sem=b_send.at[d], recv_sem=b_recv.at[d],
            device_id=(lax.rem(sp + d, n_sp), tp), device_id_type=MESH,
        )
        copy.start()
        started.append(copy)

    copy = pltpu.make_async_remote_copy(
        src_ref=head_ref, dst_ref=out_head, send_sem=h_send.at[0], recv_sem=h_recv.at[0],
        device_id=(lax.rem(sp + n_sp - 1, n_sp), tp), device_id_type=MESH,
    )
    copy.start()
    started.append(copy)

    own_chunk = expert // size
    other_quarter = 2 * (1 - row) + core

    def first_of(k):
        return lax.rem(own_chunk + chunks - k, chunks) * size

    def own_stage(k, t):
        first = first_of(k)
        for i in range(size):
            source = first + i
            d = lax.rem(expert + experts - source, experts)
            wait_arrival(spot(t, parity, source, tp, 1), z_recv.at[t, d])
        block = spot(t, parity, first, tp, size)
        send(block, x_side, own_send.at[t, k, 0], near_recv.at[t, k, 0])
        send(block, y_side, own_send.at[t, k, 1], near_recv.at[t, k, 1])
        send(block, pair, pair_send.at[t, k, 0], pair_recv.at[t, k, 0])

    def near_stage(k, t):
        first = first_of(k)
        from_x = spot(t, 1 - parity, first, tp, size)
        from_y = spot(t, parity, first, other_quarter, size)
        wait_arrival(from_x, near_recv.at[t, k, 0])
        if (k + t) % 2 == 0:
            send(from_x, y_side, relay_send.at[t, k], diag_recv.at[t, k])
        send(from_x, pair, pair_send.at[t, k, 1], pair_recv.at[t, k, 1])
        wait_arrival(from_y, near_recv.at[t, k, 1])
        if (k + t) % 2 == 1:
            send(from_y, x_side, relay_send.at[t, k], diag_recv.at[t, k])
        send(from_y, pair, pair_send.at[t, k, 2], pair_recv.at[t, k, 2])

    def far_stage(k, t):
        block = spot(t, 1 - parity, first_of(k), other_quarter, size)
        wait_arrival(block, diag_recv.at[t, k])
        send(block, pair, pair_send.at[t, k, 3], pair_recv.at[t, k, 3])

    order = [0] + [k for n in range(1, chunks // 2 + 1) for k in dict.fromkeys((n, chunks - n))]
    steps = [(k, t) for k in order for t in range(2)]
    for n in range(len(steps) + 3):
        if n < len(steps):
            own_stage(*steps[n])
        if 1 <= n < len(steps) + 1:
            near_stage(*steps[n - 1])
        if 3 <= n < len(steps) + 3:
            far_stage(*steps[n - 3])
    for k, t in steps:
        first = first_of(k)
        quarters = (2 * row + 1 - core, 2 * (1 - row) + 1 - core)
        spots = ((parity, quarters[0]), (1 - parity, quarters[0]),
                 (parity, quarters[1]), (1 - parity, quarters[1]))
        for j, (par, quarter) in enumerate(spots):
            wait_arrival(spot(t, par, first, quarter, size), pair_recv.at[t, k, j])
    for d in range(n_sp):
        wait_arrival(out_b.at[lax.rem(sp + n_sp - d, n_sp)], b_recv.at[d])
    wait_arrival(out_head, h_recv.at[0])
    for copy in started:
        copy.wait_send()


def dispatch(x, g, branch, head, n_sp, n_tp):
    experts, capacity, width = x.shape
    chunks = min(experts, 4)
    dma = pltpu.SemaphoreType.DMA
    rows = jax.ShapeDtypeStruct((2, experts, capacity, width * n_tp), jnp.bfloat16)
    return pl.pallas_call(
        functools.partial(dispatch_kernel, n_sp, n_tp, chunks),
        out_shape=(
            rows, rows, jax.ShapeDtypeStruct((n_sp,) + branch.shape, branch.dtype),
            jax.ShapeDtypeStruct(head.shape, head.dtype),
        ),
        in_specs=[VMEM] * 4,
        out_specs=(VMEM,) * 4,
        scratch_shapes=[
            dma((2, experts)), dma((2, experts)), dma((2, chunks, 2)), dma((2, chunks)),
            dma((2, chunks, 2)), dma((2, chunks)), dma((2, chunks, 4)), dma((2, chunks, 4)),
            dma((n_sp,)), dma((n_sp,)), dma((1,)), dma((1,)),
        ],
        compiler_params=pltpu.CompilerParams(
            collective_id=0, has_side_effects=True, vmem_limit_bytes=48 * 1024 * 1024
        ),
    )(x, g, branch, head)


def return_kernel(
    n_sp, n_tp, chunks,
    part_ref, out_ref,
    from_pair, summed, from_chips, final,
    pair_send, pair_recv, chip_send, chip_recv, z_send, z_recv,
):
    experts = n_sp // 2
    sp, tp, expert, parity, row, core = place(n_tp)
    width = out_ref.shape[-1]
    pair = (sp, 2 * row + 1 - core)
    offsets = ((1, 1), (1, 0), (0, 1), (0, 0))

    def other(dp, dr):
        return lax.rem(parity + dp, 2), lax.rem(row + dr, 2)

    chips = [(2 * expert + other(dp, dr)[0], 2 * other(dp, dr)[1] + core) for dp, dr in offsets[:3]]
    along = [(2 * lax.rem(expert + d, experts) + parity, tp) for d in range(1, experts)]
    greet([pair] + chips + along)
    started, guarded = [], []

    def send(src, dst, send_sem, recv_sem, device):
        copy = pltpu.make_async_remote_copy(
            src_ref=src, dst_ref=dst, send_sem=send_sem, recv_sem=recv_sem,
            device_id=device, device_id_type=MESH,
        )
        copy.start()
        started.append(copy)

    size = experts // chunks
    own_chunk = expert // size
    order = [chunks // 2] if chunks > 1 else []
    order += [k for k in range(1, chunks) if k not in order] + [0]

    def first_of(k):
        return lax.rem(own_chunk + k, chunks) * size

    for k in order:
        part = pl.ds(first_of(k), size)
        for n, (dp, dr) in enumerate(offsets):
            par, line = other(dp, dr)
            src = part_ref.at[par, part, :, columns(2 * line + 1 - core, width)]
            send(src, from_pair.at[n, part], pair_send.at[n, k], pair_recv.at[n, k], pair)
    for k in order:
        first = first_of(k)
        part = pl.ds(first, size)
        for n, (dp, dr) in enumerate(offsets):
            par, line = other(dp, dr)
            wait_arrival(from_pair.at[n, part], pair_recv.at[n, k])
            for i in range(size):
                mine = part_ref[par, first + i, :, columns(2 * line + core, width)]
                total = mine.astype(jnp.float32) + from_pair[n, first + i].astype(jnp.float32)
                summed[n, first + i] = total.astype(jnp.bfloat16)
            if n < 3:
                send(summed.at[n, part], from_chips.at[n, part], chip_send.at[n, k],
                     chip_recv.at[n, k], chips[n])
    for k in order:
        first = first_of(k)
        part = pl.ds(first, size)
        for n in range(3):
            wait_arrival(from_chips.at[n, part], chip_recv.at[n, k])
        for i in range(size):
            target = first + i
            total = summed[3, target].astype(jnp.float32)
            for n in range(3):
                total = total + from_chips[n, target].astype(jnp.float32)
            final[target] = total.astype(jnp.bfloat16)
            away = target != expert
            copy = pltpu.make_async_remote_copy(
                src_ref=final.at[target], dst_ref=out_ref.at[expert],
                send_sem=z_send.at[target], recv_sem=z_recv.at[expert],
                device_id=(2 * target + parity, tp), device_id_type=MESH,
            )
            if size == 1 and k:
                copy.start()
                started.append(copy)
                continue
            if size == 1:
                out_ref[expert] = final[target]
                continue

            @pl.when(away)
            def _(copy=copy):
                copy.start()

            @pl.when(jnp.logical_not(away))
            def _():
                out_ref[expert] = final[expert]

            guarded.append((away, copy))
    for d in range(1, experts):
        source = lax.rem(expert + experts - d, experts)
        wait_arrival(out_ref.at[source], z_recv.at[source])
    for copy in started:
        copy.wait_send()
    for away, copy in guarded:
        pl.when(away)(copy.wait_send)


def give_back(part, n_sp, n_tp):
    _, experts, capacity, model_width = part.shape
    width = model_width // n_tp
    dma = pltpu.SemaphoreType.DMA
    block = (experts, capacity, width)
    chunks = min(experts, 4)
    return pl.pallas_call(
        functools.partial(return_kernel, n_sp, n_tp, chunks),
        out_shape=jax.ShapeDtypeStruct(block, jnp.bfloat16),
        in_specs=[VMEM],
        out_specs=VMEM,
        scratch_shapes=[
            pltpu.VMEM((4,) + block, jnp.bfloat16), pltpu.VMEM((4,) + block, jnp.bfloat16),
            pltpu.VMEM((3,) + block, jnp.bfloat16), pltpu.VMEM(block, jnp.bfloat16),
            dma((4, chunks)), dma((4, chunks)), dma((3, chunks)), dma((3, chunks)),
            dma((experts,)), dma((experts,)),
        ],
        compiler_params=pltpu.CompilerParams(
            collective_id=1, has_side_effects=True, vmem_limit_bytes=48 * 1024 * 1024
        ),
    )(part)


def dot(left, right, left_dim, right_dim):
    return lax.dot_general(
        left, right, (((left_dim,), (right_dim,)), ((), ())), preferred_element_type=jnp.float32
    )


def flipped(index, bits):
    bit = 1
    while bit <= bits:
        if bits & bit:
            index = index + bit - 2 * bit * lax.rem(index // bit, 2)
        bit *= 2
    return index


PLAN_CHUNKS = (1, 3, 2)
PLAN_OVER_X = (0, 5)
PLAN_EXTRA = (0, 1)
PLAN = (
    ("depart", 3), ("cross", 0, 0), ("cross", 0, 1), ("cross", 1, 0), ("cross", 1, 1), ("depart", 0),
    ("depart", 2), ("depart", 1), ("across", 0, 0), ("across", 0, 1), ("across", 1, 0), ("across", 1, 1),
    ("depart", 4), ("extra", 0), ("depart", 5), ("own", 3), ("own", 0), ("near_x", 3), ("own", 2),
    ("aside", 0, 0), ("aside", 0, 1), ("near_y", 3), ("own", 1), ("aside", 1, 0), ("aside", 1, 1),
    ("near_x", 2), ("far", 3), ("extra", 1), ("own", 4), ("share",), ("near_y", 2), ("pre", 0), ("near_y", 0),
    ("own", 5), ("far", 2), ("hidden", 0), ("near_x", 4), ("back", 0), ("near_y", 4), ("pre", 3),
    ("near_x", 1), ("near_y", 1), ("far", 0), ("hidden", 3), ("near_y", 5), ("back", 3), ("near_x", 0),
    ("near_x", 5), ("pair_x", 3), ("far", 4), ("pair_x", 0), ("pair_y", 3), ("pair_y", 0), ("pre", 1),
    ("far", 5), ("pre", 2), ("far", 1), ("hidden", 2), ("back", 2), ("fold_y", 3), ("fold_x", 3),
    ("hidden", 1), ("pair_x", 2), ("pair_y", 2), ("back", 1), ("grad", 3), ("pair_x", 1), ("left", 3),
    ("right", 3), ("pair_y", 1), ("grad", 5), ("grad", 11), ("grad", 8), ("fold_x", 2), ("grad", 10),
    ("fold_y", 2), ("fold_y", 0), ("fold_x", 1), ("grad", 9), ("fold_y", 1), ("left", 2), ("right", 2),
    ("fold_x", 0), ("left", 1), ("right", 1), ("grad", 7), ("grad", 2), ("grad", 4), ("left", 0),
    ("right", 0), ("grad", 0), ("grad", 1), ("grad", 6),
)


def expert_kernel(
    n_sp, n_tp, *refs,
):
    hbm, refs = refs[:13], refs[13:]
    out_gate, out_up, out_down, out_proj_grad, out_hidden, out_gate_b, out_gate_c = refs[:7]
    vmem, refs = refs[7:20], refs[20:]
    routes, route_weights, token_x, token_g, gate_b, conv_out, *vmem_rest = vmem
    gate_c, hidden_h, wg, wu, wd, out_proj, taps = vmem_rest
    (
        stream_ref, block_ref, out_b, out_head, chosen_ref, weight_ref, extended,
        sent_x, sent_g, extra, out_back, part_ref,
        rows_x, rows_g, act, dup, dgt, part_out, part_mine, from_pair, summed,
        near_x, near_y, passed, far_x, far_y, final, gate_pre, up_pre,
        load_sem, z_send, z_recv, own_send, own_recv, line_send, line_recv, relay_send, relay_recv,
        pair_send, pair_recv, own_pair_send, own_pair_recv, b_send, b_recv, h_send, h_recv,
        rp_send, rp_recv, near_send, near_recv, far_send, far_recv, back_send, back_recv,
        gather_send, gather_recv, halo_send, halo_recv, place_send, place_recv, held_send, held_recv,
    ) = refs
    experts = n_sp // 2
    sp, tp, expert, parity, row, core = place(n_tp)
    capacity, width = sent_x.shape[1:]
    tokens, model_width = token_x.shape
    half = width // 2
    halo = out_head.shape[0]
    x_side = (2 * expert + 1 - parity, tp)
    y_side = (sp, 2 * (1 - row) + core)
    pair = (sp, 2 * row + 1 - core)
    other_quarter = 2 * (1 - row) + core
    sources, rows = (sent_x, sent_g), (rows_x, rows_g)
    started = []

    def send(src, dst, send_sem, recv_sem, device):
        copy = pltpu.make_async_remote_copy(
            src_ref=src, dst_ref=dst, send_sem=send_sem, recv_sem=recv_sem,
            device_id=device, device_id_type=MESH,
        )
        copy.start()
        started.append(copy)

    def spot(t, j, par, quarter):
        return rows[t].at[flipped(expert, j), par, :, columns(quarter, width)]

    loads = [
        pltpu.make_async_copy(src, dst, load_sem.at[n]) for n, (src, dst) in enumerate(zip(hbm, vmem))
    ]
    for load in loads[:6]:
        load.start()
    before, after = lax.rem(sp + n_sp - 1, n_sp), lax.rem(sp + 1, n_sp)
    fixed = [x_side, y_side, pair] + [(2 * flipped(expert, j) + parity, tp) for j in PLAN_CHUNKS]
    fixed += [(near, (lax.rem(tp + n, n_tp))) for near in (before, after) for n in range(n_tp)]
    targets = [(2 * (core + 2 * h) + row, expert) for h in range(2)]
    origins = [(2 * tp + par, 2 * parity + lax.rem(expert, 2)) for par in range(2)]
    barrier = pltpu.get_barrier_semaphore()
    for peer in fixed:
        pl.semaphore_signal(barrier, inc=1, device_id=peer, device_id_type=MESH)
    expected = len(fixed)
    for peer in targets + origins:
        away = jnp.logical_or(peer[0] != sp, peer[1] != tp)

        @pl.when(away)
        def _(peer=peer):
            pl.semaphore_signal(barrier, inc=1, device_id=peer, device_id_type=MESH)

        expected = expected + away.astype(jnp.int32)
    for load in loads[:2]:
        load.wait()
    lanes = lax.broadcasted_iota(jnp.int32, (tokens, tokens), 1)
    below = lax.broadcasted_iota(jnp.int32, (tokens, tokens), 0) < lanes
    first, second = routes[0:1], routes[1:2]
    ids = lax.broadcasted_iota(jnp.int32, (16, tokens), 0)
    first_hot = (ids == first).astype(jnp.float32)
    count = first_hot + (ids == second).astype(jnp.float32)
    earlier = dot(count.astype(jnp.bfloat16), below.astype(jnp.bfloat16), 1, 0)
    slot = lax.broadcasted_iota(jnp.int32, (capacity, tokens), 0)
    for e in range(experts):
        rank = earlier[e : e + 1].astype(jnp.int32)
        again = rank + first_hot[e : e + 1].astype(jnp.int32)
        hit = slot == jnp.where(first == e, rank, -1)
        hit_again = slot == jnp.where(second == e, again, -1)
        chosen_ref[e] = jnp.logical_or(hit, hit_again).astype(jnp.float32).astype(jnp.bfloat16)
        weight_ref[e] = jnp.where(hit, route_weights[0:1], 0.0) + jnp.where(
            hit_again, route_weights[1:2], 0.0
        )
    for load in loads[2:6]:
        load.wait()
    for load in loads[6:]:
        load.start()
    out_b[parity, expert] = (
        gate_b[...].astype(jnp.float32) * conv_out[...].astype(jnp.float32)
    ).astype(jnp.bfloat16)
    tokens_in, prepared = (token_x, token_g), []

    def select(t, one_hot, weight, cols):
        value = dot(one_hot, tokens_in[t][:, cols], 1, 0)
        return (weight * value if t else value).astype(jnp.bfloat16)

    def prepare(kind, t):
        if (kind, t) not in prepared:
            prepared.append((kind, t))
            if kind == "own":
                weight = jnp.sum(weight_ref[expert], axis=1, keepdims=True)
                rows[t][expert, parity] = select(t, chosen_ref[expert], weight, slice(None))
            elif kind == "sent":
                weight = jnp.sum(weight_ref[...].reshape(-1, tokens), axis=1, keepdims=True)
                one_hot = chosen_ref[...].reshape(-1, tokens)
                value = select(t, one_hot, weight, columns(tp, width))
                sources[t][...] = value.reshape(experts, capacity, width)
            else:
                target = flipped(expert, 1)
                weight = jnp.sum(weight_ref[target], axis=1, keepdims=True)
                extra[t] = select(t, chosen_ref[target], weight, columns(other_quarter, width))

    for t in range(2):
        prepare("own", t)
        prepare("sent", t)
    for n in PLAN_EXTRA:
        prepare("extra", n % 2)
    pl.semaphore_wait(barrier, expected)
    steps = [(j, t) for j in PLAN_CHUNKS for t in range(2)]

    def depart(n):
        j, t = steps[n]
        target = flipped(expert, j)
        prepare("sent", t)
        send(sources[t].at[target], rows[t].at[expert, parity, :, columns(tp, width)],
             z_send.at[t, j], z_recv.at[t, j], (2 * target + parity, tp))

    def piece(t, par, which, line, part):
        part = pl.ds(part * (capacity // 2), capacity // 2)
        return rows[t].at[expert, par, part, columns(2 * which + line, width)]

    def depart_extra(n):
        j, t = steps[n]
        prepare("extra", t)
        send(extra.at[t], rows[t].at[expert, parity, :, columns(other_quarter, width)],
             line_send.at[t, j, 1], line_recv.at[t, j, 1], (2 * flipped(expert, j) + parity, tp))

    def cross(t, part):
        block = piece(t, parity, core, row, part)
        send(block, block, own_send.at[t, 0, part], own_recv.at[t, 0, part], x_side)

    def own_stage(n):
        j, t = steps[n]
        block = spot(t, j, parity, tp)
        wait_arrival(block, z_recv.at[t, j])
        send(block, block, line_send.at[t, j, 0], line_recv.at[t, j, 0], x_side)
        if n not in PLAN_EXTRA:
            send(block, block, line_send.at[t, j, 1], line_recv.at[t, j, 1], y_side)
        send(block, block, pair_send.at[t, j, 0], pair_recv.at[t, j, 0], pair)

    def across_stage(t, part):
        block = piece(t, 1 - parity, core, row, part)
        wait_arrival(block, own_recv.at[t, 0, part])
        send(block, block, own_send.at[t, 1, part], own_recv.at[t, 1, part], y_side)
        send(block, block, own_pair_send.at[t, 0, part], own_pair_recv.at[t, 0, part], pair)

    def aside_stage(t, part):
        block = piece(t, 1 - parity, core, 1 - row, part)
        wait_arrival(block, own_recv.at[t, 1, part])
        send(block, block, own_pair_send.at[t, 1, part], own_pair_recv.at[t, 1, part], pair)

    def near_x_stage(n):
        j, t = steps[n]
        block = spot(t, j, 1 - parity, tp)
        wait_arrival(block, line_recv.at[t, j, 0])
        if n not in PLAN_OVER_X:
            send(block, block, relay_send.at[t, j], relay_recv.at[t, j], y_side)
        send(block, block, pair_send.at[t, j, 1], pair_recv.at[t, j, 1], pair)

    def near_y_stage(n):
        j, t = steps[n]
        block = spot(t, j, parity, other_quarter)
        wait_arrival(block, line_recv.at[t, j, 1])
        if n in PLAN_OVER_X:
            send(block, block, relay_send.at[t, j], relay_recv.at[t, j], x_side)
        send(block, block, pair_send.at[t, j, 2], pair_recv.at[t, j, 2], pair)

    def far_stage(n):
        j, t = steps[n]
        block = spot(t, j, 1 - parity, other_quarter)
        wait_arrival(block, relay_recv.at[t, j])
        send(block, block, pair_send.at[t, j, 3], pair_recv.at[t, j, 3], pair)

    def arrived(j, t):
        if j == 0:
            for part in range(2):
                for n, line in enumerate((row, 1 - row)):
                    block = piece(t, 1 - parity, 1 - core, line, part)
                    wait_arrival(block, own_pair_recv.at[t, n, part])
            return
        quarters = (2 * row + 1 - core, 2 * (1 - row) + 1 - core)
        spots = ((parity, quarters[0]), (1 - parity, quarters[0]),
                 (parity, quarters[1]), (1 - parity, quarters[1]))
        for n, (par, quarter) in enumerate(spots):
            wait_arrival(spot(t, j, par, quarter), pair_recv.at[t, j, n])

    def pre_stage(j):
        arrived(j, 0)
        if waiting:
            for load in waiting:
                load.wait()
            waiting.clear()
        x = rows_x[flipped(expert, j)].reshape(2 * capacity, model_width)
        gate_pre[j] = dot(x, wg[...], 1, 1)
        up_pre[j] = dot(x, wu[...], 1, 1)

    def hidden_stage(j):
        arrived(j, 1)
        source = flipped(expert, j)
        g = rows_g[source].reshape(2 * capacity, model_width)
        d_act = dot(g, wd[...], 1, 1)
        gate, up = gate_pre[j], up_pre[j]
        s = jax.nn.sigmoid(gate)
        silu = gate * s
        act[source] = (silu * up).astype(jnp.bfloat16)
        dup[source] = (d_act * silu).astype(jnp.bfloat16)
        dgt[source] = (d_act * up * s * (1.0 + gate * (1.0 - s))).astype(jnp.bfloat16)

    def backward(j):
        source = flipped(expert, j)
        for kept in range(2):
            side_core = core if kept else 1 - core
            store = part_mine if kept else part_out
            for h in range(2):
                cols = columns(2 * h + side_core, width)
                value = (
                    dot(dgt[source], wg[:, cols], 1, 0) + dot(dup[source], wu[:, cols], 1, 0)
                ).astype(jnp.bfloat16)
                for par in range(2):
                    piece = value[par * capacity : (par + 1) * capacity]
                    store[j, h, par, 0] = piece[:, :half]
                    store[j, h, par, 1] = piece[:, half:]
                if not kept:
                    send(part_out.at[j, h], from_pair.at[j, h], rp_send.at[j, h], rp_recv.at[j, h], pair)

    def add_pair(j, h):
        wait_arrival(from_pair.at[j, h], rp_recv.at[j, h])
        total = part_mine[j, h].astype(jnp.float32) + from_pair[j, h].astype(jnp.float32)
        summed[j, h] = total.astype(jnp.bfloat16)

    def pair_x(j):
        add_pair(j, 0)
        send(summed.at[j, 0, 1 - parity], near_x.at[j], near_send.at[j, 0], near_recv.at[j, 0], x_side)

    def pair_y(j):
        add_pair(j, 1)
        send(summed.at[j, 1, :, 1 - row], near_y.at[j], near_send.at[j, 1], near_recv.at[j, 1], y_side)

    def fold_x(j):
        wait_arrival(near_x.at[j], near_recv.at[j, 0])
        total = summed[j, 0, parity, 1 - row].astype(jnp.float32) + near_x[j, 1 - row].astype(jnp.float32)
        passed[j, 0] = total.astype(jnp.bfloat16)
        send(passed.at[j, 0], far_y.at[j], far_send.at[j, 0], far_recv.at[j, 0], y_side)

    def fold_y(j):
        wait_arrival(near_y.at[j], near_recv.at[j, 1])
        total = summed[j, 1, 1 - parity, row].astype(jnp.float32) + near_y[j, 1 - parity].astype(jnp.float32)
        passed[j, 1] = total.astype(jnp.bfloat16)
        send(passed.at[j, 1], far_x.at[j], far_send.at[j, 1], far_recv.at[j, 1], x_side)

    def go_home(j, h, value):
        cols = pl.ds(h * half, half)
        if j == 0:
            out_back[expert, :, cols] = value
            return
        final[j, :, cols] = value
        send(final.at[j, :, cols], out_back.at[expert, :, cols], back_send.at[j, h], back_recv.at[j, h],
             (2 * flipped(expert, j) + parity, tp))

    def home_left(j):
        wait_arrival(far_y.at[j], far_recv.at[j, 0])
        total = summed[j, 0, parity, row].astype(jnp.float32) + near_x[j, row].astype(jnp.float32)
        go_home(j, 0, (total + far_y[j].astype(jnp.float32)).astype(jnp.bfloat16))

    def home_right(j):
        wait_arrival(far_x.at[j], far_recv.at[j, 1])
        total = summed[j, 1, parity, row].astype(jnp.float32) + near_y[j, parity].astype(jnp.float32)
        go_home(j, 1, (total + far_x[j].astype(jnp.float32)).astype(jnp.bfloat16))

    def weight_grad(n):
        out, left, right = (
            (out_down, act, rows_g), (out_gate, dgt, rows_x), (out_up, dup, rows_x)
        )[n // 4]
        tile = model_width // 4
        cols = slice(n % 4 * tile, (n % 4 + 1) * tile)
        lhs = left[...].reshape(-1, left.shape[-1])
        rhs = right[:, :, :, cols].reshape(-1, tile)
        out[:, cols] = dot(lhs, rhs, 0, 0).astype(jnp.bfloat16)

    def share_branch():
        block = out_b.at[parity, expert]
        for j in PLAN_CHUNKS:
            send(block, block, b_send.at[j], b_recv.at[j], (2 * flipped(expert, j) + parity, tp))
        send(gate_b.at[pl.ds(0, halo)], out_head, h_send.at[0], h_recv.at[0], (before, tp))

    def cross_branch():
        for j in PLAN_CHUNKS:
            wait_arrival(out_b.at[parity, flipped(expert, j)], b_recv.at[j])
        send(out_b.at[parity], out_b.at[parity], b_send.at[0], b_recv.at[0], x_side)

    stages = {
        "depart": depart, "extra": depart_extra, "cross": cross, "own": own_stage,
        "across": across_stage, "aside": aside_stage,
        "near_x": near_x_stage, "near_y": near_y_stage, "far": far_stage,
        "pre": pre_stage, "hidden": hidden_stage, "back": backward, "pair_x": pair_x, "pair_y": pair_y,
        "fold_x": fold_x, "fold_y": fold_y, "left": home_left, "right": home_right, "grad": weight_grad,
        "share": share_branch,
    }
    waiting = loads[6:]
    folds = [n for n, stage in enumerate(PLAN) if stage[0] in ("fold_x", "fold_y")]
    for n, (name, *numbers) in enumerate(PLAN):
        stages[name](*numbers)
        if n == folds[-1]:
            cross_branch()

    def block_columns(h, line, side_core):
        return columns(4 * h + 2 * side_core + line, half)

    total = dot(chosen_ref[expert], out_back[expert], 0, 0)
    for j in dict.fromkeys(stage[1] for stage in PLAN if stage[0] == "right" and stage[1]):
        source = flipped(expert, j)
        for h in range(2):
            wait_arrival(out_back.at[source, :, pl.ds(h * half, half)], back_recv.at[j, h])
        total = total + dot(chosen_ref[source], out_back[source], 0, 0)
    guarded = []
    for h in range(2):
        cols = block_columns(h, row, core)
        base = token_g[:, cols].astype(jnp.float32)
        value = (base + total[:, h * half : (h + 1) * half]).astype(jnp.bfloat16)
        part_ref[h] = value
        stream_ref[pl.ds(0, tokens), cols] = value
    for h in range(2):
        src, dst, recv = part_ref.at[h], block_ref.at[parity, expert], place_recv.at[parity]
        away = jnp.logical_or(targets[h][0] != sp, targets[h][1] != tp)
        copy = pltpu.make_async_remote_copy(
            src_ref=src, dst_ref=dst, send_sem=place_send.at[h], recv_sem=recv,
            device_id=targets[h], device_id_type=MESH,
        )

        @pl.when(away)
        def _(copy=copy):
            copy.start()

        @pl.when(jnp.logical_not(away))
        def _(src=src, dst=dst, recv=recv):
            pltpu.make_async_copy(src, dst, recv).start()

        guarded.append((away, copy))
    for h in range(2):
        src, cols = part_ref.at[h], block_columns(h, row, core)
        dst = stream_ref.at[pl.ds(0, tokens), cols]
        send(src, dst, gather_send.at[h, 0], gather_recv.at[h, 0], y_side)
        send(src, dst, gather_send.at[h, 1], gather_recv.at[h, 1], pair)
    for h in range(2):
        src, cols = part_ref.at[h], block_columns(h, row, core)
        for n in range(n_tp):
            send(src.at[pl.ds(0, halo)], stream_ref.at[pl.ds(tokens, halo), cols],
                 halo_send.at[h, n], halo_recv.at[h, n], (before, lax.rem(tp + n, n_tp)))
    for par in range(2):
        block = block_ref.at[par, tp]
        wait_arrival(block, place_recv.at[par])
        send(block, block, held_send.at[par, 0], held_recv.at[par, 0], y_side)
        send(block, block, held_send.at[par, 1], held_recv.at[par, 1], pair)
    for h in range(2):
        block = stream_ref.at[pl.ds(0, tokens), block_columns(h, 1 - row, core)]
        wait_arrival(block, gather_recv.at[h, 0])
        send(block, block, gather_send.at[h, 2], gather_recv.at[h, 2], pair)
    for h in range(2):
        for line, slot in ((row, 1), (1 - row, 2)):
            wait_arrival(
                stream_ref.at[pl.ds(0, tokens), block_columns(h, line, 1 - core)], gather_recv.at[h, slot]
            )
        for n in range(n_tp):
            source = lax.rem(tp + n_tp - n, n_tp)
            cols = block_columns(h, source // 2, lax.rem(source, 2))
            wait_arrival(stream_ref.at[pl.ds(tokens, halo), cols], halo_recv.at[h, n])
    wait_arrival(out_head, h_recv.at[0])
    channels = conv_out.shape[1]
    reach = taps.shape[0] - 1
    d_branch = dot(stream_ref[...], out_proj[...], 1, 0)
    following = jnp.where(sp == n_sp - 1, 0.0, d_branch[tokens:] * out_head[...].astype(jnp.float32))
    d_branch = d_branch[:tokens]
    out_gate_b[...] = (d_branch * conv_out[...].astype(jnp.float32)).astype(jnp.bfloat16)
    extended[pl.ds(0, tokens)] = d_branch * gate_b[...].astype(jnp.float32)
    extended[pl.ds(tokens, halo)] = following
    d_input = jnp.zeros((tokens, channels), jnp.float32)
    for tap in range(reach + 1):
        d_input = d_input + taps[tap : tap + 1] * extended[pl.ds(reach - tap, tokens)]
    out_hidden[...] = (d_input * gate_c[...].astype(jnp.float32)).astype(jnp.bfloat16)
    out_gate_c[...] = (d_input * hidden_h[...].astype(jnp.float32)).astype(jnp.bfloat16)
    for par in range(2):
        block = block_ref.at[par, other_quarter]
        wait_arrival(block, held_recv.at[par, 0])
        send(block, block, held_send.at[par, 2], held_recv.at[par, 2], pair)
    wait_arrival(out_b.at[1 - parity], b_recv.at[0])
    for par in range(2):
        for line, slot in ((row, 1), (1 - row, 2)):
            wait_arrival(block_ref.at[par, 2 * line + 1 - core], held_recv.at[par, slot])
    out_proj_grad[...] = dot(
        block_ref[...].reshape(-1, half), out_b[...].reshape(-1, channels), 0, 0
    )
    for copy in started:
        copy.wait_send()
    for away, copy in guarded:
        pl.when(away)(copy.wait_send)


def run_experts(operands, halo, n_sp):
    _, _, token_x, token_g, gate_b, _, _, _, wg, *_ = operands
    tokens, model_width = token_x.shape
    experts = n_tp = n_sp // 2
    capacity = 2 * (3 * tokens // n_sp)
    width = model_width // n_tp
    units = wg.shape[0]
    half = width // 2
    channels = gate_b.shape[1]
    dma = pltpu.SemaphoreType.DMA

    def vmem(*shape):
        return pltpu.VMEM(shape, jnp.bfloat16)

    def wide(*shape):
        return pltpu.VMEM(shape, jnp.float32)

    rows = vmem(experts, 2, capacity, model_width)
    hidden = vmem(experts, 2 * capacity, units)
    blocks = vmem(experts, 2, 2, 2, capacity, half)
    near = vmem(experts, 2, capacity, half)
    far = vmem(experts, capacity, half)
    routed = vmem(experts, capacity, width)
    weight = vmem(units, model_width)
    pre = wide(experts, 2 * capacity, units)
    small = vmem(tokens, channels)
    return pl.pallas_call(
        functools.partial(expert_kernel, n_sp, n_tp),
        out_shape=(weight, weight, weight, wide(half, channels), small, small, small),
        in_specs=[HBM] * len(operands),
        out_specs=(VMEM,) * 7,
        scratch_shapes=[
            *(pltpu.VMEM(operand.shape, operand.dtype) for operand in operands),
            vmem(tokens + halo, model_width), vmem(2, experts, tokens, half),
            vmem(2, experts, tokens, channels), vmem(halo, channels),
            vmem(experts, capacity, tokens), wide(experts, capacity, tokens),
            wide(tokens + halo, channels),
            routed, routed, vmem(2, capacity, width), routed, vmem(2, tokens, half),
            rows, rows, hidden, hidden, hidden, blocks, blocks, blocks, blocks,
            near, near, near, far, far, routed, pre, pre,
            dma((len(operands),)), dma((2, experts)), dma((2, experts)), dma((2, 2, 2)), dma((2, 2, 2)),
            dma((2, experts, 2)), dma((2, experts, 2)), dma((2, experts)), dma((2, experts)),
            dma((2, experts, 4)), dma((2, experts, 4)), dma((2, 2, 2)), dma((2, 2, 2)),
            dma((experts,)), dma((experts,)), dma((1,)), dma((1,)),
            dma((experts, 2)), dma((experts, 2)), dma((experts, 2)), dma((experts, 2)),
            dma((experts, 2)), dma((experts, 2)), dma((experts, 2)), dma((experts, 2)),
            dma((2, 3)), dma((2, 3)), dma((2, n_tp)), dma((2, n_tp)),
            dma((2,)), dma((2,)), dma((2, 3)), dma((2, 3)),
        ],
        compiler_params=pltpu.CompilerParams(
            collective_id=3, has_side_effects=True, vmem_limit_bytes=48 * 1024 * 1024
        ),
    )(*operands)


def store_kernel(*refs):
    count = len(refs) // 2
    moves = [
        pltpu.make_async_copy(refs[n], refs[count + n], refs[-1].at[n]) for n in range(count)
    ]
    for move in moves:
        move.start()
    for move in moves:
        move.wait()


def store(arrays):
    return pl.pallas_call(
        store_kernel,
        out_shape=tuple(jax.ShapeDtypeStruct(a.shape, a.dtype) for a in arrays),
        in_specs=[VMEM] * len(arrays),
        out_specs=(HBM,) * len(arrays),
        scratch_shapes=[pltpu.SemaphoreType.DMA((len(arrays),))],
        compiler_params=pltpu.CompilerParams(vmem_limit_bytes=16 * 1024 * 1024),
    )(*arrays)


def stream_kernel(
    n_sp, n_tp, part_ref, stream_ref, block_ref,
    tp_send, tp_recv, h_send, h_recv, b_send, b_recv, s_send, s_recv,
):
    sp, tp = lax.axis_index("sp"), lax.axis_index("tp")
    tokens, width = part_ref.shape
    block = block_ref.shape[2]
    halo = stream_ref.shape[0] - tokens
    per_part, per_peer = width // block, n_sp // n_tp
    greet([
        (lax.rem(sp + i, n_sp), lax.rem(tp + j, n_tp))
        for i in range(n_sp) for j in range(n_tp) if i or j
    ])
    started = []

    def send(src, dst, send_sem, recv_sem, device):
        copy = pltpu.make_async_remote_copy(
            src_ref=src, dst_ref=dst, send_sem=send_sem, recv_sem=recv_sem,
            device_id=device, device_id_type=MESH,
        )
        copy.start()
        started.append((None, copy))

    keeper = sp // per_peer
    for b in range(per_part):
        target = tp * per_part + b
        src = part_ref.at[:, b * block : (b + 1) * block]
        dst = block_ref.at[sp]
        away = jnp.logical_or(target != sp, keeper != tp)
        copy = pltpu.make_async_remote_copy(
            src_ref=src, dst_ref=dst, send_sem=b_send.at[b], recv_sem=b_recv.at[lax.rem(sp, per_peer)],
            device_id=(target, keeper), device_id_type=MESH,
        )

        @pl.when(away)
        def _(copy=copy):
            copy.start()

        @pl.when(jnp.logical_not(away))
        def _(src=src, dst=dst):
            pltpu.make_async_copy(src, dst, b_recv.at[lax.rem(sp, per_peer)]).start()

        started.append((away, copy))
    mine = stream_ref.at[pl.ds(0, tokens), columns(tp, width)]
    edge = stream_ref.at[pl.ds(tokens, halo), columns(tp, width)]
    before = lax.rem(sp + n_sp - 1, n_sp)
    pltpu.make_async_copy(part_ref, mine, tp_recv.at[0]).start()
    for j in range(n_tp):
        peer = lax.rem(tp + j, n_tp)
        if j:
            send(part_ref, mine, tp_send.at[j], tp_recv.at[j], (sp, peer))
        send(part_ref.at[pl.ds(0, halo)], edge, h_send.at[j], h_recv.at[j], (before, peer))
    for n in range(per_peer):
        held = block_ref.at[tp * per_peer + n]
        wait_arrival(held, b_recv.at[n])
        for j in range(1, n_tp):
            send(held, held, s_send.at[n, j], s_recv.at[n, j], (sp, lax.rem(tp + j, n_tp)))
    for j in range(n_tp):
        source = lax.rem(tp + n_tp - j, n_tp)
        wait_arrival(stream_ref.at[pl.ds(0, tokens), columns(source, width)], tp_recv.at[j])
        wait_arrival(stream_ref.at[pl.ds(tokens, halo), columns(source, width)], h_recv.at[j])
        for n in range(per_peer):
            if j:
                wait_arrival(block_ref.at[source * per_peer + n], s_recv.at[n, j])
    for away, copy in started:
        if away is None:
            copy.wait_send()
        else:
            pl.when(away)(copy.wait_send)


def share_stream(part, halo, n_sp, n_tp):
    tokens, width = part.shape
    dma = pltpu.SemaphoreType.DMA
    block = width * n_tp // n_sp
    per_peer = n_sp // n_tp
    return pl.pallas_call(
        functools.partial(stream_kernel, n_sp, n_tp),
        out_shape=(
            jax.ShapeDtypeStruct((tokens + halo, width * n_tp), jnp.bfloat16),
            jax.ShapeDtypeStruct((n_sp, tokens, block), jnp.bfloat16),
        ),
        in_specs=[VMEM],
        out_specs=(VMEM, VMEM),
        scratch_shapes=[
            dma((n_tp,)), dma((n_tp,)), dma((n_tp,)), dma((n_tp,)),
            dma((width // block,)), dma((per_peer,)), dma((per_peer, n_tp)), dma((per_peer, n_tp)),
        ],
        compiler_params=pltpu.CompilerParams(collective_id=2, has_side_effects=True),
    )(part)


def slot_choice(routes, experts, capacity):
    flat_ids = routes.reshape(-1)
    one_hot = (flat_ids[:, None] == jnp.arange(experts, dtype=jnp.int32)[None, :])
    count = flat_ids.shape[0]
    before = jnp.arange(count)[:, None] > jnp.arange(count)[None, :]
    earlier = jnp.dot(
        before.astype(jnp.bfloat16), one_hot.astype(jnp.bfloat16), preferred_element_type=jnp.float32
    )
    ranked = jnp.sum(jnp.where(one_hot, earlier, 0.0), axis=1).astype(jnp.int32)
    return (flat_ids * capacity + ranked).reshape(routes.shape)


def contract_rows(left_side, right_side):
    return lax.dot_general(
        left_side, right_side, (((0,), (0,)), ((), ())), preferred_element_type=jnp.float32
    )


def contract_cols(left_side, right_side):
    return lax.dot_general(
        left_side, right_side, (((1,), (1,)), ((), ())), preferred_element_type=jnp.float32
    )


def per_device(
    moe_input,
    out_grad,
    routes,
    route_weights,
    gate_cols,
    up_cols,
    down_rows,
    out_proj,
    conv_out,
    gate_b,
    gate_c,
    hidden_h,
    conv_taps,
):
    seq_devices = lax.axis_size("sp")
    experts = seq_devices // 2
    tokens_here, model_width = moe_input.shape
    top_count = routes.shape[1]
    half_cap = 3 * tokens_here // seq_devices
    capacity = 2 * half_cap
    slot_count = experts * capacity
    n_tp = lax.axis_size("tp")
    halo = 16
    aligned = model_width % (seq_devices * 128) == 0
    planned = aligned and experts == len(PLAN_CHUNKS) + 1 == n_tp and capacity % 32 == 0
    if planned and top_count == 2 and conv_taps.shape[0] <= halo:
        operands = (
            routes.T, route_weights.T, moe_input, out_grad, gate_b, conv_out, gate_c, hidden_h,
            gate_cols.T, up_cols.T, down_rows, out_proj, conv_taps,
        )
        operands = tuple(pltpu.with_memory_space_constraint(a, pltpu.HBM) for a in operands)
        grads = run_experts(operands, halo, seq_devices)
        grad_gate, grad_up, *rest = store(grads)
        return (grad_gate.T, grad_up.T, *rest)
    positions = slot_choice(routes, experts, capacity)
    slots = jnp.arange(slot_count, dtype=jnp.int32)
    hits = slots[:, None, None] == positions[None]
    chosen = jnp.any(hits, axis=2).astype(jnp.bfloat16)
    slot_weight = jnp.sum(jnp.where(hits, route_weights[None], 0.0), axis=(1, 2))
    quarter = model_width // n_tp
    column_start = lax.axis_index("tp") * quarter
    source_x = lax.dynamic_slice_in_dim(moe_input, column_start, quarter, 1)
    source_g = lax.dynamic_slice_in_dim(out_grad, column_start, quarter, 1)
    sent_x = jnp.dot(chosen, source_x, preferred_element_type=jnp.float32).astype(jnp.bfloat16)
    sent_g = jnp.dot(chosen, source_g, preferred_element_type=jnp.float32)
    sent_g = (slot_weight[:, None] * sent_g).astype(jnp.bfloat16)
    branch = (gate_b.astype(jnp.float32) * conv_out.astype(jnp.float32)).astype(jnp.bfloat16)
    rows_x, rows_g, all_branch, next_gate_b = dispatch(
        sent_x.reshape(experts, capacity, quarter),
        sent_g.reshape(experts, capacity, quarter),
        branch,
        gate_b[:halo],
        seq_devices,
        n_tp,
    )
    rows_x = rows_x.reshape(-1, model_width)
    rows_g = rows_g.reshape(-1, model_width)
    gate_pre = jnp.dot(rows_x, gate_cols, preferred_element_type=jnp.float32)
    up_pre = jnp.dot(rows_x, up_cols, preferred_element_type=jnp.float32)
    sigmoid_g = jax.nn.sigmoid(gate_pre)
    silu_g = gate_pre * sigmoid_g
    activation = (silu_g * up_pre).astype(jnp.bfloat16)
    grad_down = contract_rows(activation, rows_g).astype(jnp.bfloat16)
    d_act = contract_cols(rows_g, down_rows)
    d_up = (d_act * silu_g).astype(jnp.bfloat16)
    d_gate = (d_act * up_pre * sigmoid_g * (1.0 + gate_pre * (1.0 - sigmoid_g))).astype(
        jnp.bfloat16
    )
    grad_gate = contract_rows(rows_x, d_gate).astype(jnp.bfloat16)
    grad_up = contract_rows(rows_x, d_up).astype(jnp.bfloat16)
    partial_value = (contract_cols(d_gate, gate_cols) + contract_cols(d_up, up_cols)).astype(
        jnp.bfloat16
    )
    returned = give_back(
        partial_value.reshape(2, experts, capacity, model_width), seq_devices, n_tp
    ).reshape(slot_count, quarter)
    stream_part = (source_g.astype(jnp.float32) + contract_rows(chosen, returned)).astype(
        jnp.bfloat16
    )
    if aligned:
        stream, stream_block = share_stream(stream_part, halo, seq_devices, n_tp)
        grad_proj = contract_rows(
            stream_block.reshape(-1, stream_block.shape[2]),
            all_branch.reshape(-1, all_branch.shape[2]),
        )
    else:
        stream = lax.all_gather(stream_part, "tp", axis=1, tiled=True)
        grad_proj = lax.psum_scatter(
            contract_rows(stream, branch), "sp", scatter_dimension=0, tiled=True
        )
    d_branch = jnp.dot(stream, out_proj, preferred_element_type=jnp.float32)
    d_after = d_branch[tokens_here:]
    d_branch = d_branch[:tokens_here]
    grad_gate_b = (d_branch * conv_out.astype(jnp.float32)).astype(jnp.bfloat16)
    d_conv = d_branch * gate_b.astype(jnp.float32)
    kernel_taps = conv_taps.shape[0]
    kernel_reach = kernel_taps - 1
    if aligned:
        last = lax.axis_index("sp") == seq_devices - 1
        next_rows_in = jnp.where(last, 0.0, d_after * next_gate_b.astype(jnp.float32))[:kernel_reach]
    else:
        next_rows_in = from_behind(d_conv[:kernel_reach], "sp", -1)
    extended = jnp.concatenate([d_conv, next_rows_in], axis=0)
    d_input = jnp.zeros_like(d_conv)
    for tap_index in range(kernel_taps):
        offset = kernel_reach - tap_index
        d_input = d_input + conv_taps[tap_index][None, :] * extended[offset : offset + tokens_here]
    grad_hidden = (d_input * gate_c.astype(jnp.float32)).astype(jnp.bfloat16)
    grad_gate_c = (d_input * hidden_h.astype(jnp.float32)).astype(jnp.bfloat16)
    return (grad_gate, grad_up, grad_down, grad_proj, grad_hidden, grad_gate_b, grad_gate_c)


def solution(mesh):
    placed = (
        P("sp", None),
        P("sp", None),
        P("sp", None),
        P("sp", None),
        P(None, ("sp", "tp")),
        P(None, ("sp", "tp")),
        P(("sp", "tp"), None),
        P(None, "tp"),
        P("sp", "tp"),
        P("sp", "tp"),
        P("sp", "tp"),
        P("sp", "tp"),
        P(None, "tp"),
    )
    return jax.shard_map(
        per_device,
        mesh=mesh,
        in_specs=placed,
        out_specs=(
            P(None, ("sp", "tp")),
            P(None, ("sp", "tp")),
            P(("sp", "tp"), None),
            P("sp", "tp"),
            P("sp", "tp"),
            P("sp", "tp"),
            P("sp", "tp"),
        ),
        check_vma=False,
    )
```
